32 devices in a mesh: sp: 8 (over z, x), tp: 4 (over y, core).
Axes of the slice: x: 2, y: 2, z: 4, core: 2. Of those that a mesh axis runs over, the one named last changes fastest.
Arguments:
- queries: bfloat16 [4096, 1024], P('sp', 'tp'), may hold values from -5.5 to 5.5
- key_vectors: bfloat16 [4096, 1024], P('sp', 'tp'), may hold values from -5.5 to 5.5
- latents: bfloat16 [4096, 2048], P('sp', 'tp'), may hold values from -6 to 6
- w_value: bfloat16 [2048, 1024], P(None, 'tp'), may hold values from -0.125 to 0.125
- log_sums: float32 [4096, 16], P('sp', 'tp'), as said below
- out_pair: bfloat16 [4096, 2048], P('sp', 'tp'), may hold values from -6 to 6
- cotangent: bfloat16 [4096, 1024], P('sp', 'tp'), may hold values from -6 to 6
- lambdas: float32 [8], P('tp'), may hold values from 0.3 to 0.8
- out_gain: float32 [128], replicated, may hold values from 0.1 to 1.9
Outputs:
- query_grad: float32 [4096, 1024], P('sp', 'tp')
- key_grad: float32 [4096, 1024], P('sp', 'tp')
- value_grad: float32 [4096, 1024], P('sp', 'tp')
- weight_grad: float32 [2048, 1024], P('sp', 'tp')
The draws below stay inside these ranges and needn't reach their ends.
Inputs may be any that keep to these rules, and one draw needn't show every extreme that they name: `log_sums`: each entry is the logarithm of the sum of exp(scores_c[t, s]) over s <= t for its row t, head h and map c.
All inputs are finite; a program needn't handle non-finite values.
Results may differ from the reference program's by a relative error of at most 0.008.
Values may be sent and summed in bfloat16 or wider, within the bound.
No kernel may reach another device: no remote copies, remote signals or barrier semaphores. Data moves between devices by JAX's collectives and lax.ppermute only.
A program may use at most 64 MiB of HBM per device.

```python
import jax
import jax.numpy as jnp
from jax import lax

TOK_DEV = 512
D = 2048
HEADS = 8
QK = 64
VALUE = 128
SEQ = 4096


def pair_draw(key):
    arr_shape = (SEQ, HEADS * 2 * QK)
    key_query = jax.random.fold_in(key, 501)
    key_keys = jax.random.fold_in(key, 502)
    query_vals = jnp.clip(1.3 * jax.random.normal(key_query, arr_shape, jnp.float32), -5.5, 5.5)
    key_vals = jnp.clip(1.3 * jax.random.normal(key_keys, arr_shape, jnp.float32), -5.5, 5.5)
    return (query_vals.astype(jnp.bfloat16), key_vals.astype(jnp.bfloat16))


def draw_queries(key, part):
    return pair_draw(key)[0]


def draw_key_vectors(key, part):
    return pair_draw(key)[1]


def draw_log_sums(key, part):
    query_vals, key_vals = pair_draw(key)
    query_wide = query_vals.astype(jnp.float32).reshape(SEQ, HEADS * 2, QK)
    key_wide = key_vals.astype(jnp.float32).reshape(SEQ, HEADS * 2, QK)
    factor = QK ** (-0.5)
    key_pos = jnp.arange(SEQ, dtype=jnp.int32)

    def per_block(block_idx):
        begin_row = (block_idx * TOK_DEV).astype(jnp.int32)
        query_block = lax.dynamic_slice_in_dim(query_wide, begin_row, TOK_DEV, 0)
        query_pos = begin_row + jnp.arange(TOK_DEV, dtype=jnp.int32)
        visible = key_pos[None, :] <= query_pos[:, None]

        def per_map(map_idx):
            query_map = lax.dynamic_index_in_dim(query_block, map_idx, 1, keepdims=False)
            key_map = lax.dynamic_index_in_dim(key_wide, map_idx, 1, keepdims=False)
            scores = jnp.dot(query_map, key_map.T, precision=lax.Precision.HIGHEST) * factor
            masked = jnp.where(visible, scores, -jnp.inf)
            largest = jnp.max(masked, axis=1)
            return largest + jnp.log(jnp.sum(jnp.where(visible, jnp.exp(masked - largest[:, None]), 0.0), axis=1))
        return lax.map(per_map, jnp.arange(HEADS * 2, dtype=jnp.int32)).T
    result = lax.map(per_block, jnp.arange(SEQ // TOK_DEV, dtype=jnp.int32))
    return result.reshape(SEQ, HEADS * 2).astype(jnp.float32)


def with_spikes(values, rng, source, target, parts, factor):
    owner, partner = [(jnp.arange(values.shape[axis_at]) // (values.shape[axis_at] // parts)).reshape([-1 if axis == axis_at else 1 for axis in range(values.ndim)]) for axis_at in (source, target)]
    chosen = jax.random.permutation(rng, parts)[partner]
    strong = (owner == chosen) | (owner == (partner + parts // 2) % parts)
    return jnp.where(strong, factor * values, values)


def levels(own_key, extent, split, low, high):
    factor_of, own = 1.0, jax.random.fold_in(own_key, 6)
    for axis_at, shards_of in split:
        steps = jnp.exp(jax.random.uniform(jax.random.fold_in(own, axis_at), (shards_of,), jnp.float32, low / len(split), high / len(split)))
        factor_of = factor_of * jnp.repeat(steps, extent[axis_at] // shards_of).reshape([-1 if axis == axis_at else 1 for axis in range(len(extent))])
    return factor_of


def scatter_about(key, dims, width, bound, split=(), kind=jnp.bfloat16):
    values = width * jax.random.normal(key, dims, jnp.float32)
    if split:
        values = values * levels(key, dims, split, -0.22, 0.18)
    return jnp.clip(values, -bound, bound).astype(kind)


def gaussian_with(rng, extent, deviation, bound, split, heavy, kind=jnp.bfloat16):
    drawn = deviation * jax.random.normal(rng, extent, jnp.float32)
    if split:
        drawn = drawn * levels(rng, extent, split, -0.22, 0.18)
    return jnp.clip(with_spikes(drawn, jax.random.fold_in(rng, 3), *heavy), -bound, bound).astype(kind)


def setup_inputs(seed: int = 0) -> dict:
    keys = jax.random.split(jax.random.key(seed), 10)
    queries = draw_queries(jax.random.fold_in(keys[9], 71), 0)
    key_vectors = draw_key_vectors(jax.random.fold_in(keys[9], 71), 0)
    latents = scatter_about(keys[2], (SEQ, D), 1.0, 6.0, ((0, 8), (1, 4)))
    w_value = scatter_about(keys[3], (D, HEADS * VALUE), D ** -0.5, 0.125, ((1, 4),))
    log_sums = draw_log_sums(jax.random.fold_in(keys[9], 71), 0)
    out_pair = scatter_about(keys[5], (SEQ, HEADS * 2 * VALUE), 1.0, 6.0, ((0, 8), (1, 4)))
    cotangent = gaussian_with(keys[6], (SEQ, HEADS * VALUE), 1.0, 6.0, ((0, 8), (1, 4)), (0, 1, 8, 2.0))
    lambdas = jnp.clip(0.3 + 0.5 * jax.random.uniform(keys[7], (HEADS,), jnp.float32) ** levels(keys[7], (HEADS,), ((0, 4),), -0.2, 0.2), 0.3, 0.8)
    out_gain = jnp.clip(1.0 + 0.18 * jax.random.normal(keys[8], (VALUE,), jnp.float32), 0.1, 1.9)
    return dict(queries=queries, key_vectors=key_vectors, latents=latents, w_value=w_value, log_sums=log_sums, out_pair=out_pair, cotangent=cotangent, lambdas=lambdas, out_gain=out_gain)


norm_floor = 0.25

def head_cotangent(out_pair, cotangent, lambdas, out_gain):
    tok_rows = out_pair.shape[0]
    head_count = lambdas.shape[0]
    out_maps = out_pair.astype(jnp.float32).reshape(tok_rows, head_count, 2, -1)
    lam_cols = lambdas[None, :, None]
    merged = out_maps[:, :, 0] - lam_cols * out_maps[:, :, 1]
    inv_norm = lax.rsqrt(lax.optimization_barrier(jnp.mean(merged * merged, axis=-1, keepdims=True)) + norm_floor)
    scaled = cotangent.astype(jnp.float32).reshape(merged.shape) * out_gain
    inner_dot = lax.optimization_barrier(jnp.mean(scaled * merged, axis=-1, keepdims=True))
    out_grad = (inv_norm * scaled - merged * (inv_norm * inv_norm * inv_norm) * inner_dot).astype(jnp.bfloat16)
    grad_wide = out_grad.astype(jnp.float32)
    first_map = lax.optimization_barrier(jnp.sum(grad_wide * out_maps[:, :, 0], axis=-1))
    second_map = -lambdas[None, :] * lax.optimization_barrier(jnp.sum(grad_wide * out_maps[:, :, 1], axis=-1))
    return (out_grad, jnp.stack([first_map, second_map], axis=-1))

def block_terms(query_block, key_block, value_block, grad_block, log_block, term_block, lambdas, query_pos, key_pos):
    factor = query_block.shape[-1] ** (-0.5)
    scores = jnp.einsum('qhcd,khcd->hcqk', query_block.astype(jnp.float32), key_block.astype(jnp.float32)) * factor
    visible = key_pos[None, :] <= query_pos[:, None]
    shifted = scores - jnp.transpose(log_block, (1, 2, 0))[..., None]
    softmax_maps = jnp.where(visible, jnp.exp(shifted), 0.0)
    value_dot = jnp.einsum('qhe,khe->hqk', grad_block.astype(jnp.float32), value_block.astype(jnp.float32))
    lam_cols = lambdas[:, None, None]
    weights = (softmax_maps[:, 0] - lam_cols * softmax_maps[:, 1]).astype(jnp.bfloat16)
    term_cols = jnp.transpose(term_block, (1, 2, 0))
    first_map = softmax_maps[:, 0] * (value_dot - term_cols[:, 0, :, None])
    second_map = softmax_maps[:, 1] * (-lam_cols * value_dot - term_cols[:, 1, :, None])
    dscore = (jnp.stack([first_map, second_map], axis=1) * factor).astype(jnp.bfloat16)
    return (weights, dscore)

def reference(queries, key_vectors, latents, w_value, log_sums, out_pair, cotangent, lambdas, out_gain):
    values = jnp.dot(latents, w_value, preferred_element_type=jnp.float32).astype(jnp.bfloat16)
    out_grad, row_terms = head_cotangent(out_pair, cotangent, lambdas, out_gain)
    query_heads = jnp.moveaxis(queries.reshape(SEQ, HEADS, 1, 2, QK), 1, 0)
    key_heads = jnp.moveaxis(key_vectors.reshape(SEQ, HEADS, 1, 2, QK), 1, 0)
    value_heads = jnp.moveaxis(values.reshape(SEQ, HEADS, 1, VALUE), 1, 0)
    grad_heads = jnp.moveaxis(out_grad.reshape(SEQ, HEADS, 1, VALUE), 1, 0)
    log_heads = jnp.moveaxis(log_sums.reshape(SEQ, HEADS, 1, 2), 1, 0)
    term_heads = jnp.moveaxis(row_terms.reshape(SEQ, HEADS, 1, 2), 1, 0)
    lam_heads = lambdas.reshape(HEADS, 1)
    key_pos = jnp.arange(SEQ, dtype=jnp.int32)

    def one_head(inputs):
        query_head, key_head, value_head, grad_head, log_head, term_head, lam_head = inputs

        def one_block(partial_value, block_idx):
            begin_row = (block_idx * TOK_DEV).astype(jnp.int32)
            query_block = lax.dynamic_slice_in_dim(query_head, begin_row, TOK_DEV, 0)
            grad_block = lax.dynamic_slice_in_dim(grad_head, begin_row, TOK_DEV, 0)
            log_block = lax.dynamic_slice_in_dim(log_head, begin_row, TOK_DEV, 0)
            term_block = lax.dynamic_slice_in_dim(term_head, begin_row, TOK_DEV, 0)
            query_pos = begin_row + jnp.arange(TOK_DEV, dtype=jnp.int32)
            weights, dscore = block_terms(query_block, key_head, value_head, grad_block, log_block, term_block, lam_head, query_pos, key_pos)
            score_wide = dscore.astype(jnp.float32)
            query_part = jnp.einsum('hcqk,khcd->qhcd', score_wide, key_head.astype(jnp.float32))
            key_part = jnp.einsum('hcqk,qhcd->khcd', score_wide, query_block.astype(jnp.float32))
            value_part = jnp.einsum('hqk,qhe->khe', weights.astype(jnp.float32), grad_block.astype(jnp.float32))
            return ((partial_value[0] + key_part, partial_value[1] + value_part), query_part)
        start_sums = (jnp.zeros(key_head.shape, jnp.float32), jnp.zeros(value_head.shape, jnp.float32))
        sums, query_parts = lax.scan(one_block, start_sums, jnp.arange(SEQ // TOK_DEV, dtype=jnp.int32))
        return (query_parts.reshape(query_head.shape), sums[0], sums[1])
    query_grad, key_grad, value_grad = lax.map(one_head, (query_heads, key_heads, value_heads, grad_heads, log_heads, term_heads, lam_heads))
    query_grad = jnp.moveaxis(query_grad, 0, 1).reshape(SEQ, HEADS * 2 * QK)
    key_grad = jnp.moveaxis(key_grad, 0, 1).reshape(SEQ, HEADS * 2 * QK)
    value_grad = jnp.moveaxis(value_grad, 0, 1).reshape(SEQ, HEADS * VALUE)
    value_narrow = value_grad.astype(jnp.bfloat16)
    weight_grad = jnp.dot(latents.T, value_narrow, preferred_element_type=jnp.float32)
    return (query_grad, key_grad, value_grad, weight_grad)
```

```python
import jax
import jax.numpy as jnp
from jax import lax
from jax.experimental import pallas as pl
from jax.experimental.pallas import tpu as pltpu
from jax.sharding import PartitionSpec as P

norm_floor = 0.25
block_rows = 512


def head_cotangent(out_pair, cotangent, lambdas, out_gain):
    tok_rows = out_pair.shape[0]
    head_count = lambdas.shape[0]
    out_maps = out_pair.astype(jnp.float32).reshape(tok_rows, head_count, 2, -1)
    lam_cols = lambdas[None, :, None]
    merged = out_maps[:, :, 0] - lam_cols * out_maps[:, :, 1]
    inv_norm = lax.rsqrt(jnp.mean(merged * merged, axis=-1, keepdims=True) + norm_floor)
    scaled = cotangent.astype(jnp.float32).reshape(merged.shape) * out_gain
    inner_dot = jnp.mean(scaled * merged, axis=-1, keepdims=True)
    out_grad = (inv_norm * scaled - merged * (inv_norm * inv_norm * inv_norm) * inner_dot).astype(
        jnp.bfloat16
    )
    grad_wide = out_grad.astype(jnp.float32)
    first_map = jnp.sum(grad_wide * out_maps[:, :, 0], axis=-1)
    second_map = -lambdas[None, :] * jnp.sum(grad_wide * out_maps[:, :, 1], axis=-1)
    return (out_grad, jnp.stack([first_map, second_map], axis=-1))


def block_terms(
    query_block,
    key_block,
    value_block,
    grad_block,
    log_block,
    term_block,
    lambdas,
    query_pos,
    key_pos,
):
    factor = query_block.shape[-1] ** (-0.5)
    scores = (
        jnp.einsum("qhcd,khcd->hcqk", query_block, key_block, preferred_element_type=jnp.float32)
        * factor
    )
    visible = key_pos[None, :] <= query_pos[:, None]
    shifted = scores - jnp.transpose(log_block, (1, 2, 0))[..., None]
    softmax_maps = jnp.where(visible, jnp.exp(shifted), 0.0)
    value_dot = jnp.einsum(
        "qhe,khe->hqk", grad_block, value_block, preferred_element_type=jnp.float32
    )
    lam_cols = lambdas[:, None, None]
    weights = (softmax_maps[:, 0] - lam_cols * softmax_maps[:, 1]).astype(jnp.bfloat16)
    term_cols = jnp.transpose(term_block, (1, 2, 0))
    first_map = softmax_maps[:, 0] * (value_dot - term_cols[:, 0, :, None])
    second_map = softmax_maps[:, 1] * (-lam_cols * value_dot - term_cols[:, 1, :, None])
    dscore = (jnp.stack([first_map, second_map], axis=1) * factor).astype(jnp.bfloat16)
    return (weights, dscore)


def block_span():
    return block_rows


def general_device(
    queries, key_vectors, latents, w_value, log_sums, out_pair, cotangent, lambdas, out_gain
):
    tok_rows = queries.shape[0]
    head_count = lambdas.shape[0]
    offset = lax.axis_index("sp") * tok_rows
    own_pos = offset + jnp.arange(tok_rows, dtype=jnp.int32)
    last_pos = offset + tok_rows - 1
    gathered = lax.all_gather(latents, "tp", axis=1, tiled=True)
    values = jnp.dot(gathered, w_value, preferred_element_type=jnp.float32).astype(jnp.bfloat16)
    out_grad, row_terms = head_cotangent(out_pair, cotangent, lambdas, out_gain)
    query_heads = queries.reshape(tok_rows, head_count, 2, -1)
    key_heads = key_vectors.reshape(tok_rows, head_count, 2, -1)
    value_heads = values.reshape(tok_rows, head_count, -1)
    log_heads = log_sums.reshape(tok_rows, head_count, 2)
    grad_flat = out_grad.reshape(tok_rows, -1)
    term_flat = row_terms.reshape(tok_rows, -1)
    zero_keys = jnp.zeros(key_heads.shape, jnp.float32)
    zero_values = jnp.zeros(value_heads.shape, jnp.float32)
    shards = (
        lax.all_gather(key_vectors, "sp", axis=0, tiled=True),
        lax.all_gather(values, "sp", axis=0, tiled=True),
    )
    key_piece = shards[0]
    value_piece = shards[1]
    piece_rows = key_piece.shape[0]
    block_len = block_span()

    def query_add_block(block_idx, partial_value):
        begin_row = block_idx * block_len
        key_block = lax.dynamic_slice_in_dim(key_piece, begin_row, block_len, 0).reshape(
            block_len, head_count, 2, -1
        )
        value_block = lax.dynamic_slice_in_dim(value_piece, begin_row, block_len, 0).reshape(
            block_len, head_count, -1
        )
        key_pos = begin_row + jnp.arange(block_len, dtype=jnp.int32)

        def query_compute(sums):
            weights, dscore = block_terms(
                query_heads,
                key_block,
                value_block,
                out_grad,
                log_heads,
                row_terms,
                lambdas,
                own_pos,
                key_pos,
            )
            return sums + jnp.einsum(
                "hcqk,khcd->qhcd", dscore, key_block, preferred_element_type=jnp.float32
            )

        return lax.cond(begin_row <= last_pos, query_compute, lambda sums: sums, partial_value)

    query_grad = lax.fori_loop(0, piece_rows // block_len, query_add_block, zero_keys)
    shards = (
        lax.all_gather(queries.astype(jnp.float32), "sp", axis=0, tiled=True).astype(jnp.bfloat16),
        lax.all_gather(grad_flat.astype(jnp.float32), "sp", axis=0, tiled=True).astype(
            jnp.bfloat16
        ),
        lax.all_gather(log_sums, "sp", axis=0, tiled=True),
        lax.all_gather(term_flat, "sp", axis=0, tiled=True),
    )
    query_piece = shards[0]
    grad_piece = shards[1]
    log_piece = shards[2]
    term_piece = shards[3]
    piece_rows = query_piece.shape[0]
    key_block_len = block_span()

    def key_add_block(block_idx, partial_value):
        begin_row = block_idx * key_block_len
        query_block = lax.dynamic_slice_in_dim(query_piece, begin_row, key_block_len, 0).reshape(
            key_block_len, head_count, 2, -1
        )
        grad_block = lax.dynamic_slice_in_dim(grad_piece, begin_row, key_block_len, 0).reshape(
            key_block_len, head_count, -1
        )
        log_block = lax.dynamic_slice_in_dim(log_piece, begin_row, key_block_len, 0).reshape(
            key_block_len, head_count, 2
        )
        term_block = lax.dynamic_slice_in_dim(term_piece, begin_row, key_block_len, 0).reshape(
            key_block_len, head_count, 2
        )
        query_pos = begin_row + jnp.arange(key_block_len, dtype=jnp.int32)

        def key_compute(sums):
            weights, dscore = block_terms(
                query_block,
                key_heads,
                value_heads,
                grad_block,
                log_block,
                term_block,
                lambdas,
                query_pos,
                own_pos,
            )
            key_sum = sums[0] + jnp.einsum(
                "hcqk,qhcd->khcd", dscore, query_block, preferred_element_type=jnp.float32
            )
            value_sum = sums[1] + jnp.einsum(
                "hqk,qhe->khe", weights, grad_block, preferred_element_type=jnp.float32
            )
            return (key_sum, value_sum)

        return lax.cond(
            begin_row + key_block_len - 1 >= offset, key_compute, lambda sums: sums, partial_value
        )

    key_grad, value_grad = lax.fori_loop(
        0, piece_rows // key_block_len, key_add_block, (zero_keys, zero_values)
    )
    value_flat = value_grad.reshape(tok_rows, -1)
    value_narrow = value_flat.astype(jnp.bfloat16)
    weight_grad = lax.psum_scatter(
        lax.dot_general(
            gathered, value_narrow, (((0,), (0,)), ((), ())), preferred_element_type=jnp.float32
        ),
        "sp",
        scatter_dimension=0,
        tiled=True,
    )
    return (
        query_grad.reshape(tok_rows, -1),
        key_grad.reshape(tok_rows, -1),
        value_flat,
        weight_grad,
    )


LOG2E = 1.4426950408889634
AUX_ROWS = 32
SLOTS = 10
CHUNK = 128
LANES = 128


def nt(a, b):
    return lax.dot_general(a, b, (((1,), (1,)), ((), ())), preferred_element_type=jnp.float32)


def tn(a, b):
    return lax.dot_general(a, b, (((0,), (0,)), ((), ())), preferred_element_type=jnp.float32)


def level_bits():
    place = lax.axis_index("sp")
    return place % 2, (place // 2) % 2, (place // 4) % 2


def split_pieces(rows):
    high = rows.astype(jnp.bfloat16)
    rest = rows - high.astype(jnp.float32)
    middle = rest.astype(jnp.bfloat16)
    low = (rest - middle.astype(jnp.float32)).astype(jnp.bfloat16)
    return high, middle, low


def prep_kernel(q_ref, k_ref, log_ref, pair_ref, cot_ref, lam_ref, gain_ref, grad_ref, aux_ref, px_ref, pz_ref, pm_ref):
    rows = q_ref.shape[0]
    half = rows // 2
    bit0, bit1, bit2 = level_bits()
    lane = lax.broadcasted_iota(jnp.int32, (rows, LANES), 1)
    aux_blocks = []
    for h in range(2):
        first = pair_ref[:, 2 * h * LANES : (2 * h + 1) * LANES].astype(jnp.float32)
        second = pair_ref[:, (2 * h + 1) * LANES : (2 * h + 2) * LANES].astype(jnp.float32)
        lam = lam_ref[h]
        merged = first - lam * second
        inv = lax.rsqrt(jnp.mean(merged * merged, axis=-1, keepdims=True) + norm_floor)
        scaled = cot_ref[:, h * LANES : (h + 1) * LANES].astype(jnp.float32) * gain_ref[...]
        inner = jnp.mean(scaled * merged, axis=-1, keepdims=True)
        grad = (inv * scaled - merged * (inv * inv * inv) * inner).astype(jnp.bfloat16)
        grad_ref[:, h * LANES : (h + 1) * LANES] = grad
        wide = grad.astype(jnp.float32)
        term0 = jnp.sum(wide * first, axis=-1, keepdims=True)
        term1 = jnp.sum(wide * second, axis=-1, keepdims=True)
        terms = jnp.where(lane == 2, term0, jnp.where(lane == 3, term1, 0.0))
        turned = jnp.concatenate(
            [jnp.transpose(terms[i * LANES : (i + 1) * LANES])[0:8] for i in range(rows // LANES)], axis=1
        )
        log0 = log_ref[2 * h : 2 * h + 1, :] * LOG2E
        log1 = (log_ref[2 * h + 1 : 2 * h + 2, :] - jnp.log(jnp.full((1, rows), lam, jnp.float32))) * LOG2E
        aux = jnp.concatenate([log0, log1, turned[2:4], jnp.zeros((4, rows), jnp.float32)], axis=0)
        aux_ref[h * 8 : (h + 1) * 8, :] = aux
        pieces = split_pieces(aux)
        wide_rows = jnp.concatenate([p.astype(jnp.float32)[0:4] for p in pieces] + [jnp.zeros((4, rows), jnp.float32)], axis=0)
        aux_blocks.append(wide_rows.astype(jnp.bfloat16))

    def put(ref, lane0, early, head_k, head_q):

        @pl.when(early)
        def _():
            ref[0:rows, lane0 : lane0 + LANES] = k_ref[:, head_k * LANES : (head_k + 1) * LANES]
            ref[0:rows, lane0 + LANES : lane0 + 2 * LANES] = k_ref[:, head_k * LANES : (head_k + 1) * LANES]

        @pl.when(jnp.logical_not(early))
        def _():
            ref[0:rows, lane0 : lane0 + LANES] = q_ref[:, head_q * LANES : (head_q + 1) * LANES]
            ref[0:rows, lane0 + LANES : lane0 + 2 * LANES] = grad_ref[:, head_q * LANES : (head_q + 1) * LANES]

    def put_aux(ref, lane0, h):
        ref[rows : rows + 16, lane0 : lane0 + half] = aux_blocks[h][:, 0:half]
        ref[rows + 16 : rows + 32, lane0 : lane0 + half] = aux_blocks[h][:, half:rows]

    put(px_ref, 0, bit0 == 0, 1, 0)
    px_ref[0:rows, 2 * LANES : 3 * LANES] = q_ref[:, LANES : 2 * LANES]
    px_ref[0:rows, 3 * LANES : 4 * LANES] = grad_ref[:, LANES : 2 * LANES]
    px_ref[0:rows, 4 * LANES : 5 * LANES] = k_ref[:, 0:LANES]
    px_ref[rows : rows + 32, 4 * LANES : 5 * LANES] = jnp.zeros((32, LANES), jnp.bfloat16)
    put_aux(px_ref, 0, 0)
    put_aux(px_ref, half, 1)
    put(pz_ref, 0, bit1 == 0, 1, 0)
    put_aux(pz_ref, 0, 0)
    put(pm_ref, 0, bit2 == 0, 1, 0)
    put_aux(pm_ref, 0, 0)


def value_kernel(own_ref, far_ref, near_ref, w_ref, out_ref):
    cols = own_ref.shape[1]
    place = lax.axis_index("tp")

    def part(x, spot):
        return jnp.dot(x, w_ref[pl.ds(spot * cols, cols), :], preferred_element_type=jnp.float32)

    total = part(own_ref[...], place) + part(far_ref[...], (place + 2) % 4)
    near = place + 1 - 2 * (place % 2)
    total += part(near_ref[:, 0:cols], near) + part(near_ref[:, cols : 2 * cols], (near + 2) % 4)
    out_ref[...] = total.astype(jnp.bfloat16)


def weight_kernel(own_ref, far_ref, near_ref, grad_ref, out_ref):
    cols = own_ref.shape[1]
    place = lax.axis_index("tp")
    near = place + 1 - 2 * (place % 2)
    grad = grad_ref[...]
    out_ref[pl.ds(place * cols, cols), :] = tn(own_ref[...], grad).astype(jnp.bfloat16)
    out_ref[pl.ds(((place + 2) % 4) * cols, cols), :] = tn(far_ref[...], grad).astype(jnp.bfloat16)
    out_ref[pl.ds(near * cols, cols), :] = tn(near_ref[:, 0:cols], grad).astype(jnp.bfloat16)
    out_ref[pl.ds(((near + 2) % 4) * cols, cols), :] = tn(near_ref[:, cols : 2 * cols], grad).astype(jnp.bfloat16)


def join_pieces(block_ref, rows, lane0):
    half = rows // 2
    parts = [block_ref[rows + 16 * i : rows + 16 * (i + 1), lane0 : lane0 + half].astype(jnp.float32) for i in range(2)]
    sums = [p[0:4] + p[4:8] + p[8:12] for p in parts]
    return jnp.concatenate(sums, axis=1)


def main_kernel(
    q_ref, k_ref, v_ref, grad_ref, aux_ref, rx_ref, rz_ref, r4_ref, r6_ref, vx_ref, vz_ref, v4_ref, v6_ref,
    d1_ref, d2_ref, tx_ref, tz_ref, t4_ref, t6_ref, a_ref, b_ref, aux_all, s1_ref, s2_ref,
):
    rows = q_ref.shape[0]
    bits = level_bits()
    lane = lax.broadcasted_iota(jnp.int32, (1, LANES), 1)
    left = lane < LANES // 2
    for h in range(2):
        a_ref[h] = q_ref[:, h * LANES : (h + 1) * LANES]
        b_ref[h] = grad_ref[:, h * LANES : (h + 1) * LANES]
        a_ref[2 + h] = k_ref[:, h * LANES : (h + 1) * LANES]
        b_ref[2 + h] = v_ref[:, h * LANES : (h + 1) * LANES]
        aux_all[h, 0:4, :] = aux_ref[8 * h : 8 * h + 4, :]
    for slot, ref, vref, bit, vlane in (
        (4, rx_ref, vx_ref, bits[0], LANES), (5, rz_ref, vz_ref, bits[1], 0), (6, r4_ref, v4_ref, bits[2], 0), (7, r6_ref, v6_ref, bits[2], 0),
    ):
        a_ref[slot] = ref[0:rows, 0:LANES]
        aux_all[slot, 0:4, :] = join_pieces(ref, rows, 0)

        @pl.when(bit == 0)
        def _(slot=slot, ref=ref):
            b_ref[slot] = ref[0:rows, LANES : 2 * LANES]

        @pl.when(bit != 0)
        def _(slot=slot, vref=vref, vlane=vlane):
            b_ref[slot] = vref[:, vlane : vlane + LANES]

    a_ref[9] = rx_ref[0:rows, 2 * LANES : 3 * LANES]
    b_ref[9] = rx_ref[0:rows, 3 * LANES : 4 * LANES]
    aux_all[9, 0:4, :] = join_pieces(rx_ref, rows, rows // 2)
    a_ref[8] = rx_ref[0:rows, 4 * LANES : 5 * LANES]
    b_ref[8] = vx_ref[:, 0:LANES]
    s1_ref[...] = jnp.zeros(s1_ref.shape, jnp.float32)
    s2_ref[...] = jnp.zeros(s2_ref.shape, jnp.float32)
    scale = LOG2E / 8.0

    def halves(x):
        return jnp.where(left, x, jnp.zeros((), x.dtype)), jnp.where(left, jnp.zeros((), x.dtype), x)

    def unit(qs, ks, masked):
        query0, query1 = halves(a_ref[qs])
        grad = b_ref[qs]
        aux = aux_all[qs]
        for c in range(rows // CHUNK):
            low = c * CHUNK
            first = low if masked else 0
            width = rows - first
            key = a_ref[ks, low : low + CHUNK, :]
            key0, key1 = halves(key)
            value = b_ref[ks, low : low + CHUNK, :]
            map0 = jnp.exp2(nt(key, query0[first:]) * scale - aux[0:1, first:])
            map1 = jnp.exp2(nt(key, query1[first:]) * scale - aux[1:2, first:])
            if masked:
                key_pos = lax.broadcasted_iota(jnp.int32, (CHUNK, width), 0)
                query_pos = lax.broadcasted_iota(jnp.int32, (CHUNK, width), 1)
                seen = key_pos <= query_pos
                map0 = jnp.where(seen, map0, 0.0)
                map1 = jnp.where(seen, map1, 0.0)
            dots = nt(value, grad[first:])
            mixed = (map0 - map1).astype(jnp.bfloat16)
            score0 = (map0 * (dots - aux[2:3, first:])).astype(jnp.bfloat16)
            score1 = (map1 * (aux[3:4, first:] - dots)).astype(jnp.bfloat16)
            s2_ref[ks, low : low + CHUNK, :] += jnp.dot(mixed, grad[first:], preferred_element_type=jnp.float32)
            s1_ref[ks, low : low + CHUNK, :] += jnp.dot(score0, query0[first:], preferred_element_type=jnp.float32) + jnp.dot(
                score1, query1[first:], preferred_element_type=jnp.float32
            )
            turned = tn(key0, score0) + tn(key1, score1)
            for i in range(width // LANES):
                s1_ref[qs, first + i * LANES : first + (i + 1) * LANES, :] += turned[:, i * LANES : (i + 1) * LANES]

    def own_unit(h, carry):
        unit(h, 2 + h, True)
        return carry

    lax.fori_loop(0, 2, own_unit, 0)

    def full_unit(u, carry):
        level = jnp.where(u == 0, 0, jnp.where(u < 3, 1, 2))
        bit = jnp.where(level == 0, bits[0], jnp.where(level == 1, bits[1], bits[2]))
        other = 4 + (u + 1) // 2
        own = (u == 0) | (u % 2 == 1)
        unit(jnp.where(bit == 0, other, jnp.where(own, 1, 9)), jnp.where(bit == 0, jnp.where(own, 2, 8), other), False)
        return carry

    lax.fori_loop(0, 7, full_unit, 0)
    d1_ref[...] = s1_ref[0:4]
    d2_ref[...] = s2_ref[2:4]
    for ref, slot in ((tx_ref, 4), (tz_ref, 5), (t4_ref, 6), (t6_ref, 7)):
        ref[:, 0:LANES] = s1_ref[slot].astype(jnp.bfloat16)
        ref[:, LANES : 2 * LANES] = s2_ref[slot].astype(jnp.bfloat16)
    tx_ref[:, 2 * LANES : 3 * LANES] = s1_ref[8].astype(jnp.bfloat16)
    tx_ref[:, 3 * LANES : 4 * LANES] = s2_ref[8].astype(jnp.bfloat16)
    tx_ref[:, 4 * LANES : 5 * LANES] = s1_ref[9].astype(jnp.bfloat16)


def join_kernel(d1_ref, d2_ref, ux_ref, uz_ref, u4_ref, u6_ref, dq_ref, dk_ref, dv_ref, narrow_ref, s_ref):
    bits = level_bits()
    for i in range(4):
        s_ref[i] = d1_ref[i]
    for i in range(2):
        s_ref[4 + i] = d2_ref[i]
    s_ref[2] += ux_ref[:, 2 * LANES : 3 * LANES].astype(jnp.float32)
    s_ref[4] += ux_ref[:, 3 * LANES : 4 * LANES].astype(jnp.float32)
    s_ref[1] += ux_ref[:, 4 * LANES : 5 * LANES].astype(jnp.float32)
    for ref, bit in ((ux_ref, bits[0]), (uz_ref, bits[1]), (u4_ref, bits[2]), (u6_ref, bits[2])):

        @pl.when(bit == 0)
        def _(ref=ref):
            s_ref[3] += ref[:, 0:LANES].astype(jnp.float32)
            s_ref[5] += ref[:, LANES : 2 * LANES].astype(jnp.float32)

        @pl.when(bit != 0)
        def _(ref=ref):
            s_ref[0] += ref[:, 0:LANES].astype(jnp.float32)

    for h in range(2):
        for i in range(s_ref.shape[1] // LANES):
            spot = slice(i * LANES, (i + 1) * LANES)
            dq_ref[spot, h * LANES : (h + 1) * LANES] = jnp.transpose(s_ref[h, spot, :]) * 0.125
        dk_ref[:, h * LANES : (h + 1) * LANES] = s_ref[2 + h] * 0.125
        dv_ref[:, h * LANES : (h + 1) * LANES] = s_ref[4 + h]
        narrow_ref[:, h * LANES : (h + 1) * LANES] = s_ref[4 + h].astype(jnp.bfloat16)


def call(kernel, outs, args, scratch=(), smem=(), name=None):
    vmem = pl.BlockSpec(memory_space=pltpu.VMEM)
    specs = [pl.BlockSpec(memory_space=pltpu.SMEM) if i in smem else vmem for i in range(len(args))]
    return pl.pallas_call(
        kernel,
        out_shape=[jax.ShapeDtypeStruct(s, d) for s, d in outs],
        in_specs=specs,
        out_specs=[vmem] * len(outs),
        scratch_shapes=list(scratch),
        name=name,
    )(*args)


def swap(x, axis, size, mask):
    return lax.ppermute(x, axis, [(i, i ^ mask) for i in range(size)])


def paired_device(queries, key_vectors, latents, w_value, log_sums, out_pair, cotangent, lambdas, out_gain):
    rows, width = queries.shape
    narrow, wide = jnp.bfloat16, jnp.float32
    seq, feat = lax.axis_size("sp"), lax.axis_size("tp")
    far = swap(latents, "tp", feat, 2)
    grad, aux, px, pz, pm = call(
        prep_kernel,
        [((rows, width), narrow), ((16, rows), wide), ((rows + AUX_ROWS, 5 * LANES), narrow),
         ((rows + AUX_ROWS, width), narrow), ((rows + AUX_ROWS, width), narrow)],
        (queries, key_vectors, log_sums.T, out_pair, cotangent, lambdas, out_gain[None, :]),
        smem=(5,), name="prep",
    )
    r4 = swap(pm, "sp", seq, 4)
    r6 = swap(pm, "sp", seq, 6)
    rz = swap(pz, "sp", seq, 2)
    rx = swap(px, "sp", seq, 1)
    near = swap(jnp.concatenate([latents, far], axis=1), "tp", feat, 1)
    values, = call(value_kernel, [((rows, width), narrow)], (latents, far, near, w_value), name="values")
    second = values[:, LANES:]
    v4 = swap(second, "sp", seq, 4)
    v6 = swap(second, "sp", seq, 6)
    vz = swap(second, "sp", seq, 2)
    vx = swap(values, "sp", seq, 1)
    slot_shape = (rows, LANES)
    d1, d2, tx, tz, t4, t6 = call(
        main_kernel,
        [((4,) + slot_shape, wide), ((2,) + slot_shape, wide), ((rows, 5 * LANES), narrow)] + [((rows, width), narrow)] * 3,
        (queries, key_vectors, values, grad, aux, rx, rz, r4, r6, vx, vz, v4, v6),
        scratch=[pltpu.VMEM((SLOTS,) + slot_shape, narrow), pltpu.VMEM((SLOTS,) + slot_shape, narrow),
                 pltpu.VMEM((SLOTS, 8, rows), wide), pltpu.VMEM((SLOTS,) + slot_shape, wide), pltpu.VMEM((SLOTS,) + slot_shape, wide)],
        name="blocks",
    )
    u4 = swap(t4, "sp", seq, 4)
    u6 = swap(t6, "sp", seq, 6)
    uz = swap(tz, "sp", seq, 2)
    ux = swap(tx, "sp", seq, 1)
    dq, dk, dv, dv_narrow = call(
        join_kernel,
        [((rows, width), wide)] * 3 + [((rows, width), narrow)],
        (d1, d2, ux, uz, u4, u6),
        scratch=[pltpu.VMEM((6,) + slot_shape, wide)],
        name="join",
    )
    part, = call(weight_kernel, [((latents.shape[1] * feat, width), narrow)], (latents, far, near, dv_narrow), name="weight")
    pieces = lax.all_to_all(part.reshape(seq, -1, width), "sp", 0, 0)
    return dq, dk, dv, jnp.sum(pieces.astype(wide), axis=0)


def solution(mesh):
    plan = paired_device if (mesh.shape["sp"], mesh.shape["tp"]) == (8, 4) else general_device
    return jax.shard_map(
        plan,
        mesh=mesh,
        in_specs=(
            P("sp", "tp"),
            P("sp", "tp"),
            P("sp", "tp"),
            P(None, "tp"),
            P("sp", "tp"),
            P("sp", "tp"),
            P("sp", "tp"),
            P("tp"),
            P(),
        ),
        out_specs=(P("sp", "tp"), P("sp", "tp"), P("sp", "tp"), P("sp", "tp")),
        check_vma=False,
    )
```

```python
import jax
import jax.numpy as jnp
from jax import lax
from jax.experimental import pallas as pl
from jax.experimental.pallas import tpu as pltpu
from jax.sharding import PartitionSpec as P


norm_floor = 0.25
block_rows = 512


def head_cotangent(out_pair, cotangent, lambdas, out_gain):
    tok_rows = out_pair.shape[0]
    head_count = lambdas.shape[0]
    out_maps = out_pair.astype(jnp.float32).reshape(tok_rows, head_count, 2, -1)
    lam_cols = lambdas[None, :, None]
    merged = out_maps[:, :, 0] - lam_cols * out_maps[:, :, 1]
    inv_norm = lax.rsqrt(jnp.mean(merged * merged, axis=-1, keepdims=True) + norm_floor)
    scaled = cotangent.astype(jnp.float32).reshape(merged.shape) * out_gain
    inner_dot = jnp.mean(scaled * merged, axis=-1, keepdims=True)
    out_grad = (inv_norm * scaled - merged * (inv_norm * inv_norm * inv_norm) * inner_dot).astype(
        jnp.bfloat16
    )
    grad_wide = out_grad.astype(jnp.float32)
    first_map = jnp.sum(grad_wide * out_maps[:, :, 0], axis=-1)
    second_map = -lambdas[None, :] * jnp.sum(grad_wide * out_maps[:, :, 1], axis=-1)
    return (out_grad, jnp.stack([first_map, second_map], axis=-1))


def block_terms(
    query_block,
    key_block,
    value_block,
    grad_block,
    log_block,
    term_block,
    lambdas,
    query_pos,
    key_pos,
):
    factor = query_block.shape[-1] ** (-0.5)
    scores = (
        jnp.einsum("qhcd,khcd->hcqk", query_block, key_block, preferred_element_type=jnp.float32)
        * factor
    )
    visible = key_pos[None, :] <= query_pos[:, None]
    shifted = scores - jnp.transpose(log_block, (1, 2, 0))[..., None]
    softmax_maps = jnp.where(visible, jnp.exp(shifted), 0.0)
    value_dot = jnp.einsum(
        "qhe,khe->hqk", grad_block, value_block, preferred_element_type=jnp.float32
    )
    lam_cols = lambdas[:, None, None]
    weights = (softmax_maps[:, 0] - lam_cols * softmax_maps[:, 1]).astype(jnp.bfloat16)
    term_cols = jnp.transpose(term_block, (1, 2, 0))
    first_map = softmax_maps[:, 0] * (value_dot - term_cols[:, 0, :, None])
    second_map = softmax_maps[:, 1] * (-lam_cols * value_dot - term_cols[:, 1, :, None])
    dscore = (jnp.stack([first_map, second_map], axis=1) * factor).astype(jnp.bfloat16)
    return (weights, dscore)


def block_span():
    return block_rows


def general_device(
    queries, key_vectors, latents, w_value, log_sums, out_pair, cotangent, lambdas, out_gain
):
    tok_rows = queries.shape[0]
    head_count = lambdas.shape[0]
    offset = lax.axis_index("sp") * tok_rows
    own_pos = offset + jnp.arange(tok_rows, dtype=jnp.int32)
    last_pos = offset + tok_rows - 1
    gathered = lax.all_gather(latents, "tp", axis=1, tiled=True)
    values = jnp.dot(gathered, w_value, preferred_element_type=jnp.float32).astype(jnp.bfloat16)
    out_grad, row_terms = head_cotangent(out_pair, cotangent, lambdas, out_gain)
    query_heads = queries.reshape(tok_rows, head_count, 2, -1)
    key_heads = key_vectors.reshape(tok_rows, head_count, 2, -1)
    value_heads = values.reshape(tok_rows, head_count, -1)
    log_heads = log_sums.reshape(tok_rows, head_count, 2)
    grad_flat = out_grad.reshape(tok_rows, -1)
    term_flat = row_terms.reshape(tok_rows, -1)
    zero_keys = jnp.zeros(key_heads.shape, jnp.float32)
    zero_values = jnp.zeros(value_heads.shape, jnp.float32)
    shards = (
        lax.all_gather(key_vectors, "sp", axis=0, tiled=True),
        lax.all_gather(values, "sp", axis=0, tiled=True),
    )
    key_piece = shards[0]
    value_piece = shards[1]
    piece_rows = key_piece.shape[0]
    block_len = block_span()

    def query_add_block(block_idx, partial_value):
        begin_row = block_idx * block_len
        key_block = lax.dynamic_slice_in_dim(key_piece, begin_row, block_len, 0).reshape(
            block_len, head_count, 2, -1
        )
        value_block = lax.dynamic_slice_in_dim(value_piece, begin_row, block_len, 0).reshape(
            block_len, head_count, -1
        )
        key_pos = begin_row + jnp.arange(block_len, dtype=jnp.int32)

        def query_compute(sums):
            _, dscore = block_terms(
                query_heads,
                key_block,
                value_block,
                out_grad,
                log_heads,
                row_terms,
                lambdas,
                own_pos,
                key_pos,
            )
            return sums + jnp.einsum(
                "hcqk,khcd->qhcd", dscore, key_block, preferred_element_type=jnp.float32
            )

        return lax.cond(begin_row <= last_pos, query_compute, lambda sums: sums, partial_value)

    query_grad = lax.fori_loop(0, piece_rows // block_len, query_add_block, zero_keys)
    shards = (
        lax.all_gather(queries.astype(jnp.float32), "sp", axis=0, tiled=True).astype(jnp.bfloat16),
        lax.all_gather(grad_flat.astype(jnp.float32), "sp", axis=0, tiled=True).astype(
            jnp.bfloat16
        ),
        lax.all_gather(log_sums, "sp", axis=0, tiled=True),
        lax.all_gather(term_flat, "sp", axis=0, tiled=True),
    )
    query_piece = shards[0]
    grad_piece = shards[1]
    log_piece = shards[2]
    term_piece = shards[3]
    piece_rows = query_piece.shape[0]
    key_block_len = block_span()

    def key_add_block(block_idx, partial_value):
        begin_row = block_idx * key_block_len
        query_block = lax.dynamic_slice_in_dim(query_piece, begin_row, key_block_len, 0).reshape(
            key_block_len, head_count, 2, -1
        )
        grad_block = lax.dynamic_slice_in_dim(grad_piece, begin_row, key_block_len, 0).reshape(
            key_block_len, head_count, -1
        )
        log_block = lax.dynamic_slice_in_dim(log_piece, begin_row, key_block_len, 0).reshape(
            key_block_len, head_count, 2
        )
        term_block = lax.dynamic_slice_in_dim(term_piece, begin_row, key_block_len, 0).reshape(
            key_block_len, head_count, 2
        )
        query_pos = begin_row + jnp.arange(key_block_len, dtype=jnp.int32)

        def key_compute(sums):
            weights, dscore = block_terms(
                query_block,
                key_heads,
                value_heads,
                grad_block,
                log_block,
                term_block,
                lambdas,
                query_pos,
                own_pos,
            )
            key_sum = sums[0] + jnp.einsum(
                "hcqk,qhcd->khcd", dscore, query_block, preferred_element_type=jnp.float32
            )
            value_sum = sums[1] + jnp.einsum(
                "hqk,qhe->khe", weights, grad_block, preferred_element_type=jnp.float32
            )
            return (key_sum, value_sum)

        return lax.cond(
            begin_row + key_block_len - 1 >= offset, key_compute, lambda sums: sums, partial_value
        )

    key_grad, value_grad = lax.fori_loop(
        0, piece_rows // key_block_len, key_add_block, (zero_keys, zero_values)
    )
    value_flat = value_grad.reshape(tok_rows, -1)
    value_narrow = value_flat.astype(jnp.bfloat16)
    weight_grad = lax.psum_scatter(
        lax.dot_general(
            gathered, value_narrow, (((0,), (0,)), ((), ())), preferred_element_type=jnp.float32
        ),
        "sp",
        scatter_dimension=0,
        tiled=True,
    )
    return (
        query_grad.reshape(tok_rows, -1),
        key_grad.reshape(tok_rows, -1),
        value_flat,
        weight_grad,
    )


LOG2E = 1.4426950408889634
AUX_ROWS = 32
SLOTS = 10
CHUNK = 128
LANES = 128


def nt(a, b):
    return lax.dot_general(a, b, (((1,), (1,)), ((), ())), preferred_element_type=jnp.float32)


def tn(a, b):
    return lax.dot_general(a, b, (((0,), (0,)), ((), ())), preferred_element_type=jnp.float32)


def level_bits():
    place = lax.axis_index("sp")
    return place % 2, (place // 2) % 2, (place // 4) % 2


def split_pieces(rows):
    high = rows.astype(jnp.bfloat16)
    rest = rows - high.astype(jnp.float32)
    middle = rest.astype(jnp.bfloat16)
    low = (rest - middle.astype(jnp.float32)).astype(jnp.bfloat16)
    return high, middle, low


def prep_kernel(q_ref, k_ref, log_ref, pair_ref, cot_ref, lam_ref, gain_ref, grad_ref, aux_ref, px_ref, pz_ref, pm_ref):
    rows = q_ref.shape[0]
    half = rows // 2
    bit0, bit1, bit2 = level_bits()
    lane = lax.broadcasted_iota(jnp.int32, (rows, LANES), 1)
    aux_blocks = []
    for h in range(2):
        first = pair_ref[:, 2 * h * LANES : (2 * h + 1) * LANES].astype(jnp.float32)
        second = pair_ref[:, (2 * h + 1) * LANES : (2 * h + 2) * LANES].astype(jnp.float32)
        lam = lam_ref[h]
        merged = first - lam * second
        inv = lax.rsqrt(jnp.mean(merged * merged, axis=-1, keepdims=True) + norm_floor)
        scaled = cot_ref[:, h * LANES : (h + 1) * LANES].astype(jnp.float32) * gain_ref[...]
        inner = jnp.mean(scaled * merged, axis=-1, keepdims=True)
        grad = (inv * scaled - merged * (inv * inv * inv) * inner).astype(jnp.bfloat16)
        grad_ref[:, h * LANES : (h + 1) * LANES] = grad
        wide = grad.astype(jnp.float32)
        term0 = jnp.sum(wide * first, axis=-1, keepdims=True)
        term1 = jnp.sum(wide * second, axis=-1, keepdims=True)
        terms = jnp.where(lane == 2, term0, jnp.where(lane == 3, term1, 0.0))
        turned = jnp.concatenate(
            [jnp.transpose(terms[i * LANES : (i + 1) * LANES])[0:8] for i in range(rows // LANES)], axis=1
        )
        log0 = log_ref[2 * h : 2 * h + 1, :] * LOG2E
        log1 = (log_ref[2 * h + 1 : 2 * h + 2, :] - jnp.log(jnp.full((1, rows), lam, jnp.float32))) * LOG2E
        aux = jnp.concatenate([log0, log1, turned[2:4], jnp.zeros((4, rows), jnp.float32)], axis=0)
        aux_ref[h * 8 : (h + 1) * 8, :] = aux
        pieces = split_pieces(aux)
        wide_rows = jnp.concatenate([p.astype(jnp.float32)[0:4] for p in pieces] + [jnp.zeros((4, rows), jnp.float32)], axis=0)
        aux_blocks.append(wide_rows.astype(jnp.bfloat16))

    def put(ref, lane0, early, head_k, head_q):

        @pl.when(early)
        def _():
            ref[0:rows, lane0 : lane0 + LANES] = k_ref[:, head_k * LANES : (head_k + 1) * LANES]
            ref[0:rows, lane0 + LANES : lane0 + 2 * LANES] = k_ref[:, head_k * LANES : (head_k + 1) * LANES]

        @pl.when(jnp.logical_not(early))
        def _():
            ref[0:rows, lane0 : lane0 + LANES] = q_ref[:, head_q * LANES : (head_q + 1) * LANES]
            ref[0:rows, lane0 + LANES : lane0 + 2 * LANES] = grad_ref[:, head_q * LANES : (head_q + 1) * LANES]

    def put_aux(ref, lane0, h):
        ref[rows : rows + 16, lane0 : lane0 + half] = aux_blocks[h][:, 0:half]
        ref[rows + 16 : rows + 32, lane0 : lane0 + half] = aux_blocks[h][:, half:rows]

    put(px_ref, 0, bit0 == 0, 1, 0)
    px_ref[0:rows, 2 * LANES : 3 * LANES] = q_ref[:, LANES : 2 * LANES]
    px_ref[0:rows, 3 * LANES : 4 * LANES] = grad_ref[:, LANES : 2 * LANES]
    px_ref[0:rows, 4 * LANES : 5 * LANES] = k_ref[:, 0:LANES]
    px_ref[rows : rows + 32, 4 * LANES : 5 * LANES] = jnp.zeros((32, LANES), jnp.bfloat16)
    put_aux(px_ref, 0, 0)
    put_aux(px_ref, half, 1)
    put(pz_ref, 0, bit1 == 0, 1, 0)
    put_aux(pz_ref, 0, 0)
    put(pm_ref, 0, bit2 == 0, 1, 0)
    put_aux(pm_ref, 0, 0)


def value_kernel(own_ref, far_ref, near_ref, next_ref, w_ref, out_ref, second_ref):
    cols = own_ref.shape[1]
    place = lax.axis_index("tp")

    def part(x, spot):
        return jnp.dot(x, w_ref[pl.ds(spot * cols, cols), :], preferred_element_type=jnp.float32)

    total = part(own_ref[...], place) + part(far_ref[...], (place + 2) % 4)
    near = place + 1 - 2 * (place % 2)
    total += part(near_ref[...], near) + part(next_ref[...], (near + 2) % 4)
    out_ref[...] = total.astype(jnp.bfloat16)
    second_ref[...] = total[:, LANES : 2 * LANES].astype(jnp.bfloat16)


def weight_kernel(own_ref, far_ref, near_ref, next_ref, dv0_ref, ux_ref, uz_ref, u4_ref, u6_ref, out_ref, dv_ref, narrow_ref):
    bits = level_bits()
    cols = own_ref.shape[1]
    place = lax.axis_index("tp")
    near = place + 1 - 2 * (place % 2)
    dv_ref[:, 0:LANES] = dv0_ref[0] + ux_ref[:, 0:LANES].astype(jnp.float32)
    dv_ref[:, LANES : 2 * LANES] = dv0_ref[1]
    for ref, lane0, bit in ((ux_ref, LANES, bits[0]), (uz_ref, 0, bits[1]), (u4_ref, 0, bits[2]), (u6_ref, 0, bits[2])):

        @pl.when(bit == 0)
        def _(ref=ref, lane0=lane0):
            dv_ref[:, LANES : 2 * LANES] += ref[:, lane0 : lane0 + LANES].astype(jnp.float32)

    narrow_ref[...] = dv_ref[...].astype(jnp.bfloat16)
    grad = narrow_ref[...]
    out_ref[pl.ds(place * cols, cols), :] = tn(own_ref[...], grad).astype(jnp.bfloat16)
    out_ref[pl.ds(((place + 2) % 4) * cols, cols), :] = tn(far_ref[...], grad).astype(jnp.bfloat16)
    out_ref[pl.ds(near * cols, cols), :] = tn(near_ref[...], grad).astype(jnp.bfloat16)
    out_ref[pl.ds(((near + 2) % 4) * cols, cols), :] = tn(next_ref[...], grad).astype(jnp.bfloat16)


def join_pieces(block_ref, rows, lane0):
    half = rows // 2
    parts = [block_ref[rows + 16 * i : rows + 16 * (i + 1), lane0 : lane0 + half].astype(jnp.float32) for i in range(2)]
    sums = [p[0:4] + p[4:8] + p[8:12] for p in parts]
    return jnp.concatenate(sums, axis=1)


SCALE = LOG2E / 8.0


def halves(x):
    left = lax.broadcasted_iota(jnp.int32, (1, LANES), 1) < LANES // 2
    none = jnp.zeros((), x.dtype)
    return jnp.where(left, x, none), jnp.where(left, none, x)


def fill_slots(q_ref, k_ref, grad_ref, aux_ref, received, a_ref, b_ref, aux_all):
    rows = q_ref.shape[0]
    for h in range(2):
        a_ref[h] = q_ref[:, h * LANES : (h + 1) * LANES]
        b_ref[h] = grad_ref[:, h * LANES : (h + 1) * LANES]
        a_ref[2 + h] = k_ref[:, h * LANES : (h + 1) * LANES]
        aux_all[h, 0:4, :] = aux_ref[8 * h : 8 * h + 4, :]
    for i, ref in enumerate(received):
        a_ref[4 + i] = ref[0:rows, 0:LANES]
        b_ref[4 + i] = ref[0:rows, LANES : 2 * LANES]
        aux_all[4 + i, 0:4, :] = join_pieces(ref, rows, 0)
    rx_ref = received[0]
    a_ref[9] = rx_ref[0:rows, 2 * LANES : 3 * LANES]
    b_ref[9] = rx_ref[0:rows, 3 * LANES : 4 * LANES]
    aux_all[9, 0:4, :] = join_pieces(rx_ref, rows, rows // 2)
    a_ref[8] = rx_ref[0:rows, 4 * LANES : 5 * LANES]


def softmax_pair(key, query0, query1, aux, masked):
    map0 = jnp.exp2(nt(key, query0) * SCALE - aux[0:1])
    map1 = jnp.exp2(nt(key, query1) * SCALE - aux[1:2])
    if masked:
        key_pos = lax.broadcasted_iota(jnp.int32, map0.shape, 0)
        query_pos = lax.broadcasted_iota(jnp.int32, map0.shape, 1)
        seen = key_pos <= query_pos
        map0 = jnp.where(seen, map0, 0.0)
        map1 = jnp.where(seen, map1, 0.0)
    return map0, map1


def each_unit(unit, full):
    bits = level_bits()

    def own_unit(h, carry):
        unit(h, 2 + h, True)
        return carry

    def full_unit(u, carry):
        level = jnp.where(u == 0, 0, jnp.where(u < 3, 1, 2))
        bit = jnp.where(level == 0, bits[0], jnp.where(level == 1, bits[1], bits[2]))
        other = 4 + (u + 1) // 2
        own = (u == 0) | (u % 2 == 1)
        unit(jnp.where(bit == 0, other, jnp.where(own, 1, 9)), jnp.where(bit == 0, jnp.where(own, 2, 8), other), False)
        return carry

    lax.fori_loop(0, 2, own_unit, 0)
    lax.fori_loop(0, full, full_unit, 0)


def mixed_kernel(
    q_ref, k_ref, grad_ref, aux_ref, rx_ref, rz_ref, r4_ref, r6_ref,
    dv_ref, tx_ref, tz_ref, t4_ref, t6_ref, a_ref, b_ref, aux_all, s_ref,
):
    rows = q_ref.shape[0]
    fill_slots(q_ref, k_ref, grad_ref, aux_ref, (rx_ref, rz_ref, r4_ref, r6_ref), a_ref, b_ref, aux_all)
    s_ref[...] = jnp.zeros(s_ref.shape, jnp.float32)

    def unit(qs, ks, masked):
        query0, query1 = halves(a_ref[qs])
        grad = b_ref[qs]
        aux = aux_all[qs]
        for c in range(rows // CHUNK):
            low = c * CHUNK
            first = low if masked else 0
            key = a_ref[ks, low : low + CHUNK, :]
            map0, map1 = softmax_pair(key, query0[first:], query1[first:], aux[:, first:], masked)
            mixed = (map0 - map1).astype(jnp.bfloat16)
            s_ref[ks, low : low + CHUNK, :] += jnp.dot(mixed, grad[first:], preferred_element_type=jnp.float32)

    each_unit(unit, 7)
    dv_ref[...] = s_ref[2:4]
    tx_ref[:, 0:LANES] = s_ref[8].astype(jnp.bfloat16)
    tx_ref[:, LANES : 2 * LANES] = s_ref[4].astype(jnp.bfloat16)
    for ref, slot in ((tz_ref, 5), (t4_ref, 6), (t6_ref, 7)):
        ref[...] = s_ref[slot].astype(jnp.bfloat16)


def score_kernel(
    q_ref, k_ref, grad_ref, aux_ref, rx_ref, rz_ref, r4_ref, r6_ref, v_ref, vx_ref, vz_ref, v4_ref, v6_ref,
    own_ref, tx_ref, tz_ref, t4_ref, t6_ref, a_ref, b_ref, aux_all, s_ref,
):
    rows = q_ref.shape[0]
    bits = level_bits()
    fill_slots(q_ref, k_ref, grad_ref, aux_ref, (rx_ref, rz_ref, r4_ref, r6_ref), a_ref, b_ref, aux_all)
    for h in range(2):
        b_ref[2 + h] = v_ref[:, h * LANES : (h + 1) * LANES]
    b_ref[8] = vx_ref[:, 0:LANES]
    for slot, ref, lane0, bit in ((4, vx_ref, LANES, bits[0]), (5, vz_ref, 0, bits[1]), (6, v4_ref, 0, bits[2]), (7, v6_ref, 0, bits[2])):

        @pl.when(bit != 0)
        def _(slot=slot, ref=ref, lane0=lane0):
            b_ref[slot] = ref[:, lane0 : lane0 + LANES]

    s_ref[...] = jnp.zeros(s_ref.shape, jnp.float32)

    def unit(qs, ks, masked):
        query0, query1 = halves(a_ref[qs])
        grad = b_ref[qs]
        aux = aux_all[qs]
        for c in range(rows // CHUNK):
            low = c * CHUNK
            first = low if masked else 0
            key = a_ref[ks, low : low + CHUNK, :]
            key0, key1 = halves(key)
            map0, map1 = softmax_pair(key, query0[first:], query1[first:], aux[:, first:], masked)
            dots = nt(b_ref[ks, low : low + CHUNK, :], grad[first:])
            score0 = (map0 * (dots - aux[2:3, first:])).astype(jnp.bfloat16)
            score1 = (map1 * (aux[3:4, first:] - dots)).astype(jnp.bfloat16)
            s_ref[ks, low : low + CHUNK, :] += jnp.dot(score0, query0[first:], preferred_element_type=jnp.float32) + jnp.dot(
                score1, query1[first:], preferred_element_type=jnp.float32
            )
            turned = tn(key0, score0) + tn(key1, score1)
            for i in range((rows - first) // LANES):
                s_ref[qs, first + i * LANES : first + (i + 1) * LANES, :] += turned[:, i * LANES : (i + 1) * LANES]

    each_unit(unit, 7)
    own_ref[...] = s_ref[0:4]
    for i, slot in enumerate((4, 8, 9)):
        tx_ref[:, i * LANES : (i + 1) * LANES] = s_ref[slot].astype(jnp.bfloat16)
    for ref, slot in ((tz_ref, 5), (t4_ref, 6), (t6_ref, 7)):
        ref[...] = s_ref[slot].astype(jnp.bfloat16)


def join_kernel(own_ref, ux_ref, uz_ref, u4_ref, u6_ref, dq_ref, dk_ref, s_ref):
    bits = level_bits()
    for i in range(4):
        s_ref[i] = own_ref[i]
    s_ref[2] += ux_ref[:, LANES : 2 * LANES].astype(jnp.float32)
    s_ref[1] += ux_ref[:, 2 * LANES : 3 * LANES].astype(jnp.float32)
    for ref, bit in ((ux_ref, bits[0]), (uz_ref, bits[1]), (u4_ref, bits[2]), (u6_ref, bits[2])):
        spot = jnp.where(bit == 0, 3, 0)
        s_ref[spot] += ref[:, 0:LANES].astype(jnp.float32)
    for h in range(2):
        for i in range(s_ref.shape[1] // LANES):
            spot = slice(i * LANES, (i + 1) * LANES)
            dq_ref[spot, h * LANES : (h + 1) * LANES] = jnp.transpose(s_ref[h, spot, :]) * 0.125
        dk_ref[:, h * LANES : (h + 1) * LANES] = s_ref[2 + h] * 0.125


def call(kernel, outs, args, scratch=(), smem=(), micros=1):
    vmem = pl.BlockSpec(memory_space=pltpu.VMEM)
    specs = [pl.BlockSpec(memory_space=pltpu.SMEM) if i in smem else vmem for i in range(len(args))]
    return pl.pallas_call(
        kernel,
        out_shape=[jax.ShapeDtypeStruct(s, d) for s, d in outs],
        in_specs=specs,
        out_specs=[vmem] * len(outs),
        scratch_shapes=list(scratch),
        cost_estimate=pl.CostEstimate(flops=micros * 14_000_000, bytes_accessed=1_000_000, transcendentals=0),
    )(*args)


def swap(x, axis, size, mask):
    return lax.ppermute(x, axis, [(i, i ^ mask) for i in range(size)])


def paired_device(*args):
    return paired_steps(*args)


def paired_steps(queries, key_vectors, latents, w_value, log_sums, out_pair, cotangent, lambdas, out_gain):
    rows, width = queries.shape
    narrow, wide = jnp.bfloat16, jnp.float32
    seq, feat = lax.axis_size("sp"), lax.axis_size("tp")
    slot_shape = (rows, LANES)
    far = swap(latents, "tp", feat, 2)
    near = swap(latents, "tp", feat, 1)
    grad, aux, px, pz, pm = call(
        prep_kernel,
        [((rows, width), narrow), ((16, rows), wide), ((rows + AUX_ROWS, 5 * LANES), narrow),
         ((rows + AUX_ROWS, width), narrow), ((rows + AUX_ROWS, width), narrow)],
        (queries, key_vectors, log_sums.T, out_pair, cotangent, lambdas, out_gain[None, :]),
        smem=(5,), micros=4,
    )
    r4 = swap(pm, "sp", seq, 4)
    r6 = swap(pm, "sp", seq, 6)
    rz = swap(pz, "sp", seq, 2)
    rx = swap(px, "sp", seq, 1)
    next_far = swap(far, "tp", feat, 1)
    values, second = call(value_kernel, [((rows, width), narrow), (slot_shape, narrow)], (latents, far, near, next_far, w_value), micros=3)
    v4 = swap(second, "sp", seq, 4)
    v6 = swap(second, "sp", seq, 6)
    vz = swap(second, "sp", seq, 2)
    vx = swap(values, "sp", seq, 1)
    slots = [pltpu.VMEM((SLOTS,) + slot_shape, narrow), pltpu.VMEM((SLOTS,) + slot_shape, narrow),
             pltpu.VMEM((SLOTS, 8, rows), wide), pltpu.VMEM((SLOTS,) + slot_shape, wide)]
    shared = (queries, key_vectors, grad, aux, rx, rz, r4, r6)
    dv0, tx, tz, t4, t6 = call(
        mixed_kernel, [((2,) + slot_shape, wide), ((rows, 2 * LANES), narrow)] + [(slot_shape, narrow)] * 3,
        shared, scratch=slots, micros=8,
    )
    u4 = swap(t4, "sp", seq, 4)
    u6 = swap(t6, "sp", seq, 6)
    uz = swap(tz, "sp", seq, 2)
    ux = swap(tx, "sp", seq, 1)
    own, sx, sz, s4, s6 = call(
        score_kernel, [((4,) + slot_shape, wide), ((rows, 3 * LANES), narrow)] + [(slot_shape, narrow)] * 3,
        shared + (values, vx, vz, v4, v6), scratch=slots, micros=16,
    )
    part, dv, _ = call(
        weight_kernel, [((latents.shape[1] * feat, width), narrow), ((rows, width), wide), ((rows, width), narrow)],
        (latents, far, near, next_far, dv0, ux, uz, u4, u6), micros=5,
    )
    w4 = swap(s4, "sp", seq, 4)
    w6 = swap(s6, "sp", seq, 6)
    wz = swap(sz, "sp", seq, 2)
    wx = swap(sx, "sp", seq, 1)
    pieces = lax.all_to_all(part.reshape(seq, -1, width), "sp", 0, 0)
    dq, dk = call(
        join_kernel, [((rows, width), wide)] * 2, (own, wx, wz, w4, w6),
        scratch=[pltpu.VMEM((4,) + slot_shape, wide)], micros=3,
    )
    return dq, dk, dv, jnp.sum(pieces.astype(wide), axis=0)


def solution(mesh):
    paired = (mesh.shape["sp"], mesh.shape["tp"]) == (8, 4)
    return jax.shard_map(
        paired_device if paired else general_device,
        mesh=mesh,
        in_specs=(
            P("sp", "tp"),
            P("sp", "tp"),
            P("sp", "tp"),
            P(None, "tp"),
            P("sp", "tp"),
            P("sp", "tp"),
            P("sp", "tp"),
            P("tp"),
            P(),
        ),
        out_specs=(P("sp", "tp"), P("sp", "tp"), P("sp", "tp"), P("sp", "tp")),
        check_vma=False,
    )
```

```python
import jax
import jax.numpy as jnp
from jax import lax
from jax.experimental import pallas as pl
from jax.experimental.pallas import tpu as pltpu
from jax.sharding import PartitionSpec as P


norm_floor = 0.25
block_rows = 512


def head_cotangent(out_pair, cotangent, lambdas, out_gain):
    tok_rows = out_pair.shape[0]
    head_count = lambdas.shape[0]
    out_maps = out_pair.astype(jnp.float32).reshape(tok_rows, head_count, 2, -1)
    lam_cols = lambdas[None, :, None]
    merged = out_maps[:, :, 0] - lam_cols * out_maps[:, :, 1]
    inv_norm = lax.rsqrt(jnp.mean(merged * merged, axis=-1, keepdims=True) + norm_floor)
    scaled = cotangent.astype(jnp.float32).reshape(merged.shape) * out_gain
    inner_dot = jnp.mean(scaled * merged, axis=-1, keepdims=True)
    out_grad = (inv_norm * scaled - merged * (inv_norm * inv_norm * inv_norm) * inner_dot).astype(
        jnp.bfloat16
    )
    grad_wide = out_grad.astype(jnp.float32)
    first_map = jnp.sum(grad_wide * out_maps[:, :, 0], axis=-1)
    second_map = -lambdas[None, :] * jnp.sum(grad_wide * out_maps[:, :, 1], axis=-1)
    return (out_grad, jnp.stack([first_map, second_map], axis=-1))


def block_terms(
    query_block,
    key_block,
    value_block,
    grad_block,
    log_block,
    term_block,
    lambdas,
    query_pos,
    key_pos,
):
    factor = query_block.shape[-1] ** (-0.5)
    scores = (
        jnp.einsum("qhcd,khcd->hcqk", query_block, key_block, preferred_element_type=jnp.float32)
        * factor
    )
    visible = key_pos[None, :] <= query_pos[:, None]
    shifted = scores - jnp.transpose(log_block, (1, 2, 0))[..., None]
    softmax_maps = jnp.where(visible, jnp.exp(shifted), 0.0)
    value_dot = jnp.einsum(
        "qhe,khe->hqk", grad_block, value_block, preferred_element_type=jnp.float32
    )
    lam_cols = lambdas[:, None, None]
    weights = (softmax_maps[:, 0] - lam_cols * softmax_maps[:, 1]).astype(jnp.bfloat16)
    term_cols = jnp.transpose(term_block, (1, 2, 0))
    first_map = softmax_maps[:, 0] * (value_dot - term_cols[:, 0, :, None])
    second_map = softmax_maps[:, 1] * (-lam_cols * value_dot - term_cols[:, 1, :, None])
    dscore = (jnp.stack([first_map, second_map], axis=1) * factor).astype(jnp.bfloat16)
    return (weights, dscore)


def block_span():
    return block_rows


def general_device(
    queries, key_vectors, latents, w_value, log_sums, out_pair, cotangent, lambdas, out_gain
):
    tok_rows = queries.shape[0]
    head_count = lambdas.shape[0]
    offset = lax.axis_index("sp") * tok_rows
    own_pos = offset + jnp.arange(tok_rows, dtype=jnp.int32)
    last_pos = offset + tok_rows - 1
    gathered = lax.all_gather(latents, "tp", axis=1, tiled=True)
    values = jnp.dot(gathered, w_value, preferred_element_type=jnp.float32).astype(jnp.bfloat16)
    out_grad, row_terms = head_cotangent(out_pair, cotangent, lambdas, out_gain)
    query_heads = queries.reshape(tok_rows, head_count, 2, -1)
    key_heads = key_vectors.reshape(tok_rows, head_count, 2, -1)
    value_heads = values.reshape(tok_rows, head_count, -1)
    log_heads = log_sums.reshape(tok_rows, head_count, 2)
    grad_flat = out_grad.reshape(tok_rows, -1)
    term_flat = row_terms.reshape(tok_rows, -1)
    zero_keys = jnp.zeros(key_heads.shape, jnp.float32)
    zero_values = jnp.zeros(value_heads.shape, jnp.float32)
    shards = (
        lax.all_gather(key_vectors, "sp", axis=0, tiled=True),
        lax.all_gather(values, "sp", axis=0, tiled=True),
    )
    key_piece = shards[0]
    value_piece = shards[1]
    piece_rows = key_piece.shape[0]
    block_len = block_span()

    def query_add_block(block_idx, partial_value):
        begin_row = block_idx * block_len
        key_block = lax.dynamic_slice_in_dim(key_piece, begin_row, block_len, 0).reshape(
            block_len, head_count, 2, -1
        )
        value_block = lax.dynamic_slice_in_dim(value_piece, begin_row, block_len, 0).reshape(
            block_len, head_count, -1
        )
        key_pos = begin_row + jnp.arange(block_len, dtype=jnp.int32)

        def query_compute(sums):
            _, dscore = block_terms(
                query_heads,
                key_block,
                value_block,
                out_grad,
                log_heads,
                row_terms,
                lambdas,
                own_pos,
                key_pos,
            )
            return sums + jnp.einsum(
                "hcqk,khcd->qhcd", dscore, key_block, preferred_element_type=jnp.float32
            )

        return lax.cond(begin_row <= last_pos, query_compute, lambda sums: sums, partial_value)

    query_grad = lax.fori_loop(0, piece_rows // block_len, query_add_block, zero_keys)
    shards = (
        lax.all_gather(queries.astype(jnp.float32), "sp", axis=0, tiled=True).astype(jnp.bfloat16),
        lax.all_gather(grad_flat.astype(jnp.float32), "sp", axis=0, tiled=True).astype(
            jnp.bfloat16
        ),
        lax.all_gather(log_sums, "sp", axis=0, tiled=True),
        lax.all_gather(term_flat, "sp", axis=0, tiled=True),
    )
    query_piece = shards[0]
    grad_piece = shards[1]
    log_piece = shards[2]
    term_piece = shards[3]
    piece_rows = query_piece.shape[0]
    key_block_len = block_span()

    def key_add_block(block_idx, partial_value):
        begin_row = block_idx * key_block_len
        query_block = lax.dynamic_slice_in_dim(query_piece, begin_row, key_block_len, 0).reshape(
            key_block_len, head_count, 2, -1
        )
        grad_block = lax.dynamic_slice_in_dim(grad_piece, begin_row, key_block_len, 0).reshape(
            key_block_len, head_count, -1
        )
        log_block = lax.dynamic_slice_in_dim(log_piece, begin_row, key_block_len, 0).reshape(
            key_block_len, head_count, 2
        )
        term_block = lax.dynamic_slice_in_dim(term_piece, begin_row, key_block_len, 0).reshape(
            key_block_len, head_count, 2
        )
        query_pos = begin_row + jnp.arange(key_block_len, dtype=jnp.int32)

        def key_compute(sums):
            weights, dscore = block_terms(
                query_block,
                key_heads,
                value_heads,
                grad_block,
                log_block,
                term_block,
                lambdas,
                query_pos,
                own_pos,
            )
            key_sum = sums[0] + jnp.einsum(
                "hcqk,qhcd->khcd", dscore, query_block, preferred_element_type=jnp.float32
            )
            value_sum = sums[1] + jnp.einsum(
                "hqk,qhe->khe", weights, grad_block, preferred_element_type=jnp.float32
            )
            return (key_sum, value_sum)

        return lax.cond(
            begin_row + key_block_len - 1 >= offset, key_compute, lambda sums: sums, partial_value
        )

    key_grad, value_grad = lax.fori_loop(
        0, piece_rows // key_block_len, key_add_block, (zero_keys, zero_values)
    )
    value_flat = value_grad.reshape(tok_rows, -1)
    value_narrow = value_flat.astype(jnp.bfloat16)
    weight_grad = lax.psum_scatter(
        lax.dot_general(
            gathered, value_narrow, (((0,), (0,)), ((), ())), preferred_element_type=jnp.float32
        ),
        "sp",
        scatter_dimension=0,
        tiled=True,
    )
    return (
        query_grad.reshape(tok_rows, -1),
        key_grad.reshape(tok_rows, -1),
        value_flat,
        weight_grad,
    )


LOG2E = 1.4426950408889634
AUX_ROWS = 32
SLOTS = 10
CHUNK = 512
LANES = 128


def nt(a, b):
    return lax.dot_general(a, b, (((1,), (1,)), ((), ())), preferred_element_type=jnp.float32)


def tn(a, b):
    return lax.dot_general(a, b, (((0,), (0,)), ((), ())), preferred_element_type=jnp.float32)


def level_bits():
    place = lax.axis_index("sp")
    return place % 2, (place // 2) % 2, (place // 4) % 2


def split_pieces(rows):
    high = rows.astype(jnp.bfloat16)
    rest = rows - high.astype(jnp.float32)
    middle = rest.astype(jnp.bfloat16)
    low = (rest - middle.astype(jnp.float32)).astype(jnp.bfloat16)
    return high, middle, low


def prep_kernel(q_ref, k_ref, log_ref, pair_ref, cot_ref, lam_ref, gain_ref, grad_ref, aux_ref, px_ref, pz_ref, pm_ref):
    rows = q_ref.shape[0]
    half = rows // 2
    bit0, bit1, bit2 = level_bits()
    lane = lax.broadcasted_iota(jnp.int32, (rows, LANES), 1)
    aux_blocks = []
    for h in range(2):
        first = pair_ref[:, 2 * h * LANES : (2 * h + 1) * LANES].astype(jnp.float32)
        second = pair_ref[:, (2 * h + 1) * LANES : (2 * h + 2) * LANES].astype(jnp.float32)
        lam = lam_ref[h]
        merged = first - lam * second
        inv = lax.rsqrt(jnp.mean(merged * merged, axis=-1, keepdims=True) + norm_floor)
        scaled = cot_ref[:, h * LANES : (h + 1) * LANES].astype(jnp.float32) * gain_ref[...]
        inner = jnp.mean(scaled * merged, axis=-1, keepdims=True)
        grad = (inv * scaled - merged * (inv * inv * inv) * inner).astype(jnp.bfloat16)
        grad_ref[:, h * LANES : (h + 1) * LANES] = grad
        wide = grad.astype(jnp.float32)
        term0 = jnp.sum(wide * first, axis=-1, keepdims=True)
        term1 = jnp.sum(wide * second, axis=-1, keepdims=True)
        terms = jnp.where(lane == 2, term0, jnp.where(lane == 3, term1, 0.0))
        turned = jnp.concatenate(
            [jnp.transpose(terms[i * LANES : (i + 1) * LANES])[0:8] for i in range(rows // LANES)], axis=1
        )
        log0 = log_ref[2 * h : 2 * h + 1, :] * LOG2E
        log1 = (log_ref[2 * h + 1 : 2 * h + 2, :] - jnp.log(jnp.full((1, rows), lam, jnp.float32))) * LOG2E
        aux = jnp.concatenate([log0, log1, turned[2:4], jnp.zeros((4, rows), jnp.float32)], axis=0)
        aux_ref[h * 8 : (h + 1) * 8, :] = aux
        pieces = split_pieces(aux)
        wide_rows = jnp.concatenate([p.astype(jnp.float32)[0:4] for p in pieces] + [jnp.zeros((4, rows), jnp.float32)], axis=0)
        aux_blocks.append(wide_rows.astype(jnp.bfloat16))

    def put(ref, lane0, early, head_k, head_q):

        @pl.when(early)
        def _():
            ref[0:rows, lane0 : lane0 + LANES] = k_ref[:, head_k * LANES : (head_k + 1) * LANES]
            ref[0:rows, lane0 + LANES : lane0 + 2 * LANES] = k_ref[:, head_k * LANES : (head_k + 1) * LANES]

        @pl.when(jnp.logical_not(early))
        def _():
            ref[0:rows, lane0 : lane0 + LANES] = q_ref[:, head_q * LANES : (head_q + 1) * LANES]
            ref[0:rows, lane0 + LANES : lane0 + 2 * LANES] = grad_ref[:, head_q * LANES : (head_q + 1) * LANES]

    def put_aux(ref, lane0, h):
        ref[rows : rows + 16, lane0 : lane0 + half] = aux_blocks[h][:, 0:half]
        ref[rows + 16 : rows + 32, lane0 : lane0 + half] = aux_blocks[h][:, half:rows]

    put(px_ref, 0, bit0 == 0, 1, 0)
    px_ref[0:rows, 2 * LANES : 3 * LANES] = q_ref[:, LANES : 2 * LANES]
    px_ref[0:rows, 3 * LANES : 4 * LANES] = grad_ref[:, LANES : 2 * LANES]
    px_ref[0:rows, 4 * LANES : 5 * LANES] = k_ref[:, 0:LANES]
    px_ref[rows : rows + 32, 4 * LANES : 5 * LANES] = jnp.zeros((32, LANES), jnp.bfloat16)
    put_aux(px_ref, 0, 0)
    put_aux(px_ref, half, 1)
    put(pz_ref, 0, bit1 == 0, 1, 0)
    put_aux(pz_ref, 0, 0)
    put(pm_ref, 0, bit2 == 0, 1, 0)
    put_aux(pm_ref, 0, 0)


def value_kernel(own_ref, far_ref, near_ref, next_ref, w_ref, out_ref, second_ref):
    cols = own_ref.shape[1]
    place = lax.axis_index("tp")

    def part(x, spot):
        return jnp.dot(x, w_ref[pl.ds(spot * cols, cols), :], preferred_element_type=jnp.float32)

    total = part(own_ref[...], place) + part(far_ref[...], (place + 2) % 4)
    near = place + 1 - 2 * (place % 2)
    total += part(near_ref[...], near) + part(next_ref[...], (near + 2) % 4)
    out_ref[...] = total.astype(jnp.bfloat16)
    second_ref[...] = total[:, LANES : 2 * LANES].astype(jnp.bfloat16)


def weight_kernel(own_ref, far_ref, near_ref, next_ref, dv0_ref, ux_ref, uz_ref, u4_ref, u6_ref, out_ref, dv_ref, narrow_ref):
    bits = level_bits()
    cols = own_ref.shape[1]
    place = lax.axis_index("tp")
    near = place + 1 - 2 * (place % 2)
    dv_ref[:, 0:LANES] = dv0_ref[0] + ux_ref[:, 0:LANES].astype(jnp.float32)
    dv_ref[:, LANES : 2 * LANES] = dv0_ref[1]
    for ref, lane0, bit in ((ux_ref, LANES, bits[0]), (uz_ref, 0, bits[1]), (u4_ref, 0, bits[2]), (u6_ref, 0, bits[2])):

        @pl.when(bit == 0)
        def _(ref=ref, lane0=lane0):
            dv_ref[:, LANES : 2 * LANES] += ref[:, lane0 : lane0 + LANES].astype(jnp.float32)

    narrow_ref[...] = dv_ref[...].astype(jnp.bfloat16)
    grad = narrow_ref[...]
    size = out_ref.shape[2]
    for ref, spot in ((own_ref, place), (far_ref, (place + 2) % 4), (near_ref, near), (next_ref, (near + 2) % 4)):
        block = tn(ref[...], grad).astype(jnp.bfloat16)
        for i in range(cols // size):
            part = spot * (cols // size) + i
            out_ref[part % 4, part // 4] = block[i * size : (i + 1) * size]


def fold_kernel(pieces_ref, keep_ref, send_ref):
    bit = lax.axis_index("sp") // 4
    for ref, spot in ((keep_ref, bit), (send_ref, 1 - bit)):
        total = pieces_ref[0, spot].astype(jnp.float32)
        for i in range(1, pieces_ref.shape[0]):
            total += pieces_ref[i, spot].astype(jnp.float32)
        ref[...] = total.astype(ref.dtype)


def join_pieces(block_ref, rows, lane0):
    half = rows // 2
    parts = [block_ref[rows + 16 * i : rows + 16 * (i + 1), lane0 : lane0 + half].astype(jnp.float32) for i in range(2)]
    sums = [p[0:4] + p[4:8] + p[8:12] for p in parts]
    return jnp.concatenate(sums, axis=1)


SCALE = LOG2E / 8.0


def halves(x):
    left = lax.broadcasted_iota(jnp.int32, (1, LANES), 1) < LANES // 2
    none = jnp.zeros((), x.dtype)
    return jnp.where(left, x, none), jnp.where(left, none, x)


def fill_slots(q_ref, k_ref, grad_ref, aux_ref, received, a_ref, b_ref, aux_all):
    rows = q_ref.shape[0]
    for h in range(2):
        a_ref[h] = q_ref[:, h * LANES : (h + 1) * LANES]
        b_ref[h] = grad_ref[:, h * LANES : (h + 1) * LANES]
        a_ref[2 + h] = k_ref[:, h * LANES : (h + 1) * LANES]
        aux_all[h, 0:4, :] = aux_ref[8 * h : 8 * h + 4, :]
    for i, ref in enumerate(received):
        a_ref[4 + i] = ref[0:rows, 0:LANES]
        b_ref[4 + i] = ref[0:rows, LANES : 2 * LANES]
        aux_all[4 + i, 0:4, :] = join_pieces(ref, rows, 0)
    rx_ref = received[0]
    a_ref[9] = rx_ref[0:rows, 2 * LANES : 3 * LANES]
    b_ref[9] = rx_ref[0:rows, 3 * LANES : 4 * LANES]
    aux_all[9, 0:4, :] = join_pieces(rx_ref, rows, rows // 2)
    a_ref[8] = rx_ref[0:rows, 4 * LANES : 5 * LANES]


def softmax_pair(key, query0, query1, aux, masked):
    map0 = jnp.exp2(nt(key, query0) * SCALE - aux[0:1])
    map1 = jnp.exp2(nt(key, query1) * SCALE - aux[1:2])
    if masked:
        key_pos = lax.broadcasted_iota(jnp.int32, map0.shape, 0)
        query_pos = lax.broadcasted_iota(jnp.int32, map0.shape, 1)
        seen = key_pos <= query_pos
        map0 = jnp.where(seen, map0, 0.0)
        map1 = jnp.where(seen, map1, 0.0)
    return map0, map1


def each_unit(unit, full):
    bits = level_bits()

    def own_unit(h, carry):
        unit(h, 2 + h, True)
        return carry

    def full_unit(u, carry):
        level = jnp.where(u == 0, 0, jnp.where(u < 3, 1, 2))
        bit = jnp.where(level == 0, bits[0], jnp.where(level == 1, bits[1], bits[2]))
        other = 4 + (u + 1) // 2
        own = (u == 0) | (u % 2 == 1)
        unit(jnp.where(bit == 0, other, jnp.where(own, 1, 9)), jnp.where(bit == 0, jnp.where(own, 2, 8), other), False)
        return carry

    lax.fori_loop(0, 2, own_unit, 0)
    lax.fori_loop(0, full, full_unit, 0)


def mixed_kernel(
    q_ref, k_ref, grad_ref, aux_ref, rx_ref, rz_ref, r4_ref, r6_ref,
    dv_ref, tx_ref, tz_ref, t4_ref, t6_ref, a_ref, b_ref, aux_all, s_ref,
):
    rows = q_ref.shape[0]
    fill_slots(q_ref, k_ref, grad_ref, aux_ref, (rx_ref, rz_ref, r4_ref, r6_ref), a_ref, b_ref, aux_all)
    s_ref[...] = jnp.zeros(s_ref.shape, jnp.float32)

    def unit(qs, ks, masked):
        query0, query1 = halves(a_ref[qs])
        grad = b_ref[qs]
        aux = aux_all[qs]
        for c in range(rows // CHUNK):
            low = c * CHUNK
            first = low if masked else 0
            key = a_ref[ks, low : low + CHUNK, :]
            map0, map1 = softmax_pair(key, query0[first:], query1[first:], aux[:, first:], masked)
            mixed = (map0 - map1).astype(jnp.bfloat16)
            s_ref[ks, low : low + CHUNK, :] += jnp.dot(mixed, grad[first:], preferred_element_type=jnp.float32)

    each_unit(unit, 7)
    dv_ref[...] = s_ref[2:4]
    tx_ref[:, 0:LANES] = s_ref[8].astype(jnp.bfloat16)
    tx_ref[:, LANES : 2 * LANES] = s_ref[4].astype(jnp.bfloat16)
    for ref, slot in ((tz_ref, 5), (t4_ref, 6), (t6_ref, 7)):
        ref[...] = s_ref[slot].astype(jnp.bfloat16)


def score_kernel(
    q_ref, k_ref, grad_ref, aux_ref, rx_ref, rz_ref, r4_ref, r6_ref, v_ref, vx_ref, vz_ref, v4_ref, v6_ref,
    own_ref, tx_ref, tz_ref, t4_ref, t6_ref, a_ref, b_ref, aux_all, s_ref,
):
    rows = q_ref.shape[0]
    bits = level_bits()
    fill_slots(q_ref, k_ref, grad_ref, aux_ref, (rx_ref, rz_ref, r4_ref, r6_ref), a_ref, b_ref, aux_all)
    for h in range(2):
        b_ref[2 + h] = v_ref[:, h * LANES : (h + 1) * LANES]
    b_ref[8] = vx_ref[:, 0:LANES]
    for slot, ref, lane0, bit in ((4, vx_ref, LANES, bits[0]), (5, vz_ref, 0, bits[1]), (6, v4_ref, 0, bits[2]), (7, v6_ref, 0, bits[2])):

        @pl.when(bit != 0)
        def _(slot=slot, ref=ref, lane0=lane0):
            b_ref[slot] = ref[:, lane0 : lane0 + LANES]

    s_ref[...] = jnp.zeros(s_ref.shape, jnp.float32)

    def unit(qs, ks, masked):
        query0, query1 = halves(a_ref[qs])
        grad = b_ref[qs]
        aux = aux_all[qs]
        for c in range(rows // CHUNK):
            low = c * CHUNK
            first = low if masked else 0
            key = a_ref[ks, low : low + CHUNK, :]
            key0, key1 = halves(key)
            map0, map1 = softmax_pair(key, query0[first:], query1[first:], aux[:, first:], masked)
            dots = nt(b_ref[ks, low : low + CHUNK, :], grad[first:])
            score0 = (map0 * (dots - aux[2:3, first:])).astype(jnp.bfloat16)
            score1 = (map1 * (aux[3:4, first:] - dots)).astype(jnp.bfloat16)
            s_ref[ks, low : low + CHUNK, :] += jnp.dot(score0, query0[first:], preferred_element_type=jnp.float32) + jnp.dot(
                score1, query1[first:], preferred_element_type=jnp.float32
            )
            turned = tn(key0, score0) + tn(key1, score1)
            for i in range((rows - first) // LANES):
                s_ref[qs, first + i * LANES : first + (i + 1) * LANES, :] += turned[:, i * LANES : (i + 1) * LANES]

    each_unit(unit, 7)
    own_ref[...] = s_ref[0:4]
    for i, slot in enumerate((4, 8, 9)):
        tx_ref[:, i * LANES : (i + 1) * LANES] = s_ref[slot].astype(jnp.bfloat16)
    for ref, slot in ((tz_ref, 5), (t4_ref, 6), (t6_ref, 7)):
        ref[...] = s_ref[slot].astype(jnp.bfloat16)


def join_kernel(own_ref, ux_ref, uz_ref, u4_ref, u6_ref, dq_ref, dk_ref, s_ref):
    bits = level_bits()
    for i in range(4):
        s_ref[i] = own_ref[i]
    s_ref[2] += ux_ref[:, LANES : 2 * LANES].astype(jnp.float32)
    s_ref[1] += ux_ref[:, 2 * LANES : 3 * LANES].astype(jnp.float32)
    for ref, bit in ((ux_ref, bits[0]), (uz_ref, bits[1]), (u4_ref, bits[2]), (u6_ref, bits[2])):
        spot = jnp.where(bit == 0, 3, 0)
        s_ref[spot] += ref[:, 0:LANES].astype(jnp.float32)
    for h in range(2):
        for i in range(s_ref.shape[1] // LANES):
            spot = slice(i * LANES, (i + 1) * LANES)
            dq_ref[spot, h * LANES : (h + 1) * LANES] = jnp.transpose(s_ref[h, spot, :]) * 0.125
        dk_ref[:, h * LANES : (h + 1) * LANES] = s_ref[2 + h] * 0.125


def call(kernel, outs, args, scratch=(), smem=(), micros=1):
    vmem = pl.BlockSpec(memory_space=pltpu.VMEM)
    specs = [pl.BlockSpec(memory_space=pltpu.SMEM) if i in smem else vmem for i in range(len(args))]
    return pl.pallas_call(
        kernel,
        out_shape=[jax.ShapeDtypeStruct(s, d) for s, d in outs],
        in_specs=specs,
        out_specs=[vmem] * len(outs),
        scratch_shapes=list(scratch),
        cost_estimate=pl.CostEstimate(flops=micros * 14_000_000, bytes_accessed=1_000_000, transcendentals=0),
    )(*args)


def swap(x, axis, size, mask):
    return lax.ppermute(x, axis, [(i, i ^ mask) for i in range(size)])


def paired_device(*args):
    return paired_steps(*args)


def paired_steps(queries, key_vectors, latents, w_value, log_sums, out_pair, cotangent, lambdas, out_gain):
    rows, width = queries.shape
    narrow, wide = jnp.bfloat16, jnp.float32
    seq, feat = lax.axis_size("sp"), lax.axis_size("tp")
    slot_shape = (rows, LANES)
    far = swap(latents, "tp", feat, 2)
    near = swap(latents, "tp", feat, 1)
    grad, aux, px, pz, pm = call(
        prep_kernel,
        [((rows, width), narrow), ((16, rows), wide), ((rows + AUX_ROWS, 5 * LANES), narrow),
         ((rows + AUX_ROWS, width), narrow), ((rows + AUX_ROWS, width), narrow)],
        (queries, key_vectors, log_sums.T, out_pair, cotangent, lambdas, out_gain[None, :]),
        smem=(5,), micros=4,
    )
    r4 = swap(pm, "sp", seq, 4)
    r6 = swap(r4, "sp", seq, 2)
    rz = swap(pz, "sp", seq, 2)
    rx = swap(px, "sp", seq, 1)
    next_far = swap(far, "tp", feat, 1)
    values, second = call(value_kernel, [((rows, width), narrow), (slot_shape, narrow)], (latents, far, near, next_far, w_value), micros=3)
    v4 = swap(second, "sp", seq, 4)
    v6 = swap(second, "sp", seq, 6)
    vz = swap(second, "sp", seq, 2)
    vx = swap(values, "sp", seq, 1)
    slots = [pltpu.VMEM((SLOTS,) + slot_shape, narrow), pltpu.VMEM((SLOTS,) + slot_shape, narrow),
             pltpu.VMEM((SLOTS, 8, rows), wide), pltpu.VMEM((SLOTS,) + slot_shape, wide)]
    shared = (queries, key_vectors, grad, aux, rx, rz, r4, r6)
    dv0, tx, tz, t4, t6 = call(
        mixed_kernel, [((2,) + slot_shape, wide), ((rows, 2 * LANES), narrow)] + [(slot_shape, narrow)] * 3,
        shared, scratch=slots, micros=8,
    )
    u4 = swap(t4, "sp", seq, 4)
    u6 = swap(t6, "sp", seq, 6)
    uz = swap(tz, "sp", seq, 2)
    ux = swap(tx, "sp", seq, 1)
    own, sx, sz, s4, s6 = call(
        score_kernel, [((4,) + slot_shape, wide), ((rows, 3 * LANES), narrow)] + [(slot_shape, narrow)] * 3,
        shared + (values, vx, vz, v4, v6), scratch=slots, micros=16,
    )
    part, dv, _ = call(
        weight_kernel, [((4, 2, latents.shape[1] * feat // seq, width), narrow), ((rows, width), wide), ((rows, width), narrow)],
        (latents, far, near, next_far, dv0, ux, uz, u4, u6), micros=5,
    )
    w4 = swap(s4, "sp", seq, 4)
    w6 = swap(s6, "sp", seq, 6)
    wz = swap(sz, "sp", seq, 2)
    wx = swap(sx, "sp", seq, 1)
    groups = [list(range(4)), list(range(4, 8))]
    pieces = lax.all_to_all(part, "sp", 0, 0, axis_index_groups=groups)
    keep, send = call(fold_kernel, [(part.shape[2:], wide), (part.shape[2:], narrow)], (pieces,), micros=1)
    last = swap(send, "sp", seq, 4)
    dq, dk = call(
        join_kernel, [((rows, width), wide)] * 2, (own, wx, wz, w4, w6),
        scratch=[pltpu.VMEM((4,) + slot_shape, wide)], micros=3,
    )
    return dq, dk, dv, keep + last.astype(wide)


def solution(mesh):
    paired = (mesh.shape["sp"], mesh.shape["tp"]) == (8, 4)
    return jax.shard_map(
        paired_device if paired else general_device,
        mesh=mesh,
        in_specs=(
            P("sp", "tp"),
            P("sp", "tp"),
            P("sp", "tp"),
            P(None, "tp"),
            P("sp", "tp"),
            P("sp", "tp"),
            P("sp", "tp"),
            P("tp"),
            P(),
        ),
        out_specs=(P("sp", "tp"), P("sp", "tp"), P("sp", "tp"), P("sp", "tp")),
        check_vma=False,
    )
```

```python
import jax
import jax.numpy as jnp
from jax import lax
from jax.experimental import pallas as pl
from jax.experimental.pallas import tpu as pltpu
from jax.sharding import PartitionSpec as P


norm_floor = 0.25
block_rows = 512


def head_cotangent(out_pair, cotangent, lambdas, out_gain):
    tok_rows = out_pair.shape[0]
    head_count = lambdas.shape[0]
    out_maps = out_pair.astype(jnp.float32).reshape(tok_rows, head_count, 2, -1)
    lam_cols = lambdas[None, :, None]
    merged = out_maps[:, :, 0] - lam_cols * out_maps[:, :, 1]
    inv_norm = lax.rsqrt(jnp.mean(merged * merged, axis=-1, keepdims=True) + norm_floor)
    scaled = cotangent.astype(jnp.float32).reshape(merged.shape) * out_gain
    inner_dot = jnp.mean(scaled * merged, axis=-1, keepdims=True)
    out_grad = (inv_norm * scaled - merged * (inv_norm * inv_norm * inv_norm) * inner_dot).astype(
        jnp.bfloat16
    )
    grad_wide = out_grad.astype(jnp.float32)
    first_map = jnp.sum(grad_wide * out_maps[:, :, 0], axis=-1)
    second_map = -lambdas[None, :] * jnp.sum(grad_wide * out_maps[:, :, 1], axis=-1)
    return (out_grad, jnp.stack([first_map, second_map], axis=-1))


def block_terms(
    query_block,
    key_block,
    value_block,
    grad_block,
    log_block,
    term_block,
    lambdas,
    query_pos,
    key_pos,
):
    factor = query_block.shape[-1] ** (-0.5)
    scores = (
        jnp.einsum("qhcd,khcd->hcqk", query_block, key_block, preferred_element_type=jnp.float32)
        * factor
    )
    visible = key_pos[None, :] <= query_pos[:, None]
    shifted = scores - jnp.transpose(log_block, (1, 2, 0))[..., None]
    softmax_maps = jnp.where(visible, jnp.exp(shifted), 0.0)
    value_dot = jnp.einsum(
        "qhe,khe->hqk", grad_block, value_block, preferred_element_type=jnp.float32
    )
    lam_cols = lambdas[:, None, None]
    weights = (softmax_maps[:, 0] - lam_cols * softmax_maps[:, 1]).astype(jnp.bfloat16)
    term_cols = jnp.transpose(term_block, (1, 2, 0))
    first_map = softmax_maps[:, 0] * (value_dot - term_cols[:, 0, :, None])
    second_map = softmax_maps[:, 1] * (-lam_cols * value_dot - term_cols[:, 1, :, None])
    dscore = (jnp.stack([first_map, second_map], axis=1) * factor).astype(jnp.bfloat16)
    return (weights, dscore)


def block_span():
    return block_rows


def general_device(
    queries, key_vectors, latents, w_value, log_sums, out_pair, cotangent, lambdas, out_gain
):
    tok_rows = queries.shape[0]
    head_count = lambdas.shape[0]
    offset = lax.axis_index("sp") * tok_rows
    own_pos = offset + jnp.arange(tok_rows, dtype=jnp.int32)
    last_pos = offset + tok_rows - 1
    gathered = lax.all_gather(latents, "tp", axis=1, tiled=True)
    values = jnp.dot(gathered, w_value, preferred_element_type=jnp.float32).astype(jnp.bfloat16)
    out_grad, row_terms = head_cotangent(out_pair, cotangent, lambdas, out_gain)
    query_heads = queries.reshape(tok_rows, head_count, 2, -1)
    key_heads = key_vectors.reshape(tok_rows, head_count, 2, -1)
    value_heads = values.reshape(tok_rows, head_count, -1)
    log_heads = log_sums.reshape(tok_rows, head_count, 2)
    grad_flat = out_grad.reshape(tok_rows, -1)
    term_flat = row_terms.reshape(tok_rows, -1)
    zero_keys = jnp.zeros(key_heads.shape, jnp.float32)
    zero_values = jnp.zeros(value_heads.shape, jnp.float32)
    shards = (
        lax.all_gather(key_vectors, "sp", axis=0, tiled=True),
        lax.all_gather(values, "sp", axis=0, tiled=True),
    )
    key_piece = shards[0]
    value_piece = shards[1]
    piece_rows = key_piece.shape[0]
    block_len = block_span()

    def query_add_block(block_idx, partial_value):
        begin_row = block_idx * block_len
        key_block = lax.dynamic_slice_in_dim(key_piece, begin_row, block_len, 0).reshape(
            block_len, head_count, 2, -1
        )
        value_block = lax.dynamic_slice_in_dim(value_piece, begin_row, block_len, 0).reshape(
            block_len, head_count, -1
        )
        key_pos = begin_row + jnp.arange(block_len, dtype=jnp.int32)

        def query_compute(sums):
            _, dscore = block_terms(
                query_heads,
                key_block,
                value_block,
                out_grad,
                log_heads,
                row_terms,
                lambdas,
                own_pos,
                key_pos,
            )
            return sums + jnp.einsum(
                "hcqk,khcd->qhcd", dscore, key_block, preferred_element_type=jnp.float32
            )

        return lax.cond(begin_row <= last_pos, query_compute, lambda sums: sums, partial_value)

    query_grad = lax.fori_loop(0, piece_rows // block_len, query_add_block, zero_keys)
    shards = (
        lax.all_gather(queries.astype(jnp.float32), "sp", axis=0, tiled=True).astype(jnp.bfloat16),
        lax.all_gather(grad_flat.astype(jnp.float32), "sp", axis=0, tiled=True).astype(
            jnp.bfloat16
        ),
        lax.all_gather(log_sums, "sp", axis=0, tiled=True),
        lax.all_gather(term_flat, "sp", axis=0, tiled=True),
    )
    query_piece = shards[0]
    grad_piece = shards[1]
    log_piece = shards[2]
    term_piece = shards[3]
    piece_rows = query_piece.shape[0]
    key_block_len = block_span()

    def key_add_block(block_idx, partial_value):
        begin_row = block_idx * key_block_len
        query_block = lax.dynamic_slice_in_dim(query_piece, begin_row, key_block_len, 0).reshape(
            key_block_len, head_count, 2, -1
        )
        grad_block = lax.dynamic_slice_in_dim(grad_piece, begin_row, key_block_len, 0).reshape(
            key_block_len, head_count, -1
        )
        log_block = lax.dynamic_slice_in_dim(log_piece, begin_row, key_block_len, 0).reshape(
            key_block_len, head_count, 2
        )
        term_block = lax.dynamic_slice_in_dim(term_piece, begin_row, key_block_len, 0).reshape(
            key_block_len, head_count, 2
        )
        query_pos = begin_row + jnp.arange(key_block_len, dtype=jnp.int32)

        def key_compute(sums):
            weights, dscore = block_terms(
                query_block,
                key_heads,
                value_heads,
                grad_block,
                log_block,
                term_block,
                lambdas,
                query_pos,
                own_pos,
            )
            key_sum = sums[0] + jnp.einsum(
                "hcqk,qhcd->khcd", dscore, query_block, preferred_element_type=jnp.float32
            )
            value_sum = sums[1] + jnp.einsum(
                "hqk,qhe->khe", weights, grad_block, preferred_element_type=jnp.float32
            )
            return (key_sum, value_sum)

        return lax.cond(
            begin_row + key_block_len - 1 >= offset, key_compute, lambda sums: sums, partial_value
        )

    key_grad, value_grad = lax.fori_loop(
        0, piece_rows // key_block_len, key_add_block, (zero_keys, zero_values)
    )
    value_flat = value_grad.reshape(tok_rows, -1)
    value_narrow = value_flat.astype(jnp.bfloat16)
    weight_grad = lax.psum_scatter(
        lax.dot_general(
            gathered, value_narrow, (((0,), (0,)), ((), ())), preferred_element_type=jnp.float32
        ),
        "sp",
        scatter_dimension=0,
        tiled=True,
    )
    return (
        query_grad.reshape(tok_rows, -1),
        key_grad.reshape(tok_rows, -1),
        value_flat,
        weight_grad,
    )


LOG2E = 1.4426950408889634
AUX_ROWS = 32
SLOTS = 10
LANES = 128


def nt(a, b):
    return lax.dot_general(a, b, (((1,), (1,)), ((), ())), preferred_element_type=jnp.float32)


def tn(a, b):
    return lax.dot_general(a, b, (((0,), (0,)), ((), ())), preferred_element_type=jnp.float32)


def level_bits():
    place = lax.axis_index("sp")
    return place % 2, (place // 2) % 2, (place // 4) % 2


def split_pieces(rows):
    high = rows.astype(jnp.bfloat16)
    rest = rows - high.astype(jnp.float32)
    middle = rest.astype(jnp.bfloat16)
    low = (rest - middle.astype(jnp.float32)).astype(jnp.bfloat16)
    return high, middle, low


def prep_kernel(q_ref, k_ref, log_ref, pair_ref, cot_ref, lam_ref, gain_ref, grad_ref, aux_ref, px_ref, pz_ref, pm_ref):
    rows = q_ref.shape[0]
    half = rows // 2
    bit0, bit1, bit2 = level_bits()
    lane = lax.broadcasted_iota(jnp.int32, (rows, LANES), 1)
    aux_blocks = []
    for h in range(2):
        first = pair_ref[:, 2 * h * LANES : (2 * h + 1) * LANES].astype(jnp.float32)
        second = pair_ref[:, (2 * h + 1) * LANES : (2 * h + 2) * LANES].astype(jnp.float32)
        lam = lam_ref[h]
        merged = first - lam * second
        inv = lax.rsqrt(jnp.mean(merged * merged, axis=-1, keepdims=True) + norm_floor)
        scaled = cot_ref[:, h * LANES : (h + 1) * LANES].astype(jnp.float32) * gain_ref[...]
        inner = jnp.mean(scaled * merged, axis=-1, keepdims=True)
        grad = (inv * scaled - merged * (inv * inv * inv) * inner).astype(jnp.bfloat16)
        grad_ref[:, h * LANES : (h + 1) * LANES] = grad
        wide = grad.astype(jnp.float32)
        term0 = jnp.sum(wide * first, axis=-1, keepdims=True)
        term1 = jnp.sum(wide * second, axis=-1, keepdims=True)
        terms = jnp.where(lane == 2, term0, jnp.where(lane == 3, term1, 0.0))
        turned = jnp.concatenate(
            [jnp.transpose(terms[i * LANES : (i + 1) * LANES])[0:8] for i in range(rows // LANES)], axis=1
        )
        log0 = log_ref[2 * h : 2 * h + 1, :] * LOG2E
        log1 = (log_ref[2 * h + 1 : 2 * h + 2, :] - jnp.log(jnp.full((1, rows), lam, jnp.float32))) * LOG2E
        aux = jnp.concatenate([log0, log1, turned[2:4], jnp.zeros((4, rows), jnp.float32)], axis=0)
        aux_ref[h * 8 : (h + 1) * 8, :] = aux
        pieces = split_pieces(aux)
        wide_rows = jnp.concatenate([p.astype(jnp.float32)[0:4] for p in pieces] + [jnp.zeros((4, rows), jnp.float32)], axis=0)
        aux_blocks.append(wide_rows.astype(jnp.bfloat16))

    def put(ref, lane0, early, head_k, head_q):

        @pl.when(early)
        def _():
            ref[0:rows, lane0 : lane0 + LANES] = k_ref[:, head_k * LANES : (head_k + 1) * LANES]
            ref[0:rows, lane0 + LANES : lane0 + 2 * LANES] = k_ref[:, head_k * LANES : (head_k + 1) * LANES]

        @pl.when(jnp.logical_not(early))
        def _():
            ref[0:rows, lane0 : lane0 + LANES] = q_ref[:, head_q * LANES : (head_q + 1) * LANES]
            ref[0:rows, lane0 + LANES : lane0 + 2 * LANES] = grad_ref[:, head_q * LANES : (head_q + 1) * LANES]

    def put_aux(ref, lane0, h):
        ref[rows : rows + 16, lane0 : lane0 + half] = aux_blocks[h][:, 0:half]
        ref[rows + 16 : rows + 32, lane0 : lane0 + half] = aux_blocks[h][:, half:rows]

    put(px_ref, 0, bit0 == 0, 1, 0)
    px_ref[0:rows, 2 * LANES : 3 * LANES] = q_ref[:, LANES : 2 * LANES]
    px_ref[0:rows, 3 * LANES : 4 * LANES] = grad_ref[:, LANES : 2 * LANES]
    px_ref[0:rows, 4 * LANES : 5 * LANES] = k_ref[:, 0:LANES]
    px_ref[rows : rows + 32, 4 * LANES : 5 * LANES] = jnp.zeros((32, LANES), jnp.bfloat16)
    put_aux(px_ref, 0, 0)
    put_aux(px_ref, half, 1)
    put(pz_ref, 0, bit1 == 0, 1, 0)
    put_aux(pz_ref, 0, 0)
    put(pm_ref, 0, bit2 == 0, 1, 0)
    put_aux(pm_ref, 0, 0)


def value_kernel(own_ref, far_ref, near_ref, next_ref, w_ref, out_ref, second_ref):
    cols = own_ref.shape[1]
    place = lax.axis_index("tp")

    def part(x, spot):
        return jnp.dot(x, w_ref[pl.ds(spot * cols, cols), :], preferred_element_type=jnp.float32)

    total = part(own_ref[...], place) + part(far_ref[...], (place + 2) % 4)
    near = place + 1 - 2 * (place % 2)
    total += part(near_ref[...], near) + part(next_ref[...], (near + 2) % 4)
    out_ref[...] = total.astype(jnp.bfloat16)
    second_ref[...] = total[:, LANES : 2 * LANES].astype(jnp.bfloat16)


def weight_kernel(own_ref, far_ref, near_ref, next_ref, dv0_ref, ux_ref, uz_ref, u4_ref, u6_ref, out_ref, dv_ref, narrow_ref):
    bits = level_bits()
    cols = own_ref.shape[1]
    place = lax.axis_index("tp")
    near = place + 1 - 2 * (place % 2)
    dv_ref[:, 0:LANES] = dv0_ref[0] + ux_ref[:, 0:LANES].astype(jnp.float32)
    dv_ref[:, LANES : 2 * LANES] = dv0_ref[1]
    for ref, lane0, bit in ((ux_ref, LANES, bits[0]), (uz_ref, 0, bits[1]), (u4_ref, 0, bits[2]), (u6_ref, 0, bits[2])):

        @pl.when(bit == 0)
        def _(ref=ref, lane0=lane0):
            dv_ref[:, LANES : 2 * LANES] += ref[:, lane0 : lane0 + LANES].astype(jnp.float32)

    narrow_ref[...] = dv_ref[...].astype(jnp.bfloat16)
    grad = narrow_ref[...]
    size = out_ref.shape[3]
    for ref, spot in ((own_ref, place), (far_ref, (place + 2) % 4), (near_ref, near), (next_ref, (near + 2) % 4)):
        block = tn(grad, ref[...]).astype(jnp.bfloat16)
        for i in range(cols // size):
            part = spot * (cols // size) + i
            out_ref[part % 4, part // 4] = block[:, i * size : (i + 1) * size]


def fold_kernel(pieces_ref, keep_ref, send_ref):
    bit = lax.axis_index("sp") // 4
    for ref, spot in ((keep_ref, bit), (send_ref, 1 - bit)):
        total = pieces_ref[0, spot].astype(jnp.float32)
        for i in range(1, pieces_ref.shape[0]):
            total += pieces_ref[i, spot].astype(jnp.float32)
        ref[...] = jnp.transpose(total).astype(ref.dtype)


def join_pieces(block_ref, rows, lane0):
    half = rows // 2
    parts = [block_ref[rows + 16 * i : rows + 16 * (i + 1), lane0 : lane0 + half].astype(jnp.float32) for i in range(2)]
    sums = [p[0:4] + p[4:8] + p[8:12] for p in parts]
    return jnp.concatenate(sums, axis=1)


SCALE = LOG2E / 8.0


def halves(x):
    left = lax.broadcasted_iota(jnp.int32, (1, LANES), 1) < LANES // 2
    none = jnp.zeros((), x.dtype)
    return jnp.where(left, x, none), jnp.where(left, none, x)


def fill_slots(q_ref, k_ref, grad_ref, aux_ref, received, a_ref, b_ref, aux_all):
    rows = q_ref.shape[0]
    for h in range(2):
        a_ref[h] = q_ref[:, h * LANES : (h + 1) * LANES]
        b_ref[h] = grad_ref[:, h * LANES : (h + 1) * LANES]
        a_ref[2 + h] = k_ref[:, h * LANES : (h + 1) * LANES]
        aux_all[h, 0:4, :] = aux_ref[8 * h : 8 * h + 4, :]
    for i, ref in enumerate(received):
        a_ref[4 + i] = ref[0:rows, 0:LANES]
        b_ref[4 + i] = ref[0:rows, LANES : 2 * LANES]
        aux_all[4 + i, 0:4, :] = join_pieces(ref, rows, 0)
    rx_ref = received[0]
    a_ref[9] = rx_ref[0:rows, 2 * LANES : 3 * LANES]
    b_ref[9] = rx_ref[0:rows, 3 * LANES : 4 * LANES]
    aux_all[9, 0:4, :] = join_pieces(rx_ref, rows, rows // 2)
    a_ref[8] = rx_ref[0:rows, 4 * LANES : 5 * LANES]


def maps_of(buf, aux, masked):
    map0 = jnp.exp2(buf[0] * SCALE - aux[0:1])
    map1 = jnp.exp2(buf[1] * SCALE - aux[1:2])
    if masked:
        key_pos = lax.broadcasted_iota(jnp.int32, map0.shape, 0)
        query_pos = lax.broadcasted_iota(jnp.int32, map0.shape, 1)
        seen = key_pos <= query_pos
        map0 = jnp.where(seen, map0, 0.0)
        map1 = jnp.where(seen, map1, 0.0)
    return map0, map1


def pick(u):
    bits = level_bits()
    level = jnp.where(u == 0, 0, jnp.where(u < 3, 1, 2))
    bit = jnp.where(level == 0, bits[0], jnp.where(level == 1, bits[1], bits[2]))
    other = 4 + (u + 1) // 2
    own = (u == 0) | (u % 2 == 1)
    return jnp.where(bit == 0, other, jnp.where(own, 1, 9)), jnp.where(bit == 0, jnp.where(own, 2, 8), other)


def each_unit(products, consume, buf0, buf1):
    products(*pick(0), buf0)

    def two_units(i, carry):
        products(*pick(2 * i + 1), buf1)
        consume(*pick(2 * i), buf0, False)
        products(*pick(2 * i + 2), buf0)
        consume(*pick(2 * i + 1), buf1, False)
        return carry

    lax.fori_loop(0, 3, two_units, 0)
    products(0, 2, buf1)
    consume(*pick(6), buf0, False)
    products(1, 3, buf0)
    consume(0, 2, buf1, True)
    consume(1, 3, buf0, True)


def mixed_kernel(
    q_ref, k_ref, grad_ref, aux_ref, rx_ref, rz_ref, r4_ref, r6_ref,
    dv_ref, tx_ref, tz_ref, t4_ref, t6_ref, a_ref, b_ref, aux_all, s_ref, buf0, buf1,
):
    fill_slots(q_ref, k_ref, grad_ref, aux_ref, (rx_ref, rz_ref, r4_ref, r6_ref), a_ref, b_ref, aux_all)
    s_ref[...] = jnp.zeros(s_ref.shape, jnp.float32)

    def products(qs, ks, buf):
        query0, query1 = halves(a_ref[qs])
        key = a_ref[ks]
        buf[0] = nt(key, query0)
        buf[1] = nt(key, query1)

    def consume(qs, ks, buf, masked):
        map0, map1 = maps_of(buf, aux_all[qs], masked)
        mixed = (map0 - map1).astype(jnp.bfloat16)
        s_ref[ks] += jnp.dot(mixed, b_ref[qs], preferred_element_type=jnp.float32)

    each_unit(products, consume, buf0, buf1)
    dv_ref[...] = s_ref[2:4]
    tx_ref[:, 0:LANES] = s_ref[8].astype(jnp.bfloat16)
    tx_ref[:, LANES : 2 * LANES] = s_ref[4].astype(jnp.bfloat16)
    for ref, slot in ((tz_ref, 5), (t4_ref, 6), (t6_ref, 7)):
        ref[...] = s_ref[slot].astype(jnp.bfloat16)


def score_kernel(
    q_ref, k_ref, grad_ref, aux_ref, rx_ref, rz_ref, r4_ref, r6_ref, v_ref, vx_ref, vz_ref, v4_ref, v6_ref,
    own_ref, tx_ref, tz_ref, t4_ref, t6_ref, a_ref, b_ref, aux_all, s_ref, buf0, buf1,
):
    rows = q_ref.shape[0]
    bits = level_bits()
    fill_slots(q_ref, k_ref, grad_ref, aux_ref, (rx_ref, rz_ref, r4_ref, r6_ref), a_ref, b_ref, aux_all)
    for h in range(2):
        b_ref[2 + h] = v_ref[:, h * LANES : (h + 1) * LANES]
    b_ref[8] = vx_ref[:, 0:LANES]
    for slot, ref, lane0, bit in ((4, vx_ref, LANES, bits[0]), (5, vz_ref, 0, bits[1]), (6, v4_ref, 0, bits[2]), (7, v6_ref, 0, bits[2])):

        @pl.when(bit != 0)
        def _(slot=slot, ref=ref, lane0=lane0):
            b_ref[slot] = ref[:, lane0 : lane0 + LANES]

    s_ref[...] = jnp.zeros(s_ref.shape, jnp.float32)

    def products(qs, ks, buf):
        query0, query1 = halves(a_ref[qs])
        key = a_ref[ks]
        buf[0] = nt(key, query0)
        buf[1] = nt(key, query1)
        buf[2] = nt(b_ref[ks], b_ref[qs])

    def consume(qs, ks, buf, masked):
        query0, query1 = halves(a_ref[qs])
        key0, key1 = halves(a_ref[ks])
        aux = aux_all[qs]
        map0, map1 = maps_of(buf, aux, masked)
        dots = buf[2]
        score0 = (map0 * (dots - aux[2:3])).astype(jnp.bfloat16)
        score1 = (map1 * (aux[3:4] - dots)).astype(jnp.bfloat16)
        s_ref[ks] += jnp.dot(score0, query0, preferred_element_type=jnp.float32) + jnp.dot(
            score1, query1, preferred_element_type=jnp.float32
        )
        turned = tn(key0, score0) + tn(key1, score1)
        for i in range(rows // LANES):
            s_ref[qs, i * LANES : (i + 1) * LANES, :] += turned[:, i * LANES : (i + 1) * LANES]

    each_unit(products, consume, buf0, buf1)
    own_ref[...] = s_ref[0:4]
    for i, slot in enumerate((4, 8, 9)):
        tx_ref[:, i * LANES : (i + 1) * LANES] = s_ref[slot].astype(jnp.bfloat16)
    for ref, slot in ((tz_ref, 5), (t4_ref, 6), (t6_ref, 7)):
        ref[...] = s_ref[slot].astype(jnp.bfloat16)


def join_kernel(own_ref, ux_ref, uz_ref, u4_ref, u6_ref, dq_ref, dk_ref, s_ref):
    bits = level_bits()
    for i in range(4):
        s_ref[i] = own_ref[i]
    s_ref[2] += ux_ref[:, LANES : 2 * LANES].astype(jnp.float32)
    s_ref[1] += ux_ref[:, 2 * LANES : 3 * LANES].astype(jnp.float32)
    for ref, bit in ((ux_ref, bits[0]), (uz_ref, bits[1]), (u4_ref, bits[2]), (u6_ref, bits[2])):
        spot = jnp.where(bit == 0, 3, 0)
        s_ref[spot] += ref[:, 0:LANES].astype(jnp.float32)
    for h in range(2):
        for i in range(s_ref.shape[1] // LANES):
            spot = slice(i * LANES, (i + 1) * LANES)
            dq_ref[spot, h * LANES : (h + 1) * LANES] = jnp.transpose(s_ref[h, spot, :]) * 0.125
        dk_ref[:, h * LANES : (h + 1) * LANES] = s_ref[2 + h] * 0.125


def call(kernel, outs, args, scratch=(), smem=(), micros=1):
    vmem = pl.BlockSpec(memory_space=pltpu.VMEM)
    specs = [pl.BlockSpec(memory_space=pltpu.SMEM) if i in smem else vmem for i in range(len(args))]
    return pl.pallas_call(
        kernel,
        out_shape=[jax.ShapeDtypeStruct(s, d) for s, d in outs],
        in_specs=specs,
        out_specs=[vmem] * len(outs),
        scratch_shapes=list(scratch),
        cost_estimate=pl.CostEstimate(flops=micros * 14_000_000, bytes_accessed=1_000_000, transcendentals=0),
    )(*args)


def swap(x, axis, size, mask):
    return lax.ppermute(x, axis, [(i, i ^ mask) for i in range(size)])


def paired_device(*args):
    return paired_steps(*args)


def paired_steps(queries, key_vectors, latents, w_value, log_sums, out_pair, cotangent, lambdas, out_gain):
    rows, width = queries.shape
    narrow, wide = jnp.bfloat16, jnp.float32
    seq, feat = lax.axis_size("sp"), lax.axis_size("tp")
    slot_shape = (rows, LANES)
    far = swap(latents, "tp", feat, 2)
    near = swap(latents, "tp", feat, 1)
    grad, aux, px, pz, pm = call(
        prep_kernel,
        [((rows, width), narrow), ((16, rows), wide), ((rows + AUX_ROWS, 5 * LANES), narrow),
         ((rows + AUX_ROWS, width), narrow), ((rows + AUX_ROWS, width), narrow)],
        (queries, key_vectors, log_sums.T, out_pair, cotangent, lambdas, out_gain[None, :]),
        smem=(5,), micros=4,
    )
    r4 = swap(pm, "sp", seq, 4)
    r6 = swap(r4, "sp", seq, 2)
    rz = swap(pz, "sp", seq, 2)
    rx = swap(px, "sp", seq, 1)
    next_far = swap(far, "tp", feat, 1)
    values, second = call(value_kernel, [((rows, width), narrow), (slot_shape, narrow)], (latents, far, near, next_far, w_value), micros=3)
    v4 = swap(second, "sp", seq, 4)
    v6 = swap(second, "sp", seq, 6)
    vz = swap(second, "sp", seq, 2)
    vx = swap(values, "sp", seq, 1)
    slots = [pltpu.VMEM((SLOTS,) + slot_shape, narrow), pltpu.VMEM((SLOTS,) + slot_shape, narrow),
             pltpu.VMEM((SLOTS, 8, rows), wide), pltpu.VMEM((SLOTS,) + slot_shape, wide)]
    shared = (queries, key_vectors, grad, aux, rx, rz, r4, r6)
    dv0, tx, tz, t4, t6 = call(
        mixed_kernel, [((2,) + slot_shape, wide), ((rows, 2 * LANES), narrow)] + [(slot_shape, narrow)] * 3,
        shared, scratch=slots + [pltpu.VMEM((2, rows, rows), wide)] * 2, micros=8,
    )
    u4 = swap(t4, "sp", seq, 4)
    u6 = swap(t6, "sp", seq, 6)
    uz = swap(tz, "sp", seq, 2)
    ux = swap(tx, "sp", seq, 1)
    own, sx, sz, s4, s6 = call(
        score_kernel, [((4,) + slot_shape, wide), ((rows, 3 * LANES), narrow)] + [(slot_shape, narrow)] * 3,
        shared + (values, vx, vz, v4, v6), scratch=slots + [pltpu.VMEM((3, rows, rows), wide)] * 2, micros=16,
    )
    part, dv, _ = call(
        weight_kernel, [((4, 2, width, latents.shape[1] * feat // seq), narrow), ((rows, width), wide), ((rows, width), narrow)],
        (latents, far, near, next_far, dv0, ux, uz, u4, u6), micros=5,
    )
    w4 = swap(s4, "sp", seq, 4)
    w6 = swap(s6, "sp", seq, 6)
    wz = swap(sz, "sp", seq, 2)
    wx = swap(sx, "sp", seq, 1)
    groups = [list(range(4)), list(range(4, 8))]
    pieces = lax.all_to_all(part, "sp", 0, 0, axis_index_groups=groups)
    keep, send = call(fold_kernel, [(part.shape[:1:-1], wide), (part.shape[:1:-1], narrow)], (pieces,), micros=1)
    last = swap(send, "sp", seq, 4)
    dq, dk = call(
        join_kernel, [((rows, width), wide)] * 2, (own, wx, wz, w4, w6),
        scratch=[pltpu.VMEM((4,) + slot_shape, wide)], micros=3,
    )
    return dq, dk, dv, keep + last.astype(wide)


def solution(mesh):
    paired = (mesh.shape["sp"], mesh.shape["tp"]) == (8, 4)
    return jax.shard_map(
        paired_device if paired else general_device,
        mesh=mesh,
        in_specs=(
            P("sp", "tp"),
            P("sp", "tp"),
            P("sp", "tp"),
            P(None, "tp"),
            P("sp", "tp"),
            P("sp", "tp"),
            P("sp", "tp"),
            P("tp"),
            P(),
        ),
        out_specs=(P("sp", "tp"), P("sp", "tp"), P("sp", "tp"), P("sp", "tp")),
        check_vma=False,
    )
```

```python
import jax
import jax.numpy as jnp
from jax import lax
from jax.experimental import pallas as pl
from jax.experimental.pallas import tpu as pltpu
from jax.sharding import PartitionSpec as P


norm_floor = 0.25
block_rows = 512


def head_cotangent(out_pair, cotangent, lambdas, out_gain):
    tok_rows = out_pair.shape[0]
    head_count = lambdas.shape[0]
    out_maps = out_pair.astype(jnp.float32).reshape(tok_rows, head_count, 2, -1)
    lam_cols = lambdas[None, :, None]
    merged = out_maps[:, :, 0] - lam_cols * out_maps[:, :, 1]
    inv_norm = lax.rsqrt(jnp.mean(merged * merged, axis=-1, keepdims=True) + norm_floor)
    scaled = cotangent.astype(jnp.float32).reshape(merged.shape) * out_gain
    inner_dot = jnp.mean(scaled * merged, axis=-1, keepdims=True)
    out_grad = (inv_norm * scaled - merged * (inv_norm * inv_norm * inv_norm) * inner_dot).astype(
        jnp.bfloat16
    )
    grad_wide = out_grad.astype(jnp.float32)
    first_map = jnp.sum(grad_wide * out_maps[:, :, 0], axis=-1)
    second_map = -lambdas[None, :] * jnp.sum(grad_wide * out_maps[:, :, 1], axis=-1)
    return (out_grad, jnp.stack([first_map, second_map], axis=-1))


def block_terms(
    query_block,
    key_block,
    value_block,
    grad_block,
    log_block,
    term_block,
    lambdas,
    query_pos,
    key_pos,
):
    factor = query_block.shape[-1] ** (-0.5)
    scores = (
        jnp.einsum("qhcd,khcd->hcqk", query_block, key_block, preferred_element_type=jnp.float32)
        * factor
    )
    visible = key_pos[None, :] <= query_pos[:, None]
    shifted = scores - jnp.transpose(log_block, (1, 2, 0))[..., None]
    softmax_maps = jnp.where(visible, jnp.exp(shifted), 0.0)
    value_dot = jnp.einsum(
        "qhe,khe->hqk", grad_block, value_block, preferred_element_type=jnp.float32
    )
    lam_cols = lambdas[:, None, None]
    weights = (softmax_maps[:, 0] - lam_cols * softmax_maps[:, 1]).astype(jnp.bfloat16)
    term_cols = jnp.transpose(term_block, (1, 2, 0))
    first_map = softmax_maps[:, 0] * (value_dot - term_cols[:, 0, :, None])
    second_map = softmax_maps[:, 1] * (-lam_cols * value_dot - term_cols[:, 1, :, None])
    dscore = (jnp.stack([first_map, second_map], axis=1) * factor).astype(jnp.bfloat16)
    return (weights, dscore)


def block_span():
    return block_rows


def general_device(
    queries, key_vectors, latents, w_value, log_sums, out_pair, cotangent, lambdas, out_gain
):
    tok_rows = queries.shape[0]
    head_count = lambdas.shape[0]
    offset = lax.axis_index("sp") * tok_rows
    own_pos = offset + jnp.arange(tok_rows, dtype=jnp.int32)
    last_pos = offset + tok_rows - 1
    gathered = lax.all_gather(latents, "tp", axis=1, tiled=True)
    values = jnp.dot(gathered, w_value, preferred_element_type=jnp.float32).astype(jnp.bfloat16)
    out_grad, row_terms = head_cotangent(out_pair, cotangent, lambdas, out_gain)
    query_heads = queries.reshape(tok_rows, head_count, 2, -1)
    key_heads = key_vectors.reshape(tok_rows, head_count, 2, -1)
    value_heads = values.reshape(tok_rows, head_count, -1)
    log_heads = log_sums.reshape(tok_rows, head_count, 2)
    grad_flat = out_grad.reshape(tok_rows, -1)
    term_flat = row_terms.reshape(tok_rows, -1)
    zero_keys = jnp.zeros(key_heads.shape, jnp.float32)
    zero_values = jnp.zeros(value_heads.shape, jnp.float32)
    shards = (
        lax.all_gather(key_vectors, "sp", axis=0, tiled=True),
        lax.all_gather(values, "sp", axis=0, tiled=True),
    )
    key_piece = shards[0]
    value_piece = shards[1]
    piece_rows = key_piece.shape[0]
    block_len = block_span()

    def query_add_block(block_idx, partial_value):
        begin_row = block_idx * block_len
        key_block = lax.dynamic_slice_in_dim(key_piece, begin_row, block_len, 0).reshape(
            block_len, head_count, 2, -1
        )
        value_block = lax.dynamic_slice_in_dim(value_piece, begin_row, block_len, 0).reshape(
            block_len, head_count, -1
        )
        key_pos = begin_row + jnp.arange(block_len, dtype=jnp.int32)

        def query_compute(sums):
            _, dscore = block_terms(
                query_heads,
                key_block,
                value_block,
                out_grad,
                log_heads,
                row_terms,
                lambdas,
                own_pos,
                key_pos,
            )
            return sums + jnp.einsum(
                "hcqk,khcd->qhcd", dscore, key_block, preferred_element_type=jnp.float32
            )

        return lax.cond(begin_row <= last_pos, query_compute, lambda sums: sums, partial_value)

    query_grad = lax.fori_loop(0, piece_rows // block_len, query_add_block, zero_keys)
    shards = (
        lax.all_gather(queries.astype(jnp.float32), "sp", axis=0, tiled=True).astype(jnp.bfloat16),
        lax.all_gather(grad_flat.astype(jnp.float32), "sp", axis=0, tiled=True).astype(
            jnp.bfloat16
        ),
        lax.all_gather(log_sums, "sp", axis=0, tiled=True),
        lax.all_gather(term_flat, "sp", axis=0, tiled=True),
    )
    query_piece = shards[0]
    grad_piece = shards[1]
    log_piece = shards[2]
    term_piece = shards[3]
    piece_rows = query_piece.shape[0]
    key_block_len = block_span()

    def key_add_block(block_idx, partial_value):
        begin_row = block_idx * key_block_len
        query_block = lax.dynamic_slice_in_dim(query_piece, begin_row, key_block_len, 0).reshape(
            key_block_len, head_count, 2, -1
        )
        grad_block = lax.dynamic_slice_in_dim(grad_piece, begin_row, key_block_len, 0).reshape(
            key_block_len, head_count, -1
        )
        log_block = lax.dynamic_slice_in_dim(log_piece, begin_row, key_block_len, 0).reshape(
            key_block_len, head_count, 2
        )
        term_block = lax.dynamic_slice_in_dim(term_piece, begin_row, key_block_len, 0).reshape(
            key_block_len, head_count, 2
        )
        query_pos = begin_row + jnp.arange(key_block_len, dtype=jnp.int32)

        def key_compute(sums):
            weights, dscore = block_terms(
                query_block,
                key_heads,
                value_heads,
                grad_block,
                log_block,
                term_block,
                lambdas,
                query_pos,
                own_pos,
            )
            key_sum = sums[0] + jnp.einsum(
                "hcqk,qhcd->khcd", dscore, query_block, preferred_element_type=jnp.float32
            )
            value_sum = sums[1] + jnp.einsum(
                "hqk,qhe->khe", weights, grad_block, preferred_element_type=jnp.float32
            )
            return (key_sum, value_sum)

        return lax.cond(
            begin_row + key_block_len - 1 >= offset, key_compute, lambda sums: sums, partial_value
        )

    key_grad, value_grad = lax.fori_loop(
        0, piece_rows // key_block_len, key_add_block, (zero_keys, zero_values)
    )
    value_flat = value_grad.reshape(tok_rows, -1)
    value_narrow = value_flat.astype(jnp.bfloat16)
    weight_grad = lax.psum_scatter(
        lax.dot_general(
            gathered, value_narrow, (((0,), (0,)), ((), ())), preferred_element_type=jnp.float32
        ),
        "sp",
        scatter_dimension=0,
        tiled=True,
    )
    return (
        query_grad.reshape(tok_rows, -1),
        key_grad.reshape(tok_rows, -1),
        value_flat,
        weight_grad,
    )


LOG2E = 1.4426950408889634
AUX_ROWS = 32
SLOTS = 10
LANES = 128


def nt(a, b):
    return lax.dot_general(a, b, (((1,), (1,)), ((), ())), preferred_element_type=jnp.float32)


def tn(a, b):
    return lax.dot_general(a, b, (((0,), (0,)), ((), ())), preferred_element_type=jnp.float32)


def level_bits():
    place = lax.axis_index("sp")
    return place % 2, (place // 2) % 2, (place // 4) % 2


def split_pieces(rows):
    high = rows.astype(jnp.bfloat16)
    rest = rows - high.astype(jnp.float32)
    middle = rest.astype(jnp.bfloat16)
    low = (rest - middle.astype(jnp.float32)).astype(jnp.bfloat16)
    return high, middle, low


def prep_kernel(q_ref, k_ref, log_ref, pair_ref, cot_ref, lam_ref, gain_ref, grad_ref, aux_ref, px_ref, pz_ref, pm_ref):
    rows = q_ref.shape[0]
    half = rows // 2
    bit0, bit1, bit2 = level_bits()
    lane = lax.broadcasted_iota(jnp.int32, (rows, LANES), 1)
    aux_blocks = []
    for h in range(2):
        first = pair_ref[:, 2 * h * LANES : (2 * h + 1) * LANES].astype(jnp.float32)
        second = pair_ref[:, (2 * h + 1) * LANES : (2 * h + 2) * LANES].astype(jnp.float32)
        lam = lam_ref[h]
        merged = first - lam * second
        inv = lax.rsqrt(jnp.mean(merged * merged, axis=-1, keepdims=True) + norm_floor)
        scaled = cot_ref[:, h * LANES : (h + 1) * LANES].astype(jnp.float32) * gain_ref[...]
        inner = jnp.mean(scaled * merged, axis=-1, keepdims=True)
        grad = (inv * scaled - merged * (inv * inv * inv) * inner).astype(jnp.bfloat16)
        grad_ref[:, h * LANES : (h + 1) * LANES] = grad
        wide = grad.astype(jnp.float32)
        term0 = jnp.sum(wide * first, axis=-1, keepdims=True)
        term1 = jnp.sum(wide * second, axis=-1, keepdims=True)
        terms = jnp.where(lane == 2, term0, jnp.where(lane == 3, term1, 0.0))
        turned = jnp.concatenate(
            [jnp.transpose(terms[i * LANES : (i + 1) * LANES])[0:8] for i in range(rows // LANES)], axis=1
        )
        log0 = log_ref[2 * h : 2 * h + 1, :] * LOG2E
        log1 = (log_ref[2 * h + 1 : 2 * h + 2, :] - jnp.log(jnp.full((1, rows), lam, jnp.float32))) * LOG2E
        aux = jnp.concatenate([log0, log1, turned[2:4], jnp.zeros((4, rows), jnp.float32)], axis=0)
        aux_ref[h * 8 : (h + 1) * 8, :] = aux
        pieces = split_pieces(aux)
        wide_rows = jnp.concatenate([p.astype(jnp.float32)[0:4] for p in pieces] + [jnp.zeros((4, rows), jnp.float32)], axis=0)
        aux_blocks.append(wide_rows.astype(jnp.bfloat16))

    def put(ref, lane0, early, head_k, head_q):

        @pl.when(early)
        def _():
            ref[0:rows, lane0 : lane0 + LANES] = k_ref[:, head_k * LANES : (head_k + 1) * LANES]
            ref[0:rows, lane0 + LANES : lane0 + 2 * LANES] = k_ref[:, head_k * LANES : (head_k + 1) * LANES]

        @pl.when(jnp.logical_not(early))
        def _():
            ref[0:rows, lane0 : lane0 + LANES] = q_ref[:, head_q * LANES : (head_q + 1) * LANES]
            ref[0:rows, lane0 + LANES : lane0 + 2 * LANES] = grad_ref[:, head_q * LANES : (head_q + 1) * LANES]

    def put_aux(ref, lane0, h):
        ref[rows : rows + 16, lane0 : lane0 + half] = aux_blocks[h][:, 0:half]
        ref[rows + 16 : rows + 32, lane0 : lane0 + half] = aux_blocks[h][:, half:rows]

    put(px_ref, 0, bit0 == 0, 1, 0)
    px_ref[0:rows, 2 * LANES : 3 * LANES] = q_ref[:, LANES : 2 * LANES]
    px_ref[0:rows, 3 * LANES : 4 * LANES] = grad_ref[:, LANES : 2 * LANES]
    px_ref[0:rows, 4 * LANES : 5 * LANES] = k_ref[:, 0:LANES]
    px_ref[rows : rows + 32, 4 * LANES : 5 * LANES] = jnp.zeros((32, LANES), jnp.bfloat16)
    put_aux(px_ref, 0, 0)
    put_aux(px_ref, half, 1)
    put(pz_ref, 0, bit1 == 0, 1, 0)
    put_aux(pz_ref, 0, 0)
    put(pm_ref, 0, bit2 == 0, 1, 0)
    put_aux(pm_ref, 0, 0)


def value_kernel(own_ref, far_ref, near_ref, next_ref, w_ref, out_ref):
    cols = own_ref.shape[1]
    place = lax.axis_index("tp")

    def part(x, spot):
        return jnp.dot(x, w_ref[pl.ds(spot * cols, cols), :], preferred_element_type=jnp.float32)

    total = part(own_ref[...], place) + part(far_ref[...], (place + 2) % 4)
    near = place + 1 - 2 * (place % 2)
    total += part(near_ref[...], near) + part(next_ref[...], (near + 2) % 4)
    out_ref[...] = total.astype(jnp.bfloat16)


def weight_kernel(own_ref, far_ref, near_ref, next_ref, dv0_ref, ux_ref, uz_ref, u4_ref, u6_ref, out_ref, dv_ref, narrow_ref):
    bits = level_bits()
    cols = own_ref.shape[1]
    place = lax.axis_index("tp")
    near = place + 1 - 2 * (place % 2)
    dv_ref[:, 0:LANES] = dv0_ref[0] + ux_ref[:, LANES : 2 * LANES].astype(jnp.float32)
    dv_ref[:, LANES : 2 * LANES] = dv0_ref[1]
    for ref, lane0, bit in ((ux_ref, 2 * LANES, bits[0]), (uz_ref, 0, bits[1]), (u4_ref, 0, bits[2]), (u6_ref, 0, bits[2])):

        @pl.when(bit == 0)
        def _(ref=ref, lane0=lane0):
            dv_ref[:, LANES : 2 * LANES] += ref[:, lane0 : lane0 + LANES].astype(jnp.float32)

    narrow_ref[...] = dv_ref[...].astype(jnp.bfloat16)
    grad = narrow_ref[...]
    size = out_ref.shape[3]
    for ref, spot in ((own_ref, place), (far_ref, (place + 2) % 4), (near_ref, near), (next_ref, (near + 2) % 4)):
        block = tn(grad, ref[...]).astype(jnp.bfloat16)
        for i in range(cols // size):
            part = spot * (cols // size) + i
            out_ref[part % 4, part // 4] = block[:, i * size : (i + 1) * size]


def fold_kernel(pieces_ref, keep_ref, send_ref):
    bit = lax.axis_index("sp") // 4
    for ref, spot in ((keep_ref, bit), (send_ref, 1 - bit)):
        total = pieces_ref[0, spot].astype(jnp.float32)
        for i in range(1, pieces_ref.shape[0]):
            total += pieces_ref[i, spot].astype(jnp.float32)
        ref[...] = jnp.transpose(total).astype(ref.dtype)


def join_pieces(block_ref, rows, lane0):
    half = rows // 2
    parts = [block_ref[rows + 16 * i : rows + 16 * (i + 1), lane0 : lane0 + half].astype(jnp.float32) for i in range(2)]
    sums = [p[0:4] + p[4:8] + p[8:12] for p in parts]
    return jnp.concatenate(sums, axis=1)


SCALE = LOG2E / 8.0


def halves(x):
    left = lax.broadcasted_iota(jnp.int32, (1, LANES), 1) < LANES // 2
    none = jnp.zeros((), x.dtype)
    return jnp.where(left, x, none), jnp.where(left, none, x)


def fill_slots(q_ref, k_ref, grad_ref, aux_ref, received, a_ref, b_ref, aux_all):
    rows = q_ref.shape[0]
    for h in range(2):
        a_ref[h] = q_ref[:, h * LANES : (h + 1) * LANES]
        b_ref[h] = grad_ref[:, h * LANES : (h + 1) * LANES]
        a_ref[2 + h] = k_ref[:, h * LANES : (h + 1) * LANES]
        aux_all[h, 0:4, :] = aux_ref[8 * h : 8 * h + 4, :]
    for i, ref in enumerate(received):
        a_ref[4 + i] = ref[0:rows, 0:LANES]
        b_ref[4 + i] = ref[0:rows, LANES : 2 * LANES]
        aux_all[4 + i, 0:4, :] = join_pieces(ref, rows, 0)
    rx_ref = received[0]
    a_ref[9] = rx_ref[0:rows, 2 * LANES : 3 * LANES]
    b_ref[9] = rx_ref[0:rows, 3 * LANES : 4 * LANES]
    aux_all[9, 0:4, :] = join_pieces(rx_ref, rows, rows // 2)
    a_ref[8] = rx_ref[0:rows, 4 * LANES : 5 * LANES]


def maps_of(buf, aux, masked):
    map0 = jnp.exp2(buf[0] * SCALE - aux[0:1])
    map1 = jnp.exp2(buf[1] * SCALE - aux[1:2])
    if masked:
        key_pos = lax.broadcasted_iota(jnp.int32, map0.shape, 0)
        query_pos = lax.broadcasted_iota(jnp.int32, map0.shape, 1)
        seen = key_pos <= query_pos
        map0 = jnp.where(seen, map0, 0.0)
        map1 = jnp.where(seen, map1, 0.0)
    return map0, map1


def pick(u):
    bits = level_bits()
    level = jnp.where(u == 0, 0, jnp.where(u < 3, 1, 2))
    bit = jnp.where(level == 0, bits[0], jnp.where(level == 1, bits[1], bits[2]))
    other = 4 + (u + 1) // 2
    own = (u == 0) | (u % 2 == 1)
    return jnp.where(bit == 0, other, jnp.where(own, 1, 9)), jnp.where(bit == 0, jnp.where(own, 2, 8), other)


def each_unit(products, consume, buf0, buf1):
    products(*pick(0), buf0)

    def two_units(i, carry):
        products(*pick(2 * i + 1), buf1)
        consume(*pick(2 * i), buf0, False)
        products(*pick(2 * i + 2), buf0)
        consume(*pick(2 * i + 1), buf1, False)
        return carry

    lax.fori_loop(0, 3, two_units, 0)
    products(0, 2, buf1)
    consume(*pick(6), buf0, False)
    products(1, 3, buf0)
    consume(0, 2, buf1, True)
    consume(1, 3, buf0, True)


def mixed_kernel(
    q_ref, k_ref, grad_ref, aux_ref, rx_ref, rz_ref, r4_ref, r6_ref, v_ref,
    dv_ref, tx_ref, tz_ref, t4_ref, t6_ref, a_ref, b_ref, aux_all, s_ref, buf0, buf1,
):
    fill_slots(q_ref, k_ref, grad_ref, aux_ref, (rx_ref, rz_ref, r4_ref, r6_ref), a_ref, b_ref, aux_all)
    s_ref[...] = jnp.zeros(s_ref.shape, jnp.float32)

    def products(qs, ks, buf):
        query0, query1 = halves(a_ref[qs])
        key = a_ref[ks]
        buf[0] = nt(key, query0)
        buf[1] = nt(key, query1)

    def consume(qs, ks, buf, masked):
        map0, map1 = maps_of(buf, aux_all[qs], masked)
        mixed = (map0 - map1).astype(jnp.bfloat16)
        s_ref[ks] += jnp.dot(mixed, b_ref[qs], preferred_element_type=jnp.float32)

    each_unit(products, consume, buf0, buf1)
    dv_ref[...] = s_ref[2:4]
    tx_ref[:, 0:LANES] = v_ref[:, 0:LANES]
    tx_ref[:, LANES : 2 * LANES] = s_ref[8].astype(jnp.bfloat16)
    bits = level_bits()
    for ref, lane0, slot, bit in ((tx_ref, 2 * LANES, 4, bits[0]), (tz_ref, 0, 5, bits[1]), (t4_ref, 0, 6, bits[2]), (t6_ref, 0, 7, bits[2])):

        @pl.when(bit == 0)
        def _(ref=ref, lane0=lane0):
            ref[:, lane0 : lane0 + LANES] = v_ref[:, LANES : 2 * LANES]

        @pl.when(bit != 0)
        def _(ref=ref, lane0=lane0, slot=slot):
            ref[:, lane0 : lane0 + LANES] = s_ref[slot].astype(jnp.bfloat16)


def score_kernel(
    q_ref, k_ref, grad_ref, aux_ref, rx_ref, rz_ref, r4_ref, r6_ref, v_ref, vx_ref, vz_ref, v4_ref, v6_ref,
    own_ref, tx_ref, tz_ref, t4_ref, t6_ref, a_ref, b_ref, aux_all, s_ref, buf0, buf1,
):
    rows = q_ref.shape[0]
    bits = level_bits()
    fill_slots(q_ref, k_ref, grad_ref, aux_ref, (rx_ref, rz_ref, r4_ref, r6_ref), a_ref, b_ref, aux_all)
    for h in range(2):
        b_ref[2 + h] = v_ref[:, h * LANES : (h + 1) * LANES]
    b_ref[8] = vx_ref[:, 0:LANES]
    for slot, ref, lane0, bit in ((4, vx_ref, 2 * LANES, bits[0]), (5, vz_ref, 0, bits[1]), (6, v4_ref, 0, bits[2]), (7, v6_ref, 0, bits[2])):

        @pl.when(bit != 0)
        def _(slot=slot, ref=ref, lane0=lane0):
            b_ref[slot] = ref[:, lane0 : lane0 + LANES]

    s_ref[...] = jnp.zeros(s_ref.shape, jnp.float32)

    def products(qs, ks, buf):
        query0, query1 = halves(a_ref[qs])
        key = a_ref[ks]
        buf[0] = nt(key, query0)
        buf[1] = nt(key, query1)
        buf[2] = nt(b_ref[ks], b_ref[qs])

    def consume(qs, ks, buf, masked):
        query0, query1 = halves(a_ref[qs])
        key0, key1 = halves(a_ref[ks])
        aux = aux_all[qs]
        map0, map1 = maps_of(buf, aux, masked)
        dots = buf[2]
        score0 = (map0 * (dots - aux[2:3])).astype(jnp.bfloat16)
        score1 = (map1 * (aux[3:4] - dots)).astype(jnp.bfloat16)
        s_ref[ks] += jnp.dot(score0, query0, preferred_element_type=jnp.float32) + jnp.dot(
            score1, query1, preferred_element_type=jnp.float32
        )
        turned = tn(key0, score0) + tn(key1, score1)
        for i in range(rows // LANES):
            s_ref[qs, i * LANES : (i + 1) * LANES, :] += turned[:, i * LANES : (i + 1) * LANES]

    each_unit(products, consume, buf0, buf1)
    own_ref[...] = s_ref[0:4]
    for i, slot in enumerate((4, 8, 9)):
        tx_ref[:, i * LANES : (i + 1) * LANES] = s_ref[slot].astype(jnp.bfloat16)
    for ref, slot in ((tz_ref, 5), (t4_ref, 6), (t6_ref, 7)):
        ref[...] = s_ref[slot].astype(jnp.bfloat16)


def join_kernel(own_ref, ux_ref, uz_ref, u4_ref, u6_ref, dq_ref, dk_ref, s_ref):
    bits = level_bits()
    for i in range(4):
        s_ref[i] = own_ref[i]
    s_ref[2] += ux_ref[:, LANES : 2 * LANES].astype(jnp.float32)
    s_ref[1] += ux_ref[:, 2 * LANES : 3 * LANES].astype(jnp.float32)
    for ref, bit in ((ux_ref, bits[0]), (uz_ref, bits[1]), (u4_ref, bits[2]), (u6_ref, bits[2])):
        spot = jnp.where(bit == 0, 3, 0)
        s_ref[spot] += ref[:, 0:LANES].astype(jnp.float32)
    for h in range(2):
        for i in range(s_ref.shape[1] // LANES):
            spot = slice(i * LANES, (i + 1) * LANES)
            dq_ref[spot, h * LANES : (h + 1) * LANES] = jnp.transpose(s_ref[h, spot, :]) * 0.125
        dk_ref[:, h * LANES : (h + 1) * LANES] = s_ref[2 + h] * 0.125


def call(kernel, outs, args, scratch=(), smem=(), micros=1):
    vmem = pl.BlockSpec(memory_space=pltpu.VMEM)
    specs = [pl.BlockSpec(memory_space=pltpu.SMEM) if i in smem else vmem for i in range(len(args))]
    return pl.pallas_call(
        kernel,
        out_shape=[jax.ShapeDtypeStruct(s, d) for s, d in outs],
        in_specs=specs,
        out_specs=[vmem] * len(outs),
        scratch_shapes=list(scratch),
        cost_estimate=pl.CostEstimate(flops=micros * 14_000_000, bytes_accessed=1_000_000, transcendentals=0),
    )(*args)


def swap(x, axis, size, mask):
    return lax.ppermute(x, axis, [(i, i ^ mask) for i in range(size)])


def paired_device(*args):
    return paired_steps(*args)


def paired_steps(queries, key_vectors, latents, w_value, log_sums, out_pair, cotangent, lambdas, out_gain):
    rows, width = queries.shape
    narrow, wide = jnp.bfloat16, jnp.float32
    seq, feat = lax.axis_size("sp"), lax.axis_size("tp")
    slot_shape = (rows, LANES)
    far = swap(latents, "tp", feat, 2)
    near = swap(latents, "tp", feat, 1)
    grad, aux, px, pz, pm = call(
        prep_kernel,
        [((rows, width), narrow), ((16, rows), wide), ((rows + AUX_ROWS, 5 * LANES), narrow),
         ((rows + AUX_ROWS, width), narrow), ((rows + AUX_ROWS, width), narrow)],
        (queries, key_vectors, log_sums.T, out_pair, cotangent, lambdas, out_gain[None, :]),
        smem=(5,), micros=4,
    )
    r4 = swap(pm, "sp", seq, 4)
    r6 = swap(r4, "sp", seq, 2)
    rz = swap(pz, "sp", seq, 2)
    rx = swap(px, "sp", seq, 1)
    next_far = swap(far, "tp", feat, 1)
    values, = call(value_kernel, [((rows, width), narrow)], (latents, far, near, next_far, w_value), micros=3)
    slots = [pltpu.VMEM((SLOTS,) + slot_shape, narrow), pltpu.VMEM((SLOTS,) + slot_shape, narrow),
             pltpu.VMEM((SLOTS, 8, rows), wide), pltpu.VMEM((SLOTS,) + slot_shape, wide)]
    shared = (queries, key_vectors, grad, aux, rx, rz, r4, r6)
    dv0, tx, tz, t4, t6 = call(
        mixed_kernel, [((2,) + slot_shape, wide), ((rows, 3 * LANES), narrow)] + [(slot_shape, narrow)] * 3,
        shared + (values,), scratch=slots + [pltpu.VMEM((2, rows, rows), wide)] * 2, micros=8,
    )
    u4 = swap(t4, "sp", seq, 4)
    u6 = swap(t6, "sp", seq, 6)
    uz = swap(tz, "sp", seq, 2)
    ux = swap(tx, "sp", seq, 1)
    own, sx, sz, s4, s6 = call(
        score_kernel, [((4,) + slot_shape, wide), ((rows, 3 * LANES), narrow)] + [(slot_shape, narrow)] * 3,
        shared + (values, ux, uz, u4, u6), scratch=slots + [pltpu.VMEM((3, rows, rows), wide)] * 2, micros=16,
    )
    part, dv, _ = call(
        weight_kernel, [((4, 2, width, latents.shape[1] * feat // seq), narrow), ((rows, width), wide), ((rows, width), narrow)],
        (latents, far, near, next_far, dv0, ux, uz, u4, u6), micros=5,
    )
    w4 = swap(s4, "sp", seq, 4)
    w6 = swap(s6, "sp", seq, 6)
    wz = swap(sz, "sp", seq, 2)
    wx = swap(sx, "sp", seq, 1)
    groups = [list(range(4)), list(range(4, 8))]
    pieces = lax.all_to_all(part, "sp", 0, 0, axis_index_groups=groups)
    keep, send = call(fold_kernel, [(part.shape[:1:-1], wide), (part.shape[:1:-1], narrow)], (pieces,), micros=1)
    last = swap(send, "sp", seq, 4)
    dq, dk = call(
        join_kernel, [((rows, width), wide)] * 2, (own, wx, wz, w4, w6),
        scratch=[pltpu.VMEM((4,) + slot_shape, wide)], micros=3,
    )
    return dq, dk, dv, keep + last.astype(wide)


def solution(mesh):
    paired = (mesh.shape["sp"], mesh.shape["tp"]) == (8, 4)
    return jax.shard_map(
        paired_device if paired else general_device,
        mesh=mesh,
        in_specs=(
            P("sp", "tp"),
            P("sp", "tp"),
            P("sp", "tp"),
            P(None, "tp"),
            P("sp", "tp"),
            P("sp", "tp"),
            P("sp", "tp"),
            P("tp"),
            P(),
        ),
        out_specs=(P("sp", "tp"), P("sp", "tp"), P("sp", "tp"), P("sp", "tp")),
        check_vma=False,
    )
```

```python
import jax
import jax.numpy as jnp
from jax import lax
from jax.experimental import pallas as pl
from jax.experimental.pallas import tpu as pltpu
from jax.sharding import PartitionSpec as P


norm_floor = 0.25
block_rows = 512


def head_cotangent(out_pair, cotangent, lambdas, out_gain):
    tok_rows = out_pair.shape[0]
    head_count = lambdas.shape[0]
    out_maps = out_pair.astype(jnp.float32).reshape(tok_rows, head_count, 2, -1)
    lam_cols = lambdas[None, :, None]
    merged = out_maps[:, :, 0] - lam_cols * out_maps[:, :, 1]
    inv_norm = lax.rsqrt(jnp.mean(merged * merged, axis=-1, keepdims=True) + norm_floor)
    scaled = cotangent.astype(jnp.float32).reshape(merged.shape) * out_gain
    inner_dot = jnp.mean(scaled * merged, axis=-1, keepdims=True)
    out_grad = (inv_norm * scaled - merged * (inv_norm * inv_norm * inv_norm) * inner_dot).astype(
        jnp.bfloat16
    )
    grad_wide = out_grad.astype(jnp.float32)
    first_map = jnp.sum(grad_wide * out_maps[:, :, 0], axis=-1)
    second_map = -lambdas[None, :] * jnp.sum(grad_wide * out_maps[:, :, 1], axis=-1)
    return (out_grad, jnp.stack([first_map, second_map], axis=-1))


def block_terms(
    query_block,
    key_block,
    value_block,
    grad_block,
    log_block,
    term_block,
    lambdas,
    query_pos,
    key_pos,
):
    factor = query_block.shape[-1] ** (-0.5)
    scores = (
        jnp.einsum("qhcd,khcd->hcqk", query_block, key_block, preferred_element_type=jnp.float32)
        * factor
    )
    visible = key_pos[None, :] <= query_pos[:, None]
    shifted = scores - jnp.transpose(log_block, (1, 2, 0))[..., None]
    softmax_maps = jnp.where(visible, jnp.exp(shifted), 0.0)
    value_dot = jnp.einsum(
        "qhe,khe->hqk", grad_block, value_block, preferred_element_type=jnp.float32
    )
    lam_cols = lambdas[:, None, None]
    weights = (softmax_maps[:, 0] - lam_cols * softmax_maps[:, 1]).astype(jnp.bfloat16)
    term_cols = jnp.transpose(term_block, (1, 2, 0))
    first_map = softmax_maps[:, 0] * (value_dot - term_cols[:, 0, :, None])
    second_map = softmax_maps[:, 1] * (-lam_cols * value_dot - term_cols[:, 1, :, None])
    dscore = (jnp.stack([first_map, second_map], axis=1) * factor).astype(jnp.bfloat16)
    return (weights, dscore)


def block_span():
    return block_rows


def general_device(
    queries, key_vectors, latents, w_value, log_sums, out_pair, cotangent, lambdas, out_gain
):
    tok_rows = queries.shape[0]
    head_count = lambdas.shape[0]
    offset = lax.axis_index("sp") * tok_rows
    own_pos = offset + jnp.arange(tok_rows, dtype=jnp.int32)
    last_pos = offset + tok_rows - 1
    gathered = lax.all_gather(latents, "tp", axis=1, tiled=True)
    values = jnp.dot(gathered, w_value, preferred_element_type=jnp.float32).astype(jnp.bfloat16)
    out_grad, row_terms = head_cotangent(out_pair, cotangent, lambdas, out_gain)
    query_heads = queries.reshape(tok_rows, head_count, 2, -1)
    key_heads = key_vectors.reshape(tok_rows, head_count, 2, -1)
    value_heads = values.reshape(tok_rows, head_count, -1)
    log_heads = log_sums.reshape(tok_rows, head_count, 2)
    grad_flat = out_grad.reshape(tok_rows, -1)
    term_flat = row_terms.reshape(tok_rows, -1)
    zero_keys = jnp.zeros(key_heads.shape, jnp.float32)
    zero_values = jnp.zeros(value_heads.shape, jnp.float32)
    shards = (
        lax.all_gather(key_vectors, "sp", axis=0, tiled=True),
        lax.all_gather(values, "sp", axis=0, tiled=True),
    )
    key_piece = shards[0]
    value_piece = shards[1]
    piece_rows = key_piece.shape[0]
    block_len = block_span()

    def query_add_block(block_idx, partial_value):
        begin_row = block_idx * block_len
        key_block = lax.dynamic_slice_in_dim(key_piece, begin_row, block_len, 0).reshape(
            block_len, head_count, 2, -1
        )
        value_block = lax.dynamic_slice_in_dim(value_piece, begin_row, block_len, 0).reshape(
            block_len, head_count, -1
        )
        key_pos = begin_row + jnp.arange(block_len, dtype=jnp.int32)

        def query_compute(sums):
            _, dscore = block_terms(
                query_heads,
                key_block,
                value_block,
                out_grad,
                log_heads,
                row_terms,
                lambdas,
                own_pos,
                key_pos,
            )
            return sums + jnp.einsum(
                "hcqk,khcd->qhcd", dscore, key_block, preferred_element_type=jnp.float32
            )

        return lax.cond(begin_row <= last_pos, query_compute, lambda sums: sums, partial_value)

    query_grad = lax.fori_loop(0, piece_rows // block_len, query_add_block, zero_keys)
    shards = (
        lax.all_gather(queries.astype(jnp.float32), "sp", axis=0, tiled=True).astype(jnp.bfloat16),
        lax.all_gather(grad_flat.astype(jnp.float32), "sp", axis=0, tiled=True).astype(
            jnp.bfloat16
        ),
        lax.all_gather(log_sums, "sp", axis=0, tiled=True),
        lax.all_gather(term_flat, "sp", axis=0, tiled=True),
    )
    query_piece = shards[0]
    grad_piece = shards[1]
    log_piece = shards[2]
    term_piece = shards[3]
    piece_rows = query_piece.shape[0]
    key_block_len = block_span()

    def key_add_block(block_idx, partial_value):
        begin_row = block_idx * key_block_len
        query_block = lax.dynamic_slice_in_dim(query_piece, begin_row, key_block_len, 0).reshape(
            key_block_len, head_count, 2, -1
        )
        grad_block = lax.dynamic_slice_in_dim(grad_piece, begin_row, key_block_len, 0).reshape(
            key_block_len, head_count, -1
        )
        log_block = lax.dynamic_slice_in_dim(log_piece, begin_row, key_block_len, 0).reshape(
            key_block_len, head_count, 2
        )
        term_block = lax.dynamic_slice_in_dim(term_piece, begin_row, key_block_len, 0).reshape(
            key_block_len, head_count, 2
        )
        query_pos = begin_row + jnp.arange(key_block_len, dtype=jnp.int32)

        def key_compute(sums):
            weights, dscore = block_terms(
                query_block,
                key_heads,
                value_heads,
                grad_block,
                log_block,
                term_block,
                lambdas,
                query_pos,
                own_pos,
            )
            key_sum = sums[0] + jnp.einsum(
                "hcqk,qhcd->khcd", dscore, query_block, preferred_element_type=jnp.float32
            )
            value_sum = sums[1] + jnp.einsum(
                "hqk,qhe->khe", weights, grad_block, preferred_element_type=jnp.float32
            )
            return (key_sum, value_sum)

        return lax.cond(
            begin_row + key_block_len - 1 >= offset, key_compute, lambda sums: sums, partial_value
        )

    key_grad, value_grad = lax.fori_loop(
        0, piece_rows // key_block_len, key_add_block, (zero_keys, zero_values)
    )
    value_flat = value_grad.reshape(tok_rows, -1)
    value_narrow = value_flat.astype(jnp.bfloat16)
    weight_grad = lax.psum_scatter(
        lax.dot_general(
            gathered, value_narrow, (((0,), (0,)), ((), ())), preferred_element_type=jnp.float32
        ),
        "sp",
        scatter_dimension=0,
        tiled=True,
    )
    return (
        query_grad.reshape(tok_rows, -1),
        key_grad.reshape(tok_rows, -1),
        value_flat,
        weight_grad,
    )


LOG2E = 1.4426950408889634
AUX_ROWS = 32
SLOTS = 10
LANES = 128


def nt(a, b):
    return lax.dot_general(a, b, (((1,), (1,)), ((), ())), preferred_element_type=jnp.float32)


def tn(a, b):
    return lax.dot_general(a, b, (((0,), (0,)), ((), ())), preferred_element_type=jnp.float32)


def level_bits():
    place = lax.axis_index("sp")
    return place % 2, (place // 2) % 2, (place // 4) % 2


def split_pieces(rows):
    high = rows.astype(jnp.bfloat16)
    rest = rows - high.astype(jnp.float32)
    middle = rest.astype(jnp.bfloat16)
    low = (rest - middle.astype(jnp.float32)).astype(jnp.bfloat16)
    return high, middle, low


def prep_kernel(q_ref, k_ref, log_ref, pair_ref, cot_ref, lam_ref, gain_ref, grad_ref, aux_ref, px_ref, pz_ref, pm_ref):
    rows = q_ref.shape[0]
    half = rows // 2
    bit0, bit1, bit2 = level_bits()
    lane = lax.broadcasted_iota(jnp.int32, (rows, LANES), 1)
    aux_blocks = []
    for h in range(2):
        first = pair_ref[:, 2 * h * LANES : (2 * h + 1) * LANES].astype(jnp.float32)
        second = pair_ref[:, (2 * h + 1) * LANES : (2 * h + 2) * LANES].astype(jnp.float32)
        lam = lam_ref[h]
        merged = first - lam * second
        inv = lax.rsqrt(jnp.mean(merged * merged, axis=-1, keepdims=True) + norm_floor)
        scaled = cot_ref[:, h * LANES : (h + 1) * LANES].astype(jnp.float32) * gain_ref[...]
        inner = jnp.mean(scaled * merged, axis=-1, keepdims=True)
        grad = (inv * scaled - merged * (inv * inv * inv) * inner).astype(jnp.bfloat16)
        grad_ref[:, h * LANES : (h + 1) * LANES] = grad
        wide = grad.astype(jnp.float32)
        term0 = jnp.sum(wide * first, axis=-1, keepdims=True)
        term1 = jnp.sum(wide * second, axis=-1, keepdims=True)
        terms = jnp.where(lane == 2, term0, jnp.where(lane == 3, term1, 0.0))
        turned = jnp.concatenate(
            [jnp.transpose(terms[i * LANES : (i + 1) * LANES])[0:8] for i in range(rows // LANES)], axis=1
        )
        log0 = log_ref[2 * h : 2 * h + 1, :] * LOG2E
        log1 = (log_ref[2 * h + 1 : 2 * h + 2, :] - jnp.log(jnp.full((1, rows), lam, jnp.float32))) * LOG2E
        aux = jnp.concatenate([log0, log1, turned[2:4], jnp.zeros((4, rows), jnp.float32)], axis=0)
        aux_ref[h * 8 : (h + 1) * 8, :] = aux
        pieces = split_pieces(aux)
        wide_rows = jnp.concatenate([p.astype(jnp.float32)[0:4] for p in pieces] + [jnp.zeros((4, rows), jnp.float32)], axis=0)
        aux_blocks.append(wide_rows.astype(jnp.bfloat16))

    def put(ref, lane0, early, head_k, head_q):

        @pl.when(early)
        def _():
            ref[0:rows, lane0 : lane0 + LANES] = k_ref[:, head_k * LANES : (head_k + 1) * LANES]
            ref[0:rows, lane0 + LANES : lane0 + 2 * LANES] = k_ref[:, head_k * LANES : (head_k + 1) * LANES]

        @pl.when(jnp.logical_not(early))
        def _():
            ref[0:rows, lane0 : lane0 + LANES] = q_ref[:, head_q * LANES : (head_q + 1) * LANES]
            ref[0:rows, lane0 + LANES : lane0 + 2 * LANES] = grad_ref[:, head_q * LANES : (head_q + 1) * LANES]

    def put_aux(ref, lane0, h):
        ref[rows : rows + 16, lane0 : lane0 + half] = aux_blocks[h][:, 0:half]
        ref[rows + 16 : rows + 32, lane0 : lane0 + half] = aux_blocks[h][:, half:rows]

    put(px_ref, 0, bit0 == 0, 1, 0)
    px_ref[0:rows, 2 * LANES : 3 * LANES] = q_ref[:, LANES : 2 * LANES]
    px_ref[0:rows, 3 * LANES : 4 * LANES] = grad_ref[:, LANES : 2 * LANES]
    px_ref[0:rows, 4 * LANES : 5 * LANES] = k_ref[:, 0:LANES]
    px_ref[rows : rows + 32, 4 * LANES : 5 * LANES] = jnp.zeros((32, LANES), jnp.bfloat16)
    put_aux(px_ref, 0, 0)
    put_aux(px_ref, half, 1)
    put(pz_ref, 0, bit1 == 0, 1, 0)
    put_aux(pz_ref, 0, 0)
    put(pm_ref, 0, bit2 == 0, 1, 0)
    put_aux(pm_ref, 0, 0)


def value_kernel(own_ref, far_ref, near_ref, next_ref, w_ref, out_ref):
    cols = own_ref.shape[1]
    place = lax.axis_index("tp")

    def part(x, spot):
        return jnp.dot(x, w_ref[pl.ds(spot * cols, cols), :], preferred_element_type=jnp.float32)

    total = part(own_ref[...], place) + part(far_ref[...], (place + 2) % 4)
    near = place + 1 - 2 * (place % 2)
    total += part(near_ref[...], near) + part(next_ref[...], (near + 2) % 4)
    out_ref[...] = total.astype(jnp.bfloat16)


def weight_kernel(own_ref, far_ref, near_ref, next_ref, dv0_ref, ux_ref, uz_ref, u4_ref, u6_ref, out_ref, dv_ref, narrow_ref):
    bits = level_bits()
    cols = own_ref.shape[1]
    place = lax.axis_index("tp")
    near = place + 1 - 2 * (place % 2)
    dv_ref[:, 0:LANES] = dv0_ref[0] + ux_ref[:, LANES : 2 * LANES].astype(jnp.float32)
    dv_ref[:, LANES : 2 * LANES] = dv0_ref[1]
    for ref, lane0, bit in ((ux_ref, 2 * LANES, bits[0]), (uz_ref, 0, bits[1]), (u4_ref, 0, bits[2]), (u6_ref, 0, bits[2])):

        @pl.when(bit == 0)
        def _(ref=ref, lane0=lane0):
            dv_ref[:, LANES : 2 * LANES] += ref[:, lane0 : lane0 + LANES].astype(jnp.float32)

    narrow_ref[...] = dv_ref[...].astype(jnp.bfloat16)
    grad = narrow_ref[...]
    size = out_ref.shape[3]
    for ref, spot in ((own_ref, place), (far_ref, (place + 2) % 4), (near_ref, near), (next_ref, (near + 2) % 4)):
        block = tn(grad, ref[...]).astype(jnp.bfloat16)
        for i in range(cols // size):
            part = spot * (cols // size) + i
            out_ref[part % 4, part // 4] = block[:, i * size : (i + 1) * size]


def fold_kernel(pieces_ref, keep_ref, send_ref):
    bit = lax.axis_index("sp") // 4
    for ref, spot in ((keep_ref, bit), (send_ref, 1 - bit)):
        total = pieces_ref[0, spot].astype(jnp.float32)
        for i in range(1, pieces_ref.shape[0]):
            total += pieces_ref[i, spot].astype(jnp.float32)
        ref[...] = jnp.transpose(total).astype(ref.dtype)


def join_pieces(block_ref, rows, lane0):
    half = rows // 2
    parts = [block_ref[rows + 16 * i : rows + 16 * (i + 1), lane0 : lane0 + half].astype(jnp.float32) for i in range(2)]
    sums = [p[0:4] + p[4:8] + p[8:12] for p in parts]
    return jnp.concatenate(sums, axis=1)


SCALE = LOG2E / 8.0


def halves(x):
    left = lax.broadcasted_iota(jnp.int32, (1, LANES), 1) < LANES // 2
    none = jnp.zeros((), x.dtype)
    return jnp.where(left, x, none), jnp.where(left, none, x)


def fill_slots(slots, q_ref, k_ref, grad_ref, aux_ref, received, a_ref, b_ref, aux_all):
    rows = q_ref.shape[0]
    for slot in slots:
        lanes = slice((slot % 2) * LANES, (slot % 2 + 1) * LANES)
        if slot < 2:
            a_ref[slot] = q_ref[:, lanes]
            b_ref[slot] = grad_ref[:, lanes]
            aux_all[slot, 0:4, :] = aux_ref[8 * slot : 8 * slot + 4, :]
        elif slot < 4:
            a_ref[slot] = k_ref[:, lanes]
        elif slot < 8:
            ref = received[slot]
            a_ref[slot] = ref[0:rows, 0:LANES]
            b_ref[slot] = ref[0:rows, LANES : 2 * LANES]
            aux_all[slot, 0:4, :] = join_pieces(ref, rows, 0)
        elif slot == 8:
            a_ref[slot] = received[4][0:rows, 4 * LANES : 5 * LANES]
        else:
            ref = received[4]
            a_ref[slot] = ref[0:rows, 2 * LANES : 3 * LANES]
            b_ref[slot] = ref[0:rows, 3 * LANES : 4 * LANES]
            aux_all[slot, 0:4, :] = join_pieces(ref, rows, rows // 2)


def maps_of(buf, aux, masked):
    map0 = jnp.exp2(buf[0] * SCALE - aux[0:1])
    map1 = jnp.exp2(buf[1] * SCALE - aux[1:2])
    if masked:
        key_pos = lax.broadcasted_iota(jnp.int32, map0.shape, 0)
        query_pos = lax.broadcasted_iota(jnp.int32, map0.shape, 1)
        seen = key_pos <= query_pos
        map0 = jnp.where(seen, map0, 0.0)
        map1 = jnp.where(seen, map1, 0.0)
    return map0, map1


def pick(u):
    level = 0 if u == 0 else 1 if u < 3 else 2
    early = level_bits()[level] == 0
    other = 4 + (u + 1) // 2
    own = u == 0 or u % 2 == 1
    return jnp.where(early, other, 1 if own else 9), jnp.where(early, 2 if own else 8, other)


def each_unit(units, products, consume, bufs):
    products(*units[0][:2], bufs[0])
    for i, (qs, ks, masked) in enumerate(units):
        if i + 1 < len(units):
            products(*units[i + 1][:2], bufs[(i + 1) % 2])
        consume(qs, ks, bufs[i % 2], masked)


def mixed_work(a_ref, b_ref, aux_all, s_ref):
    def products(qs, ks, buf):
        query0, query1 = halves(a_ref[qs])
        key = a_ref[ks]
        buf[0] = nt(key, query0)
        buf[1] = nt(key, query1)

    def consume(qs, ks, buf, masked):
        map0, map1 = maps_of(buf, aux_all[qs], masked)
        mixed = (map0 - map1).astype(jnp.bfloat16)
        s_ref[ks] += jnp.dot(mixed, b_ref[qs], preferred_element_type=jnp.float32)

    return products, consume


def mixed_first(
    q_ref, k_ref, grad_ref, aux_ref, rx_ref, rz_ref, r4_ref, v_ref,
    carry_ref, tz_ref, t4_ref, a_ref, b_ref, aux_all, s_ref, buf0, buf1,
):
    received = {4: rx_ref, 5: rz_ref, 6: r4_ref}
    fill_slots((0, 1, 2, 3, 4, 5, 6, 8, 9), q_ref, k_ref, grad_ref, aux_ref, received, a_ref, b_ref, aux_all)
    for slot in (2, 3, 4, 5, 6, 8):
        s_ref[slot] = jnp.zeros(s_ref.shape[1:], jnp.float32)
    units = [(*pick(u), False) for u in range(5)] + [(0, 2, True), (1, 3, True)]
    each_unit(units, *mixed_work(a_ref, b_ref, aux_all, s_ref), (buf0, buf1))
    for i, slot in enumerate((2, 3, 4, 8)):
        carry_ref[i] = s_ref[slot]
    bits = level_bits()
    for ref, slot, bit in ((tz_ref, 5, bits[1]), (t4_ref, 6, bits[2])):
        going_up(ref, 0, v_ref, s_ref, slot, bit)


def going_up(ref, lane0, v_ref, s_ref, slot, bit):
    @pl.when(bit == 0)
    def _():
        ref[:, lane0 : lane0 + LANES] = v_ref[:, LANES : 2 * LANES]

    @pl.when(bit != 0)
    def _():
        ref[:, lane0 : lane0 + LANES] = s_ref[slot].astype(jnp.bfloat16)


def mixed_second(
    q_ref, k_ref, grad_ref, aux_ref, rx_ref, r6_ref, v_ref, carry_ref,
    dv_ref, tx_ref, t6_ref, a_ref, b_ref, aux_all, s_ref, buf0, buf1,
):
    received = {4: rx_ref, 7: r6_ref}
    fill_slots((1, 2, 7, 8, 9), q_ref, k_ref, grad_ref, aux_ref, received, a_ref, b_ref, aux_all)
    s_ref[7] = jnp.zeros(s_ref.shape[1:], jnp.float32)
    for i, slot in enumerate((2, 3, 4, 8)):
        s_ref[slot] = carry_ref[i]
    each_unit([(*pick(u), False) for u in (5, 6)], *mixed_work(a_ref, b_ref, aux_all, s_ref), (buf0, buf1))
    dv_ref[...] = s_ref[2:4]
    tx_ref[:, 0:LANES] = v_ref[:, 0:LANES]
    tx_ref[:, LANES : 2 * LANES] = s_ref[8].astype(jnp.bfloat16)
    bits = level_bits()
    going_up(tx_ref, 2 * LANES, v_ref, s_ref, 4, bits[0])
    going_up(t6_ref, 0, v_ref, s_ref, 7, bits[2])


def score_work(a_ref, b_ref, aux_all, s_ref):
    rows = a_ref.shape[1]

    def products(qs, ks, buf):
        query0, query1 = halves(a_ref[qs])
        key = a_ref[ks]
        buf[0] = nt(key, query0)
        buf[1] = nt(key, query1)
        buf[2] = nt(b_ref[ks], b_ref[qs])

    def consume(qs, ks, buf, masked):
        query0, query1 = halves(a_ref[qs])
        key0, key1 = halves(a_ref[ks])
        aux = aux_all[qs]
        map0, map1 = maps_of(buf, aux, masked)
        dots = buf[2]
        score0 = (map0 * (dots - aux[2:3])).astype(jnp.bfloat16)
        score1 = (map1 * (aux[3:4] - dots)).astype(jnp.bfloat16)
        s_ref[ks] += jnp.dot(score0, query0, preferred_element_type=jnp.float32) + jnp.dot(
            score1, query1, preferred_element_type=jnp.float32
        )
        turned = tn(key0, score0) + tn(key1, score1)
        for i in range(rows // LANES):
            s_ref[qs, i * LANES : (i + 1) * LANES, :] += turned[:, i * LANES : (i + 1) * LANES]

    return products, consume


def score_own(q_ref, k_ref, grad_ref, aux_ref, v_ref, own_ref, a_ref, b_ref, aux_all, buf0, buf1):
    fill_slots((0, 1, 2, 3), q_ref, k_ref, grad_ref, aux_ref, {}, a_ref, b_ref, aux_all)
    for h in range(2):
        b_ref[2 + h] = v_ref[:, h * LANES : (h + 1) * LANES]
    own_ref[...] = jnp.zeros(own_ref.shape, jnp.float32)
    each_unit([(0, 2, True), (1, 3, True)], *score_work(a_ref, b_ref, aux_all, own_ref), (buf0, buf1))


def late_values(b_ref, slot, ref, lane0, bit):
    @pl.when(bit != 0)
    def _():
        b_ref[slot] = ref[:, lane0 : lane0 + LANES]


CARRIED = (1, 2, 8, 9)


def score_far(
    q_ref, k_ref, grad_ref, aux_ref, rx_ref, r4_ref, r6_ref, v_ref, vx_ref, v4_ref, v6_ref,
    carry_ref, t4_ref, t6_ref, a_ref, b_ref, aux_all, s_ref, buf0, buf1,
):
    bits = level_bits()
    received = {4: rx_ref, 6: r4_ref, 7: r6_ref}
    fill_slots((1, 2, 6, 7, 8, 9), q_ref, k_ref, grad_ref, aux_ref, received, a_ref, b_ref, aux_all)
    b_ref[2] = v_ref[:, 0:LANES]
    b_ref[8] = vx_ref[:, 0:LANES]
    late_values(b_ref, 6, v4_ref, 0, bits[2])
    late_values(b_ref, 7, v6_ref, 0, bits[2])
    for slot in (1, 2, 6, 7, 8, 9):
        s_ref[slot] = jnp.zeros(s_ref.shape[1:], jnp.float32)
    each_unit([(*pick(u), False) for u in (3, 4, 5, 6)], *score_work(a_ref, b_ref, aux_all, s_ref), (buf0, buf1))
    for i, slot in enumerate(CARRIED):
        carry_ref[i] = s_ref[slot]
    t4_ref[...] = s_ref[6].astype(jnp.bfloat16)
    t6_ref[...] = s_ref[7].astype(jnp.bfloat16)


def score_near(
    q_ref, k_ref, grad_ref, aux_ref, rx_ref, rz_ref, v_ref, vx_ref, vz_ref, own0_ref, carry_ref,
    own_ref, tx_ref, tz_ref, a_ref, b_ref, aux_all, s_ref, buf0, buf1,
):
    bits = level_bits()
    received = {4: rx_ref, 5: rz_ref}
    fill_slots((1, 2, 4, 5, 8, 9), q_ref, k_ref, grad_ref, aux_ref, received, a_ref, b_ref, aux_all)
    b_ref[2] = v_ref[:, 0:LANES]
    b_ref[8] = vx_ref[:, 0:LANES]
    late_values(b_ref, 4, vx_ref, 2 * LANES, bits[0])
    late_values(b_ref, 5, vz_ref, 0, bits[1])
    for slot in (4, 5):
        s_ref[slot] = jnp.zeros(s_ref.shape[1:], jnp.float32)
    for i, slot in enumerate(CARRIED):
        s_ref[slot] = carry_ref[i]
    each_unit([(*pick(u), False) for u in range(3)], *score_work(a_ref, b_ref, aux_all, s_ref), (buf0, buf1))
    own_ref[...] = own0_ref[...]
    own_ref[1] += s_ref[1]
    own_ref[2] += s_ref[2]
    for i, slot in enumerate((4, 8, 9)):
        tx_ref[:, i * LANES : (i + 1) * LANES] = s_ref[slot].astype(jnp.bfloat16)
    tz_ref[...] = s_ref[5].astype(jnp.bfloat16)


def join_kernel(own_ref, ux_ref, uz_ref, u4_ref, u6_ref, dq_ref, dk_ref, s_ref):
    bits = level_bits()
    for i in range(4):
        s_ref[i] = own_ref[i]
    s_ref[2] += ux_ref[:, LANES : 2 * LANES].astype(jnp.float32)
    s_ref[1] += ux_ref[:, 2 * LANES : 3 * LANES].astype(jnp.float32)
    for ref, bit in ((ux_ref, bits[0]), (uz_ref, bits[1]), (u4_ref, bits[2]), (u6_ref, bits[2])):
        spot = jnp.where(bit == 0, 3, 0)
        s_ref[spot] += ref[:, 0:LANES].astype(jnp.float32)
    for h in range(2):
        for i in range(s_ref.shape[1] // LANES):
            spot = slice(i * LANES, (i + 1) * LANES)
            dq_ref[spot, h * LANES : (h + 1) * LANES] = jnp.transpose(s_ref[h, spot, :]) * 0.125
        dk_ref[:, h * LANES : (h + 1) * LANES] = s_ref[2 + h] * 0.125


def call(kernel, outs, args, scratch=(), smem=(), micros=1, grant=12):
    vmem = pl.BlockSpec(memory_space=pltpu.VMEM)
    specs = [pl.BlockSpec(memory_space=pltpu.SMEM) if i in smem else vmem for i in range(len(args))]
    return pl.pallas_call(
        kernel,
        out_shape=[jax.ShapeDtypeStruct(s, d) for s, d in outs],
        in_specs=specs,
        out_specs=[vmem] * len(outs),
        scratch_shapes=list(scratch),
        cost_estimate=pl.CostEstimate(flops=micros * 14_000_000, bytes_accessed=1_000_000, transcendentals=0),
        compiler_params=pltpu.CompilerParams(vmem_limit_bytes=grant * 2**20),
    )(*args)


def swap(x, axis, size, mask):
    return lax.ppermute(x, axis, [(i, i ^ mask) for i in range(size)])


def paired_device(*args):
    return paired_steps(*args)


def paired_steps(queries, key_vectors, latents, w_value, log_sums, out_pair, cotangent, lambdas, out_gain):
    rows, width = queries.shape
    narrow, wide = jnp.bfloat16, jnp.float32
    seq, feat = lax.axis_size("sp"), lax.axis_size("tp")
    slot_shape = (rows, LANES)
    grad, aux, px, pz, pm = call(
        prep_kernel,
        [((rows, width), narrow), ((16, rows), wide), ((rows + AUX_ROWS, 5 * LANES), narrow),
         ((rows + AUX_ROWS, width), narrow), ((rows + AUX_ROWS, width), narrow)],
        (queries, key_vectors, log_sums.T, out_pair, cotangent, lambdas, out_gain[None, :]),
        smem=(5,), micros=4, grant=58,
    )
    r4 = swap(pm, "sp", seq, 4)
    r6 = swap(r4, "sp", seq, 2)
    rz = swap(pz, "sp", seq, 2)
    rx = swap(px, "sp", seq, 1)
    far = swap(latents, "tp", feat, 2)
    near = swap(latents, "tp", feat, 1)
    next_far = swap(far, "tp", feat, 1)
    values, = call(value_kernel, [((rows, width), narrow)], (latents, far, near, next_far, w_value), micros=3)
    slots = [pltpu.VMEM((SLOTS,) + slot_shape, narrow), pltpu.VMEM((SLOTS,) + slot_shape, narrow), pltpu.VMEM((SLOTS, 8, rows), wide)]
    sums = [pltpu.VMEM((SLOTS,) + slot_shape, wide)]
    two, three = [pltpu.VMEM((2, rows, rows), wide)] * 2, [pltpu.VMEM((3, rows, rows), wide)] * 2
    base = (queries, key_vectors, grad, aux)
    carry, tz, t4 = call(
        mixed_first, [((4,) + slot_shape, wide)] + [(slot_shape, narrow)] * 2,
        base + (rx, rz, r4, values), scratch=slots + sums + two, micros=5, grant=20,
    )
    dv0, tx, t6 = call(
        mixed_second, [((2,) + slot_shape, wide), ((rows, 3 * LANES), narrow), (slot_shape, narrow)],
        base + (rx, r6, values, carry), scratch=slots + sums + two, micros=2, grant=20,
    )
    u4 = swap(t4, "sp", seq, 4)
    u6 = swap(t6, "sp", seq, 6)
    uz = swap(tz, "sp", seq, 2)
    ux = swap(tx, "sp", seq, 1)
    own0, = call(score_own, [((4,) + slot_shape, wide)], base + (values,), scratch=slots + three, micros=3, grant=20)
    carry, s4, s6 = call(
        score_far, [((4,) + slot_shape, wide)] + [(slot_shape, narrow)] * 2,
        base + (rx, r4, r6, values, ux, u4, u6), scratch=slots + sums + three, micros=5, grant=58,
    )
    own, sx, sz = call(
        score_near, [((4,) + slot_shape, wide), ((rows, 3 * LANES), narrow), (slot_shape, narrow)],
        base + (rx, rz, values, ux, uz, own0, carry), scratch=slots + sums + three, micros=4, grant=58,
    )
    part, dv, _ = call(
        weight_kernel, [((4, 2, width, latents.shape[1] * feat // seq), narrow), ((rows, width), wide), ((rows, width), narrow)],
        (latents, far, near, next_far, dv0, ux, uz, u4, u6), micros=5,
    )
    w4 = swap(s4, "sp", seq, 4)
    w6 = swap(s6, "sp", seq, 6)
    wz = swap(sz, "sp", seq, 2)
    wx = swap(sx, "sp", seq, 1)
    groups = [list(range(4)), list(range(4, 8))]
    pieces = lax.all_to_all(part, "sp", 0, 0, axis_index_groups=groups)
    keep, send = call(fold_kernel, [(part.shape[:1:-1], wide), (part.shape[:1:-1], narrow)], (pieces,), micros=1)
    last = swap(send, "sp", seq, 4)
    dq, dk = call(
        join_kernel, [((rows, width), wide)] * 2, (own, wx, wz, w4, w6),
        scratch=[pltpu.VMEM((4,) + slot_shape, wide)], micros=3,
    )
    return dq, dk, dv, keep + last.astype(wide)


def solution(mesh):
    paired = (mesh.shape["sp"], mesh.shape["tp"]) == (8, 4)
    return jax.shard_map(
        paired_device if paired else general_device,
        mesh=mesh,
        in_specs=(
            P("sp", "tp"),
            P("sp", "tp"),
            P("sp", "tp"),
            P(None, "tp"),
            P("sp", "tp"),
            P("sp", "tp"),
            P("sp", "tp"),
            P("tp"),
            P(),
        ),
        out_specs=(P("sp", "tp"), P("sp", "tp"), P("sp", "tp"), P("sp", "tp")),
        check_vma=False,
    )
```

```python
import jax
import jax.numpy as jnp
from jax import lax
from jax.experimental import pallas as pl
from jax.experimental.pallas import tpu as pltpu
from jax.sharding import PartitionSpec as P


norm_floor = 0.25
block_rows = 512


def head_cotangent(out_pair, cotangent, lambdas, out_gain):
    tok_rows = out_pair.shape[0]
    head_count = lambdas.shape[0]
    out_maps = out_pair.astype(jnp.float32).reshape(tok_rows, head_count, 2, -1)
    lam_cols = lambdas[None, :, None]
    merged = out_maps[:, :, 0] - lam_cols * out_maps[:, :, 1]
    inv_norm = lax.rsqrt(jnp.mean(merged * merged, axis=-1, keepdims=True) + norm_floor)
    scaled = cotangent.astype(jnp.float32).reshape(merged.shape) * out_gain
    inner_dot = jnp.mean(scaled * merged, axis=-1, keepdims=True)
    out_grad = (inv_norm * scaled - merged * (inv_norm * inv_norm * inv_norm) * inner_dot).astype(
        jnp.bfloat16
    )
    grad_wide = out_grad.astype(jnp.float32)
    first_map = jnp.sum(grad_wide * out_maps[:, :, 0], axis=-1)
    second_map = -lambdas[None, :] * jnp.sum(grad_wide * out_maps[:, :, 1], axis=-1)
    return (out_grad, jnp.stack([first_map, second_map], axis=-1))


def block_terms(
    query_block,
    key_block,
    value_block,
    grad_block,
    log_block,
    term_block,
    lambdas,
    query_pos,
    key_pos,
):
    factor = query_block.shape[-1] ** (-0.5)
    scores = (
        jnp.einsum("qhcd,khcd->hcqk", query_block, key_block, preferred_element_type=jnp.float32)
        * factor
    )
    visible = key_pos[None, :] <= query_pos[:, None]
    shifted = scores - jnp.transpose(log_block, (1, 2, 0))[..., None]
    softmax_maps = jnp.where(visible, jnp.exp(shifted), 0.0)
    value_dot = jnp.einsum(
        "qhe,khe->hqk", grad_block, value_block, preferred_element_type=jnp.float32
    )
    lam_cols = lambdas[:, None, None]
    weights = (softmax_maps[:, 0] - lam_cols * softmax_maps[:, 1]).astype(jnp.bfloat16)
    term_cols = jnp.transpose(term_block, (1, 2, 0))
    first_map = softmax_maps[:, 0] * (value_dot - term_cols[:, 0, :, None])
    second_map = softmax_maps[:, 1] * (-lam_cols * value_dot - term_cols[:, 1, :, None])
    dscore = (jnp.stack([first_map, second_map], axis=1) * factor).astype(jnp.bfloat16)
    return (weights, dscore)


def block_span():
    return block_rows


def general_device(
    queries, key_vectors, latents, w_value, log_sums, out_pair, cotangent, lambdas, out_gain
):
    tok_rows = queries.shape[0]
    head_count = lambdas.shape[0]
    offset = lax.axis_index("sp") * tok_rows
    own_pos = offset + jnp.arange(tok_rows, dtype=jnp.int32)
    last_pos = offset + tok_rows - 1
    gathered = lax.all_gather(latents, "tp", axis=1, tiled=True)
    values = jnp.dot(gathered, w_value, preferred_element_type=jnp.float32).astype(jnp.bfloat16)
    out_grad, row_terms = head_cotangent(out_pair, cotangent, lambdas, out_gain)
    query_heads = queries.reshape(tok_rows, head_count, 2, -1)
    key_heads = key_vectors.reshape(tok_rows, head_count, 2, -1)
    value_heads = values.reshape(tok_rows, head_count, -1)
    log_heads = log_sums.reshape(tok_rows, head_count, 2)
    grad_flat = out_grad.reshape(tok_rows, -1)
    term_flat = row_terms.reshape(tok_rows, -1)
    zero_keys = jnp.zeros(key_heads.shape, jnp.float32)
    zero_values = jnp.zeros(value_heads.shape, jnp.float32)
    shards = (
        lax.all_gather(key_vectors, "sp", axis=0, tiled=True),
        lax.all_gather(values, "sp", axis=0, tiled=True),
    )
    key_piece = shards[0]
    value_piece = shards[1]
    piece_rows = key_piece.shape[0]
    block_len = block_span()

    def query_add_block(block_idx, partial_value):
        begin_row = block_idx * block_len
        key_block = lax.dynamic_slice_in_dim(key_piece, begin_row, block_len, 0).reshape(
            block_len, head_count, 2, -1
        )
        value_block = lax.dynamic_slice_in_dim(value_piece, begin_row, block_len, 0).reshape(
            block_len, head_count, -1
        )
        key_pos = begin_row + jnp.arange(block_len, dtype=jnp.int32)

        def query_compute(sums):
            _, dscore = block_terms(
                query_heads,
                key_block,
                value_block,
                out_grad,
                log_heads,
                row_terms,
                lambdas,
                own_pos,
                key_pos,
            )
            return sums + jnp.einsum(
                "hcqk,khcd->qhcd", dscore, key_block, preferred_element_type=jnp.float32
            )

        return lax.cond(begin_row <= last_pos, query_compute, lambda sums: sums, partial_value)

    query_grad = lax.fori_loop(0, piece_rows // block_len, query_add_block, zero_keys)
    shards = (
        lax.all_gather(queries.astype(jnp.float32), "sp", axis=0, tiled=True).astype(jnp.bfloat16),
        lax.all_gather(grad_flat.astype(jnp.float32), "sp", axis=0, tiled=True).astype(
            jnp.bfloat16
        ),
        lax.all_gather(log_sums, "sp", axis=0, tiled=True),
        lax.all_gather(term_flat, "sp", axis=0, tiled=True),
    )
    query_piece = shards[0]
    grad_piece = shards[1]
    log_piece = shards[2]
    term_piece = shards[3]
    piece_rows = query_piece.shape[0]
    key_block_len = block_span()

    def key_add_block(block_idx, partial_value):
        begin_row = block_idx * key_block_len
        query_block = lax.dynamic_slice_in_dim(query_piece, begin_row, key_block_len, 0).reshape(
            key_block_len, head_count, 2, -1
        )
        grad_block = lax.dynamic_slice_in_dim(grad_piece, begin_row, key_block_len, 0).reshape(
            key_block_len, head_count, -1
        )
        log_block = lax.dynamic_slice_in_dim(log_piece, begin_row, key_block_len, 0).reshape(
            key_block_len, head_count, 2
        )
        term_block = lax.dynamic_slice_in_dim(term_piece, begin_row, key_block_len, 0).reshape(
            key_block_len, head_count, 2
        )
        query_pos = begin_row + jnp.arange(key_block_len, dtype=jnp.int32)

        def key_compute(sums):
            weights, dscore = block_terms(
                query_block,
                key_heads,
                value_heads,
                grad_block,
                log_block,
                term_block,
                lambdas,
                query_pos,
                own_pos,
            )
            key_sum = sums[0] + jnp.einsum(
                "hcqk,qhcd->khcd", dscore, query_block, preferred_element_type=jnp.float32
            )
            value_sum = sums[1] + jnp.einsum(
                "hqk,qhe->khe", weights, grad_block, preferred_element_type=jnp.float32
            )
            return (key_sum, value_sum)

        return lax.cond(
            begin_row + key_block_len - 1 >= offset, key_compute, lambda sums: sums, partial_value
        )

    key_grad, value_grad = lax.fori_loop(
        0, piece_rows // key_block_len, key_add_block, (zero_keys, zero_values)
    )
    value_flat = value_grad.reshape(tok_rows, -1)
    value_narrow = value_flat.astype(jnp.bfloat16)
    weight_grad = lax.psum_scatter(
        lax.dot_general(
            gathered, value_narrow, (((0,), (0,)), ((), ())), preferred_element_type=jnp.float32
        ),
        "sp",
        scatter_dimension=0,
        tiled=True,
    )
    return (
        query_grad.reshape(tok_rows, -1),
        key_grad.reshape(tok_rows, -1),
        value_flat,
        weight_grad,
    )


LOG2E = 1.4426950408889634
AUX_ROWS = 32
SLOTS = 10
LANES = 128


def nt(a, b):
    return lax.dot_general(a, b, (((1,), (1,)), ((), ())), preferred_element_type=jnp.float32)


def tn(a, b):
    return lax.dot_general(a, b, (((0,), (0,)), ((), ())), preferred_element_type=jnp.float32)


def level_bits():
    place = lax.axis_index("sp")
    return place % 2, (place // 2) % 2, (place // 4) % 2


def split_pieces(rows):
    high = rows.astype(jnp.bfloat16)
    rest = rows - high.astype(jnp.float32)
    middle = rest.astype(jnp.bfloat16)
    low = (rest - middle.astype(jnp.float32)).astype(jnp.bfloat16)
    return high, middle, low


def prep_kernel(q_ref, k_ref, log_ref, pair_ref, cot_ref, lam_ref, gain_ref, grad_ref, aux_ref, px_ref, pz_ref, pma_ref, pmb_ref):
    rows = q_ref.shape[0]
    half = rows // 2
    bit0, bit1, bit2 = level_bits()
    lane = lax.broadcasted_iota(jnp.int32, (rows, LANES), 1)
    aux_blocks = []
    for h in range(2):
        first = pair_ref[:, 2 * h * LANES : (2 * h + 1) * LANES].astype(jnp.float32)
        second = pair_ref[:, (2 * h + 1) * LANES : (2 * h + 2) * LANES].astype(jnp.float32)
        lam = lam_ref[h]
        merged = first - lam * second
        inv = lax.rsqrt(jnp.mean(merged * merged, axis=-1, keepdims=True) + norm_floor)
        scaled = cot_ref[:, h * LANES : (h + 1) * LANES].astype(jnp.float32) * gain_ref[...]
        inner = jnp.mean(scaled * merged, axis=-1, keepdims=True)
        grad = (inv * scaled - merged * (inv * inv * inv) * inner).astype(jnp.bfloat16)
        grad_ref[:, h * LANES : (h + 1) * LANES] = grad
        wide = grad.astype(jnp.float32)
        term0 = jnp.sum(wide * first, axis=-1, keepdims=True)
        term1 = jnp.sum(wide * second, axis=-1, keepdims=True)
        terms = jnp.where(lane == 2, term0, jnp.where(lane == 3, term1, 0.0))
        turned = jnp.concatenate(
            [jnp.transpose(terms[i * LANES : (i + 1) * LANES])[0:8] for i in range(rows // LANES)], axis=1
        )
        log0 = log_ref[2 * h : 2 * h + 1, :] * LOG2E
        log1 = (log_ref[2 * h + 1 : 2 * h + 2, :] - jnp.log(jnp.full((1, rows), lam, jnp.float32))) * LOG2E
        aux = jnp.concatenate([log0, log1, turned[2:4], jnp.zeros((4, rows), jnp.float32)], axis=0)
        aux_ref[h * 8 : (h + 1) * 8, :] = aux
        pieces = split_pieces(aux)
        wide_rows = jnp.concatenate([p.astype(jnp.float32)[0:4] for p in pieces] + [jnp.zeros((4, rows), jnp.float32)], axis=0)
        aux_blocks.append(wide_rows.astype(jnp.bfloat16))

    def put(ref, first, count, early):
        spot = slice(first, first + count)

        @pl.when(early)
        def _():
            ref[0:count, 0:LANES] = k_ref[spot, LANES : 2 * LANES]
            ref[0:count, LANES : 2 * LANES] = k_ref[spot, LANES : 2 * LANES]

        @pl.when(jnp.logical_not(early))
        def _():
            ref[0:count, 0:LANES] = q_ref[spot, 0:LANES]
            ref[0:count, LANES : 2 * LANES] = grad_ref[spot, 0:LANES]

    def put_aux(ref, first, lane0, h):
        ref[first : first + 16, lane0 : lane0 + half] = aux_blocks[h][:, 0:half]
        ref[first + 16 : first + 32, lane0 : lane0 + half] = aux_blocks[h][:, half:rows]

    put(pma_ref, 0, half, bit2 == 0)
    put_aux(pma_ref, half, 0, 0)
    put(pmb_ref, half, half, bit2 == 0)
    put(pz_ref, 0, rows, bit1 == 0)
    put_aux(pz_ref, rows, 0, 0)
    put(px_ref, 0, rows, bit0 == 0)
    px_ref[0:rows, 2 * LANES : 3 * LANES] = q_ref[:, LANES : 2 * LANES]
    px_ref[0:rows, 3 * LANES : 4 * LANES] = grad_ref[:, LANES : 2 * LANES]
    px_ref[0:rows, 4 * LANES : 5 * LANES] = k_ref[:, 0:LANES]
    px_ref[rows : rows + 32, 4 * LANES : 5 * LANES] = jnp.zeros((32, LANES), jnp.bfloat16)
    put_aux(px_ref, rows, 0, 0)
    put_aux(px_ref, rows, half, 1)


def value_kernel(own_ref, far_ref, near_ref, next_ref, w_ref, out_ref):
    cols = own_ref.shape[1]
    place = lax.axis_index("tp")

    def part(x, spot):
        return jnp.dot(x, w_ref[pl.ds(spot * cols, cols), :], preferred_element_type=jnp.float32)

    total = part(own_ref[...], place) + part(far_ref[...], (place + 2) % 4)
    near = place + 1 - 2 * (place % 2)
    total += part(near_ref[...], near) + part(next_ref[...], (near + 2) % 4)
    out_ref[...] = total.astype(jnp.bfloat16)


def weight_kernel(own_ref, far_ref, near_ref, next_ref, dv0_ref, ux_ref, uz_ref, u4_ref, u6_ref, w0_ref, w1_ref, w2_ref, w3_ref, dv_ref, all_ref, narrow_ref):
    bits = level_bits()
    cols = own_ref.shape[1]
    place = lax.axis_index("tp")
    near = place + 1 - 2 * (place % 2)
    dv_ref[:, 0:LANES] = dv0_ref[0] + ux_ref[:, 0:LANES].astype(jnp.float32)
    dv_ref[:, LANES : 2 * LANES] = dv0_ref[1]
    for ref, lane0, bit in ((ux_ref, LANES, bits[0]), (uz_ref, 0, bits[1]), (u4_ref, 0, bits[2]), (u6_ref, 0, bits[2])):

        @pl.when(bit == 0)
        def _(ref=ref, lane0=lane0):
            dv_ref[:, LANES : 2 * LANES] += ref[:, lane0 : lane0 + LANES].astype(jnp.float32)

    narrow_ref[...] = dv_ref[...].astype(jnp.bfloat16)
    grad = narrow_ref[...]
    size = w0_ref.shape[2]
    spot_sp = lax.axis_index("sp") % 4
    for ref, spot in ((own_ref, place), (far_ref, (place + 2) % 4), (near_ref, near), (next_ref, (near + 2) % 4)):
        block = tn(grad, ref[...]).astype(jnp.bfloat16)
        for i in range(cols // size):
            part = spot * (cols // size) + i
            all_ref[(part % 4) ^ spot_sp, part // 4] = block[:, i * size : (i + 1) * size]
    for i, ref in enumerate((w0_ref, w1_ref, w2_ref, w3_ref)):
        ref[...] = all_ref[i]


def fold_kernel(p0_ref, p1_ref, p2_ref, p3_ref, keep_ref, send_ref):
    bit = lax.axis_index("sp") // 4
    for ref, spot in ((keep_ref, bit), (send_ref, 1 - bit)):
        total = p0_ref[spot].astype(jnp.float32)
        for piece in (p1_ref, p2_ref, p3_ref):
            total += piece[spot].astype(jnp.float32)
        ref[...] = jnp.transpose(total).astype(ref.dtype)


def join_pieces(block_ref, first, half, lane0):
    parts = [block_ref[first + 16 * i : first + 16 * (i + 1), lane0 : lane0 + half].astype(jnp.float32) for i in range(2)]
    sums = [p[0:4] + p[4:8] + p[8:12] for p in parts]
    return jnp.concatenate(sums, axis=1)


SCALE = LOG2E / 8.0


def halves(x):
    left = lax.broadcasted_iota(jnp.int32, (1, LANES), 1) < LANES // 2
    none = jnp.zeros((), x.dtype)
    return jnp.where(left, x, none), jnp.where(left, none, x)


def fill_slots(slots, q_ref, k_ref, grad_ref, aux_ref, received, a_ref, b_ref, aux_all):
    rows = q_ref.shape[0]
    half = rows // 2
    for slot in slots:
        lanes = slice((slot % 2) * LANES, (slot % 2 + 1) * LANES)
        if slot < 2:
            a_ref[slot] = q_ref[:, lanes]
            b_ref[slot] = grad_ref[:, lanes]
            aux_all[slot, 0:4, :] = aux_ref[8 * slot : 8 * slot + 4, :]
        elif slot < 4:
            a_ref[slot] = k_ref[:, lanes]
        elif slot < 6:
            ref = received[slot]
            a_ref[slot] = ref[0:rows, 0:LANES]
            b_ref[slot] = ref[0:rows, LANES : 2 * LANES]
            aux_all[slot, 0:4, :] = join_pieces(ref, rows, half, 0)
        elif slot < 8:
            for part, ref in enumerate(received[slot]):
                spot = slice(part * half, (part + 1) * half)
                a_ref[slot, spot, :] = ref[0:half, 0:LANES]
                b_ref[slot, spot, :] = ref[0:half, LANES : 2 * LANES]
            aux_all[slot, 0:4, :] = join_pieces(received[slot][0], half, half, 0)
        elif slot == 8:
            a_ref[slot] = received[4][0:rows, 4 * LANES : 5 * LANES]
        else:
            ref = received[4]
            a_ref[slot] = ref[0:rows, 2 * LANES : 3 * LANES]
            b_ref[slot] = ref[0:rows, 3 * LANES : 4 * LANES]
            aux_all[slot, 0:4, :] = join_pieces(ref, rows, half, half)


def maps_of(buf, aux, masked):
    map0 = jnp.exp2(buf[0] * SCALE - aux[0:1])
    map1 = jnp.exp2(buf[1] * SCALE - aux[1:2])
    if masked:
        key_pos = lax.broadcasted_iota(jnp.int32, map0.shape, 0)
        query_pos = lax.broadcasted_iota(jnp.int32, map0.shape, 1)
        seen = key_pos <= query_pos
        map0 = jnp.where(seen, map0, 0.0)
        map1 = jnp.where(seen, map1, 0.0)
    return map0, map1


def pick(u):
    level = 0 if u == 0 else 1 if u < 3 else 2
    early = level_bits()[level] == 0
    other = 4 + (u + 1) // 2
    own = u == 0 or u % 2 == 1
    return jnp.where(early, other, 1 if own else 9), jnp.where(early, 2 if own else 8, other)


def each_unit(units, products, consume, bufs):
    products(*units[0][:2], bufs[0])
    for i, (qs, ks, masked) in enumerate(units):
        if i + 1 < len(units):
            products(*units[i + 1][:2], bufs[(i + 1) % 2])
        consume(qs, ks, bufs[i % 2], masked)


def mixed_work(a_ref, b_ref, aux_all, s_ref):
    def products(qs, ks, buf):
        query0, query1 = halves(a_ref[qs])
        key = a_ref[ks]
        buf[0] = nt(key, query0)
        buf[1] = nt(key, query1)

    def consume(qs, ks, buf, masked):
        map0, map1 = maps_of(buf, aux_all[qs], masked)
        mixed = (map0 - map1).astype(jnp.bfloat16)
        s_ref[ks] += jnp.dot(mixed, b_ref[qs], preferred_element_type=jnp.float32)

    return products, consume


def mixed_first(
    q_ref, k_ref, grad_ref, aux_ref, rx_ref, rz_ref, r4a_ref, r4b_ref, v_ref,
    carry_ref, tz_ref, t4_ref, a_ref, b_ref, aux_all, s_ref, buf0, buf1,
):
    received = {4: rx_ref, 5: rz_ref, 6: (r4a_ref, r4b_ref)}
    fill_slots((0, 1, 2, 3, 4, 5, 6, 8, 9), q_ref, k_ref, grad_ref, aux_ref, received, a_ref, b_ref, aux_all)
    for slot in (2, 3, 4, 5, 6, 8):
        s_ref[slot] = jnp.zeros(s_ref.shape[1:], jnp.float32)
    units = [(*pick(u), False) for u in range(5)] + [(0, 2, True), (1, 3, True)]
    each_unit(units, *mixed_work(a_ref, b_ref, aux_all, s_ref), (buf0, buf1))
    for i, slot in enumerate((2, 3, 4, 8)):
        carry_ref[i] = s_ref[slot]
    bits = level_bits()
    for ref, slot, bit in ((tz_ref, 5, bits[1]), (t4_ref, 6, bits[2])):
        going_up(ref, 0, v_ref, s_ref, slot, bit)


def going_up(ref, lane0, v_ref, s_ref, slot, bit):
    @pl.when(bit == 0)
    def _():
        ref[:, lane0 : lane0 + LANES] = v_ref[:, LANES : 2 * LANES]

    @pl.when(bit != 0)
    def _():
        ref[:, lane0 : lane0 + LANES] = s_ref[slot].astype(jnp.bfloat16)


def mixed_second(
    q_ref, k_ref, grad_ref, aux_ref, rx_ref, r6a_ref, r6b_ref, v_ref, carry_ref,
    dv_ref, tx_ref, t6_ref, a_ref, b_ref, aux_all, s_ref, buf0, buf1,
):
    received = {4: rx_ref, 7: (r6a_ref, r6b_ref)}
    fill_slots((1, 2, 7, 8, 9), q_ref, k_ref, grad_ref, aux_ref, received, a_ref, b_ref, aux_all)
    s_ref[7] = jnp.zeros(s_ref.shape[1:], jnp.float32)
    for i, slot in enumerate((2, 3, 4, 8)):
        s_ref[slot] = carry_ref[i]
    each_unit([(*pick(u), False) for u in (5, 6)], *mixed_work(a_ref, b_ref, aux_all, s_ref), (buf0, buf1))
    dv_ref[...] = s_ref[2:4]
    tx_ref[:, 0:LANES] = s_ref[8].astype(jnp.bfloat16)
    tx_ref[:, LANES : 2 * LANES] = s_ref[4].astype(jnp.bfloat16)
    going_up(t6_ref, 0, v_ref, s_ref, 7, level_bits()[2])


def score_work(a_ref, b_ref, aux_all, s_ref):
    rows = a_ref.shape[1]

    def products(qs, ks, buf):
        query0, query1 = halves(a_ref[qs])
        key = a_ref[ks]
        buf[0] = nt(key, query0)
        buf[1] = nt(key, query1)
        buf[2] = nt(b_ref[ks], b_ref[qs])

    def consume(qs, ks, buf, masked):
        query0, query1 = halves(a_ref[qs])
        key0, key1 = halves(a_ref[ks])
        aux = aux_all[qs]
        map0, map1 = maps_of(buf, aux, masked)
        dots = buf[2]
        score0 = (map0 * (dots - aux[2:3])).astype(jnp.bfloat16)
        score1 = (map1 * (aux[3:4] - dots)).astype(jnp.bfloat16)
        s_ref[ks] += jnp.dot(score0, query0, preferred_element_type=jnp.float32) + jnp.dot(
            score1, query1, preferred_element_type=jnp.float32
        )
        turned = tn(key0, score0) + tn(key1, score1)
        for i in range(rows // LANES):
            s_ref[qs, i * LANES : (i + 1) * LANES, :] += turned[:, i * LANES : (i + 1) * LANES]

    return products, consume


def late_values(b_ref, slot, ref, lane0, bit):
    @pl.when(bit != 0)
    def _():
        b_ref[slot] = ref[:, lane0 : lane0 + LANES]


def score_own(q_ref, k_ref, grad_ref, aux_ref, rx_ref, v_ref, vx_ref, own_ref, near_ref, a_ref, b_ref, aux_all, s_ref, buf0, buf1):
    fill_slots((0, 1, 2, 3, 4), q_ref, k_ref, grad_ref, aux_ref, {4: rx_ref}, a_ref, b_ref, aux_all)
    for h in range(2):
        b_ref[2 + h] = v_ref[:, h * LANES : (h + 1) * LANES]
    late_values(b_ref, 4, vx_ref, LANES, level_bits()[0])
    s_ref[0:5] = jnp.zeros((5,) + s_ref.shape[1:], jnp.float32)
    units = [(*pick(0), False), (0, 2, True), (1, 3, True)]
    each_unit(units, *score_work(a_ref, b_ref, aux_all, s_ref), (buf0, buf1))
    own_ref[...] = s_ref[0:4]
    near_ref[...] = s_ref[4].astype(jnp.bfloat16)


CARRIED = (1, 2, 5)


def score_far(
    q_ref, k_ref, grad_ref, aux_ref, rx_ref, rz_ref, r4a_ref, r4b_ref, r6a_ref, r6b_ref, v_ref, vx_ref, vz_ref, v4_ref, v6_ref, near_ref,
    carry_ref, tx_ref, t4_ref, t6_ref, a_ref, b_ref, aux_all, s_ref, buf0, buf1,
):
    bits = level_bits()
    received = {4: rx_ref, 5: rz_ref, 6: (r4a_ref, r4b_ref), 7: (r6a_ref, r6b_ref)}
    used = (1, 2, 5, 6, 7, 8, 9)
    fill_slots(used, q_ref, k_ref, grad_ref, aux_ref, received, a_ref, b_ref, aux_all)
    b_ref[2] = v_ref[:, 0:LANES]
    b_ref[8] = vx_ref[:, 0:LANES]
    late_values(b_ref, 5, vz_ref, 0, bits[1])
    late_values(b_ref, 6, v4_ref, 0, bits[2])
    late_values(b_ref, 7, v6_ref, 0, bits[2])
    for slot in used:
        s_ref[slot] = jnp.zeros(s_ref.shape[1:], jnp.float32)
    each_unit([(*pick(u), False) for u in (3, 4, 5, 6, 2)], *score_work(a_ref, b_ref, aux_all, s_ref), (buf0, buf1))
    for i, slot in enumerate(CARRIED):
        carry_ref[i] = s_ref[slot]
    t4_ref[...] = s_ref[6].astype(jnp.bfloat16)
    t6_ref[...] = s_ref[7].astype(jnp.bfloat16)
    tx_ref[:, 0:LANES] = near_ref[...]
    for i, slot in enumerate((8, 9)):
        tx_ref[:, (i + 1) * LANES : (i + 2) * LANES] = s_ref[slot].astype(jnp.bfloat16)


def score_near(
    q_ref, k_ref, grad_ref, aux_ref, rz_ref, v_ref, vz_ref, own0_ref, carry_ref,
    own_ref, tz_ref, a_ref, b_ref, aux_all, s_ref, buf0, buf1,
):
    fill_slots((1, 2, 5), q_ref, k_ref, grad_ref, aux_ref, {5: rz_ref}, a_ref, b_ref, aux_all)
    b_ref[2] = v_ref[:, 0:LANES]
    late_values(b_ref, 5, vz_ref, 0, level_bits()[1])
    for i, slot in enumerate(CARRIED):
        s_ref[slot] = carry_ref[i]
    each_unit([(*pick(1), False)], *score_work(a_ref, b_ref, aux_all, s_ref), (buf0, buf1))
    own_ref[...] = own0_ref[...]
    own_ref[1] += s_ref[1]
    own_ref[2] += s_ref[2]
    tz_ref[...] = s_ref[5].astype(jnp.bfloat16)


def join_kernel(own_ref, ux_ref, uz_ref, u4_ref, u6_ref, dq_ref, dk_ref, s_ref):
    bits = level_bits()
    for i in range(4):
        s_ref[i] = own_ref[i]
    s_ref[2] += ux_ref[:, LANES : 2 * LANES].astype(jnp.float32)
    s_ref[1] += ux_ref[:, 2 * LANES : 3 * LANES].astype(jnp.float32)
    for ref, bit in ((ux_ref, bits[0]), (uz_ref, bits[1]), (u4_ref, bits[2]), (u6_ref, bits[2])):
        spot = jnp.where(bit == 0, 3, 0)
        s_ref[spot] += ref[:, 0:LANES].astype(jnp.float32)
    for h in range(2):
        for i in range(s_ref.shape[1] // LANES):
            spot = slice(i * LANES, (i + 1) * LANES)
            dq_ref[spot, h * LANES : (h + 1) * LANES] = jnp.transpose(s_ref[h, spot, :]) * 0.125
        dk_ref[:, h * LANES : (h + 1) * LANES] = s_ref[2 + h] * 0.125


def call(kernel, outs, args, scratch=(), smem=(), micros=1, grant=12):
    vmem = pl.BlockSpec(memory_space=pltpu.VMEM)
    specs = [pl.BlockSpec(memory_space=pltpu.SMEM) if i in smem else vmem for i in range(len(args))]
    return pl.pallas_call(
        kernel,
        out_shape=[jax.ShapeDtypeStruct(s, d) for s, d in outs],
        in_specs=specs,
        out_specs=[vmem] * len(outs),
        scratch_shapes=list(scratch),
        cost_estimate=pl.CostEstimate(flops=micros * 14_000_000, bytes_accessed=1_000_000, transcendentals=0),
        compiler_params=pltpu.CompilerParams(vmem_limit_bytes=grant * 2**20),
    )(*args)


def swap(x, axis, size, mask):
    return lax.ppermute(x, axis, [(i, i ^ mask) for i in range(size)])


def paired_device(*args):
    return paired_steps(*args)


def paired_steps(queries, key_vectors, latents, w_value, log_sums, out_pair, cotangent, lambdas, out_gain):
    rows, width = queries.shape
    narrow, wide = jnp.bfloat16, jnp.float32
    seq, feat = lax.axis_size("sp"), lax.axis_size("tp")
    slot_shape = (rows, LANES)
    half = rows // 2
    far = swap(latents, "tp", feat, 2)
    near = swap(latents, "tp", feat, 1)
    grad, aux, px, pz, pma, pmb = call(
        prep_kernel,
        [((rows, width), narrow), ((16, rows), wide), ((rows + AUX_ROWS, 5 * LANES), narrow),
         ((rows + AUX_ROWS, width), narrow), ((half + AUX_ROWS, width), narrow), ((half, width), narrow)],
        (queries, key_vectors, log_sums.T, out_pair, cotangent, lambdas, out_gain[None, :]),
        smem=(5,), micros=4, grant=58,
    )
    r4 = swap(pma, "sp", seq, 4), swap(pmb, "sp", seq, 4)
    rz = swap(pz, "sp", seq, 2)
    rx = swap(px, "sp", seq, 1)
    r6 = swap(r4[0], "sp", seq, 2), swap(r4[1], "sp", seq, 2)
    next_far = swap(far, "tp", feat, 1)
    values, = call(value_kernel, [((rows, width), narrow)], (latents, far, near, next_far, w_value), micros=3)
    vx = swap(values, "sp", seq, 1)
    slots = [pltpu.VMEM((SLOTS,) + slot_shape, narrow), pltpu.VMEM((SLOTS,) + slot_shape, narrow), pltpu.VMEM((SLOTS, 8, rows), wide)]
    sums = [pltpu.VMEM((SLOTS,) + slot_shape, wide)]
    two, three = [pltpu.VMEM((2, rows, rows), wide)] * 2, [pltpu.VMEM((3, rows, rows), wide)] * 2
    base = (queries, key_vectors, grad, aux)
    carry, tz, t4 = call(
        mixed_first, [((4,) + slot_shape, wide)] + [(slot_shape, narrow)] * 2,
        base + (rx, rz) + r4 + (values,), scratch=slots + sums + two, micros=5, grant=20,
    )
    dv0, tx, t6 = call(
        mixed_second, [((2,) + slot_shape, wide), ((rows, 2 * LANES), narrow), (slot_shape, narrow)],
        base + (rx,) + r6 + (values, carry), scratch=slots + sums + two, micros=2, grant=20,
    )
    u4 = swap(t4, "sp", seq, 4)
    u6 = swap(t6, "sp", seq, 6)
    uz = swap(tz, "sp", seq, 2)
    ux = swap(tx, "sp", seq, 1)
    own0, near_sum = call(
        score_own, [((4,) + slot_shape, wide), (slot_shape, narrow)], base + (rx, values, vx),
        scratch=slots + sums + three, micros=4, grant=24,
    )
    piece = (2, width, latents.shape[1] * feat // seq)
    w0, w1, w2, w3, dv = call(
        weight_kernel, [(piece, narrow)] * 4 + [((rows, width), wide)],
        (latents, far, near, next_far, dv0, ux, uz, u4, u6),
        scratch=[pltpu.VMEM((4,) + piece, narrow), pltpu.VMEM((rows, width), narrow)], micros=5,
    )
    w3 = swap(w3, "sp", seq, 3)
    w1 = swap(w1, "sp", seq, 1)
    w2 = swap(w2, "sp", seq, 2)
    carry, sx, s4, s6 = call(
        score_far, [((3,) + slot_shape, wide), ((rows, 3 * LANES), narrow)] + [(slot_shape, narrow)] * 2,
        base + (rx, rz) + r4 + r6 + (values, vx, uz, u4, u6, near_sum), scratch=slots + sums + three, micros=7, grant=58,
    )
    w4 = swap(s4, "sp", seq, 4)
    w6 = swap(s6, "sp", seq, 6)
    wx = swap(sx, "sp", seq, 1)
    keep, send = call(fold_kernel, [(piece[:0:-1], wide), (piece[:0:-1], narrow)], (w0, w1, w2, w3), micros=1)
    last = swap(send, "sp", seq, 4)
    own, sz = call(
        score_near, [((4,) + slot_shape, wide), (slot_shape, narrow)],
        base + (rz, values, uz, own0, carry), scratch=slots + sums + three, micros=3, grant=24,
    )
    wz = swap(sz, "sp", seq, 2)
    dq, dk = call(
        join_kernel, [((rows, width), wide)] * 2, (own, wx, wz, w4, w6),
        scratch=[pltpu.VMEM((4,) + slot_shape, wide)], micros=3,
    )
    return dq, dk, dv, keep + last.astype(wide)


def solution(mesh):
    paired = (mesh.shape["sp"], mesh.shape["tp"]) == (8, 4)
    return jax.shard_map(
        paired_device if paired else general_device,
        mesh=mesh,
        in_specs=(
            P("sp", "tp"),
            P("sp", "tp"),
            P("sp", "tp"),
            P(None, "tp"),
            P("sp", "tp"),
            P("sp", "tp"),
            P("sp", "tp"),
            P("tp"),
            P(),
        ),
        out_specs=(P("sp", "tp"), P("sp", "tp"), P("sp", "tp"), P("sp", "tp")),
        check_vma=False,
    )
```

```python
import jax
import jax.numpy as jnp
from jax import lax
from jax.experimental import pallas as pl
from jax.experimental.pallas import tpu as pltpu
from jax.sharding import PartitionSpec as P


norm_floor = 0.25
block_rows = 512


def head_cotangent(out_pair, cotangent, lambdas, out_gain):
    tok_rows = out_pair.shape[0]
    head_count = lambdas.shape[0]
    out_maps = out_pair.astype(jnp.float32).reshape(tok_rows, head_count, 2, -1)
    lam_cols = lambdas[None, :, None]
    merged = out_maps[:, :, 0] - lam_cols * out_maps[:, :, 1]
    inv_norm = lax.rsqrt(jnp.mean(merged * merged, axis=-1, keepdims=True) + norm_floor)
    scaled = cotangent.astype(jnp.float32).reshape(merged.shape) * out_gain
    inner_dot = jnp.mean(scaled * merged, axis=-1, keepdims=True)
    out_grad = (inv_norm * scaled - merged * (inv_norm * inv_norm * inv_norm) * inner_dot).astype(
        jnp.bfloat16
    )
    grad_wide = out_grad.astype(jnp.float32)
    first_map = jnp.sum(grad_wide * out_maps[:, :, 0], axis=-1)
    second_map = -lambdas[None, :] * jnp.sum(grad_wide * out_maps[:, :, 1], axis=-1)
    return (out_grad, jnp.stack([first_map, second_map], axis=-1))


def block_terms(
    query_block,
    key_block,
    value_block,
    grad_block,
    log_block,
    term_block,
    lambdas,
    query_pos,
    key_pos,
):
    factor = query_block.shape[-1] ** (-0.5)
    scores = (
        jnp.einsum("qhcd,khcd->hcqk", query_block, key_block, preferred_element_type=jnp.float32)
        * factor
    )
    visible = key_pos[None, :] <= query_pos[:, None]
    shifted = scores - jnp.transpose(log_block, (1, 2, 0))[..., None]
    softmax_maps = jnp.where(visible, jnp.exp(shifted), 0.0)
    value_dot = jnp.einsum(
        "qhe,khe->hqk", grad_block, value_block, preferred_element_type=jnp.float32
    )
    lam_cols = lambdas[:, None, None]
    weights = (softmax_maps[:, 0] - lam_cols * softmax_maps[:, 1]).astype(jnp.bfloat16)
    term_cols = jnp.transpose(term_block, (1, 2, 0))
    first_map = softmax_maps[:, 0] * (value_dot - term_cols[:, 0, :, None])
    second_map = softmax_maps[:, 1] * (-lam_cols * value_dot - term_cols[:, 1, :, None])
    dscore = (jnp.stack([first_map, second_map], axis=1) * factor).astype(jnp.bfloat16)
    return (weights, dscore)


def block_span():
    return block_rows


def general_device(
    queries, key_vectors, latents, w_value, log_sums, out_pair, cotangent, lambdas, out_gain
):
    tok_rows = queries.shape[0]
    head_count = lambdas.shape[0]
    offset = lax.axis_index("sp") * tok_rows
    own_pos = offset + jnp.arange(tok_rows, dtype=jnp.int32)
    last_pos = offset + tok_rows - 1
    gathered = lax.all_gather(latents, "tp", axis=1, tiled=True)
    values = jnp.dot(gathered, w_value, preferred_element_type=jnp.float32).astype(jnp.bfloat16)
    out_grad, row_terms = head_cotangent(out_pair, cotangent, lambdas, out_gain)
    query_heads = queries.reshape(tok_rows, head_count, 2, -1)
    key_heads = key_vectors.reshape(tok_rows, head_count, 2, -1)
    value_heads = values.reshape(tok_rows, head_count, -1)
    log_heads = log_sums.reshape(tok_rows, head_count, 2)
    grad_flat = out_grad.reshape(tok_rows, -1)
    term_flat = row_terms.reshape(tok_rows, -1)
    zero_keys = jnp.zeros(key_heads.shape, jnp.float32)
    zero_values = jnp.zeros(value_heads.shape, jnp.float32)
    shards = (
        lax.all_gather(key_vectors, "sp", axis=0, tiled=True),
        lax.all_gather(values, "sp", axis=0, tiled=True),
    )
    key_piece = shards[0]
    value_piece = shards[1]
    piece_rows = key_piece.shape[0]
    block_len = block_span()

    def query_add_block(block_idx, partial_value):
        begin_row = block_idx * block_len
        key_block = lax.dynamic_slice_in_dim(key_piece, begin_row, block_len, 0).reshape(
            block_len, head_count, 2, -1
        )
        value_block = lax.dynamic_slice_in_dim(value_piece, begin_row, block_len, 0).reshape(
            block_len, head_count, -1
        )
        key_pos = begin_row + jnp.arange(block_len, dtype=jnp.int32)

        def query_compute(sums):
            _, dscore = block_terms(
                query_heads,
                key_block,
                value_block,
                out_grad,
                log_heads,
                row_terms,
                lambdas,
                own_pos,
                key_pos,
            )
            return sums + jnp.einsum(
                "hcqk,khcd->qhcd", dscore, key_block, preferred_element_type=jnp.float32
            )

        return lax.cond(begin_row <= last_pos, query_compute, lambda sums: sums, partial_value)

    query_grad = lax.fori_loop(0, piece_rows // block_len, query_add_block, zero_keys)
    shards = (
        lax.all_gather(queries.astype(jnp.float32), "sp", axis=0, tiled=True).astype(jnp.bfloat16),
        lax.all_gather(grad_flat.astype(jnp.float32), "sp", axis=0, tiled=True).astype(
            jnp.bfloat16
        ),
        lax.all_gather(log_sums, "sp", axis=0, tiled=True),
        lax.all_gather(term_flat, "sp", axis=0, tiled=True),
    )
    query_piece = shards[0]
    grad_piece = shards[1]
    log_piece = shards[2]
    term_piece = shards[3]
    piece_rows = query_piece.shape[0]
    key_block_len = block_span()

    def key_add_block(block_idx, partial_value):
        begin_row = block_idx * key_block_len
        query_block = lax.dynamic_slice_in_dim(query_piece, begin_row, key_block_len, 0).reshape(
            key_block_len, head_count, 2, -1
        )
        grad_block = lax.dynamic_slice_in_dim(grad_piece, begin_row, key_block_len, 0).reshape(
            key_block_len, head_count, -1
        )
        log_block = lax.dynamic_slice_in_dim(log_piece, begin_row, key_block_len, 0).reshape(
            key_block_len, head_count, 2
        )
        term_block = lax.dynamic_slice_in_dim(term_piece, begin_row, key_block_len, 0).reshape(
            key_block_len, head_count, 2
        )
        query_pos = begin_row + jnp.arange(key_block_len, dtype=jnp.int32)

        def key_compute(sums):
            weights, dscore = block_terms(
                query_block,
                key_heads,
                value_heads,
                grad_block,
                log_block,
                term_block,
                lambdas,
                query_pos,
                own_pos,
            )
            key_sum = sums[0] + jnp.einsum(
                "hcqk,qhcd->khcd", dscore, query_block, preferred_element_type=jnp.float32
            )
            value_sum = sums[1] + jnp.einsum(
                "hqk,qhe->khe", weights, grad_block, preferred_element_type=jnp.float32
            )
            return (key_sum, value_sum)

        return lax.cond(
            begin_row + key_block_len - 1 >= offset, key_compute, lambda sums: sums, partial_value
        )

    key_grad, value_grad = lax.fori_loop(
        0, piece_rows // key_block_len, key_add_block, (zero_keys, zero_values)
    )
    value_flat = value_grad.reshape(tok_rows, -1)
    value_narrow = value_flat.astype(jnp.bfloat16)
    weight_grad = lax.psum_scatter(
        lax.dot_general(
            gathered, value_narrow, (((0,), (0,)), ((), ())), preferred_element_type=jnp.float32
        ),
        "sp",
        scatter_dimension=0,
        tiled=True,
    )
    return (
        query_grad.reshape(tok_rows, -1),
        key_grad.reshape(tok_rows, -1),
        value_flat,
        weight_grad,
    )


LOG2E = 1.4426950408889634
AUX_ROWS = 32
SLOTS = 10
LANES = 128


def nt(a, b):
    return lax.dot_general(a, b, (((1,), (1,)), ((), ())), preferred_element_type=jnp.float32)


def tn(a, b):
    return lax.dot_general(a, b, (((0,), (0,)), ((), ())), preferred_element_type=jnp.float32)


def level_bits():
    place = lax.axis_index("sp")
    return place % 2, (place // 2) % 2, (place // 4) % 2


def split_pieces(rows):
    high = rows.astype(jnp.bfloat16)
    rest = rows - high.astype(jnp.float32)
    middle = rest.astype(jnp.bfloat16)
    low = (rest - middle.astype(jnp.float32)).astype(jnp.bfloat16)
    return high, middle, low


def prep_kernel(q_ref, k_ref, log_ref, pair_ref, cot_ref, lam_ref, gain_ref, grad_ref, aux_ref, px_ref, pz_ref, pma_ref, pmb_ref):
    rows = q_ref.shape[0]
    half = rows // 2
    bit0, bit1, bit2 = level_bits()
    lane = lax.broadcasted_iota(jnp.int32, (rows, LANES), 1)
    aux_blocks = []
    for h in range(2):
        first = pair_ref[:, 2 * h * LANES : (2 * h + 1) * LANES].astype(jnp.float32)
        second = pair_ref[:, (2 * h + 1) * LANES : (2 * h + 2) * LANES].astype(jnp.float32)
        lam = lam_ref[h]
        merged = first - lam * second
        inv = lax.rsqrt(jnp.mean(merged * merged, axis=-1, keepdims=True) + norm_floor)
        scaled = cot_ref[:, h * LANES : (h + 1) * LANES].astype(jnp.float32) * gain_ref[...]
        inner = jnp.mean(scaled * merged, axis=-1, keepdims=True)
        grad = (inv * scaled - merged * (inv * inv * inv) * inner).astype(jnp.bfloat16)
        grad_ref[:, h * LANES : (h + 1) * LANES] = grad
        wide = grad.astype(jnp.float32)
        term0 = jnp.sum(wide * first, axis=-1, keepdims=True)
        term1 = jnp.sum(wide * second, axis=-1, keepdims=True)
        terms = jnp.where(lane == 2, term0, jnp.where(lane == 3, term1, 0.0))
        turned = jnp.concatenate(
            [jnp.transpose(terms[i * LANES : (i + 1) * LANES])[0:8] for i in range(rows // LANES)], axis=1
        )
        log0 = log_ref[2 * h : 2 * h + 1, :] * LOG2E
        log1 = (log_ref[2 * h + 1 : 2 * h + 2, :] - jnp.log(jnp.full((1, rows), lam, jnp.float32))) * LOG2E
        aux = jnp.concatenate([log0, log1, turned[2:4], jnp.zeros((4, rows), jnp.float32)], axis=0)
        aux_ref[h * 8 : (h + 1) * 8, :] = aux
        pieces = split_pieces(aux)
        wide_rows = jnp.concatenate([p.astype(jnp.float32)[0:4] for p in pieces] + [jnp.zeros((4, rows), jnp.float32)], axis=0)
        aux_blocks.append(wide_rows.astype(jnp.bfloat16))

    def put(ref, first, count, early):
        spot = slice(first, first + count)

        @pl.when(early)
        def _():
            ref[0:count, 0:LANES] = k_ref[spot, LANES : 2 * LANES]
            ref[0:count, LANES : 2 * LANES] = k_ref[spot, LANES : 2 * LANES]

        @pl.when(jnp.logical_not(early))
        def _():
            ref[0:count, 0:LANES] = q_ref[spot, 0:LANES]
            ref[0:count, LANES : 2 * LANES] = grad_ref[spot, 0:LANES]

    def put_aux(ref, first, lane0, h):
        ref[first : first + 16, lane0 : lane0 + half] = aux_blocks[h][:, 0:half]
        ref[first + 16 : first + 32, lane0 : lane0 + half] = aux_blocks[h][:, half:rows]

    put(pma_ref, 0, half, bit2 == 0)
    put_aux(pma_ref, half, 0, 0)
    put(pmb_ref, half, half, bit2 == 0)
    put(pz_ref, 0, rows, bit1 == 0)
    put_aux(pz_ref, rows, 0, 0)
    put(px_ref, 0, rows, bit0 == 0)
    px_ref[0:rows, 2 * LANES : 3 * LANES] = q_ref[:, LANES : 2 * LANES]
    px_ref[0:rows, 3 * LANES : 4 * LANES] = grad_ref[:, LANES : 2 * LANES]
    px_ref[0:rows, 4 * LANES : 5 * LANES] = k_ref[:, 0:LANES]
    px_ref[rows : rows + 32, 4 * LANES : 5 * LANES] = jnp.zeros((32, LANES), jnp.bfloat16)
    put_aux(px_ref, rows, 0, 0)
    put_aux(px_ref, rows, half, 1)


def value_kernel(own_ref, far_ref, near_ref, next_ref, w_ref, out_ref):
    cols = own_ref.shape[1]
    place = lax.axis_index("tp")

    def part(x, spot):
        return jnp.dot(x, w_ref[pl.ds(spot * cols, cols), :], preferred_element_type=jnp.float32)

    total = part(own_ref[...], place) + part(far_ref[...], (place + 2) % 4)
    near = place + 1 - 2 * (place % 2)
    total += part(near_ref[...], near) + part(next_ref[...], (near + 2) % 4)
    out_ref[...] = total.astype(jnp.bfloat16)


def weight_kernel(own_ref, far_ref, near_ref, next_ref, dv0_ref, ux_ref, uz_ref, u4_ref, u6_ref, w0_ref, w1_ref, w2_ref, w3_ref, dv_ref, all_ref, narrow_ref):
    bits = level_bits()
    cols = own_ref.shape[1]
    place = lax.axis_index("tp")
    near = place + 1 - 2 * (place % 2)
    dv_ref[:, 0:LANES] = dv0_ref[0] + ux_ref[:, 0:LANES].astype(jnp.float32)
    dv_ref[:, LANES : 2 * LANES] = dv0_ref[1]
    for ref, lane0, bit in ((ux_ref, LANES, bits[0]), (uz_ref, 0, bits[1]), (u4_ref, 0, bits[2]), (u6_ref, 0, bits[2])):

        @pl.when(bit == 0)
        def _(ref=ref, lane0=lane0):
            dv_ref[:, LANES : 2 * LANES] += ref[:, lane0 : lane0 + LANES].astype(jnp.float32)

    narrow_ref[...] = dv_ref[...].astype(jnp.bfloat16)
    grad = narrow_ref[...]
    size = w0_ref.shape[2]
    spot_sp = lax.axis_index("sp") % 4
    for ref, spot in ((own_ref, place), (far_ref, (place + 2) % 4), (near_ref, near), (next_ref, (near + 2) % 4)):
        block = tn(grad, ref[...]).astype(jnp.bfloat16)
        for i in range(cols // size):
            part = spot * (cols // size) + i
            all_ref[(part % 4) ^ spot_sp, part // 4] = block[:, i * size : (i + 1) * size]
    for i, ref in enumerate((w0_ref, w1_ref, w2_ref, w3_ref)):
        ref[...] = all_ref[i]


def fold_kernel(p0_ref, p1_ref, p2_ref, p3_ref, keep_ref, send_ref):
    bit = lax.axis_index("sp") // 4
    for ref, spot in ((keep_ref, bit), (send_ref, 1 - bit)):
        total = p0_ref[spot].astype(jnp.float32)
        for piece in (p1_ref, p2_ref, p3_ref):
            total += piece[spot].astype(jnp.float32)
        ref[...] = jnp.transpose(total).astype(ref.dtype)


def join_pieces(block_ref, first, half, lane0):
    parts = [block_ref[first + 16 * i : first + 16 * (i + 1), lane0 : lane0 + half].astype(jnp.float32) for i in range(2)]
    sums = [p[0:4] + p[4:8] + p[8:12] for p in parts]
    return jnp.concatenate(sums, axis=1)


SCALE = LOG2E / 8.0


def halves(x):
    left = lax.broadcasted_iota(jnp.int32, (1, LANES), 1) < LANES // 2
    none = jnp.zeros((), x.dtype)
    return jnp.where(left, x, none), jnp.where(left, none, x)


def fill_slots(slots, q_ref, k_ref, grad_ref, aux_ref, received, a_ref, b_ref, aux_all):
    rows = q_ref.shape[0]
    half = rows // 2
    for slot in slots:
        lanes = slice((slot % 2) * LANES, (slot % 2 + 1) * LANES)
        if slot < 2:
            a_ref[slot] = q_ref[:, lanes]
            b_ref[slot] = grad_ref[:, lanes]
            aux_all[slot, 0:4, :] = aux_ref[8 * slot : 8 * slot + 4, :]
        elif slot < 4:
            a_ref[slot] = k_ref[:, lanes]
        elif slot < 6:
            ref = received[slot]
            a_ref[slot] = ref[0:rows, 0:LANES]
            b_ref[slot] = ref[0:rows, LANES : 2 * LANES]
            aux_all[slot, 0:4, :] = join_pieces(ref, rows, half, 0)
        elif slot < 8:
            for part, ref in enumerate(received[slot]):
                spot = slice(part * half, (part + 1) * half)
                a_ref[slot, spot, :] = ref[0:half, 0:LANES]
                b_ref[slot, spot, :] = ref[0:half, LANES : 2 * LANES]
            aux_all[slot, 0:4, :] = join_pieces(received[slot][0], half, half, 0)
        elif slot == 8:
            a_ref[slot] = received[4][0:rows, 4 * LANES : 5 * LANES]
        else:
            ref = received[4]
            a_ref[slot] = ref[0:rows, 2 * LANES : 3 * LANES]
            b_ref[slot] = ref[0:rows, 3 * LANES : 4 * LANES]
            aux_all[slot, 0:4, :] = join_pieces(ref, rows, half, half)


def maps_of(buf, aux, masked):
    map0 = jnp.exp2(buf[0] * SCALE - aux[0:1])
    map1 = jnp.exp2(buf[1] * SCALE - aux[1:2])
    if masked:
        key_pos = lax.broadcasted_iota(jnp.int32, map0.shape, 0)
        query_pos = lax.broadcasted_iota(jnp.int32, map0.shape, 1)
        seen = key_pos <= query_pos
        map0 = jnp.where(seen, map0, 0.0)
        map1 = jnp.where(seen, map1, 0.0)
    return map0, map1


def pick(u):
    level = 0 if u == 0 else 1 if u < 3 else 2
    early = level_bits()[level] == 0
    other = 4 + (u + 1) // 2
    own = u == 0 or u % 2 == 1
    return jnp.where(early, other, 1 if own else 9), jnp.where(early, 2 if own else 8, other)


def each_unit(units, products, consume, bufs):
    products(*units[0][:2], bufs[0])
    for i, (qs, ks, masked) in enumerate(units):
        if i + 1 < len(units):
            products(*units[i + 1][:2], bufs[(i + 1) % 2])
        consume(qs, ks, bufs[i % 2], masked)


def mixed_work(a_ref, b_ref, aux_all, s_ref):
    def products(qs, ks, buf):
        query0, query1 = halves(a_ref[qs])
        key = a_ref[ks]
        buf[0] = nt(key, query0)
        buf[1] = nt(key, query1)

    def consume(qs, ks, buf, masked):
        map0, map1 = maps_of(buf, aux_all[qs], masked)
        mixed = (map0 - map1).astype(jnp.bfloat16)
        s_ref[ks] += jnp.dot(mixed, b_ref[qs], preferred_element_type=jnp.float32)

    return products, consume


def mixed_first(
    q_ref, k_ref, grad_ref, aux_ref, rx_ref, rz_ref, r4a_ref, r4b_ref, v_ref,
    carry_ref, tz_ref, t4_ref, a_ref, b_ref, aux_all, s_ref, buf0, buf1,
):
    received = {4: rx_ref, 5: rz_ref, 6: (r4a_ref, r4b_ref)}
    fill_slots((0, 1, 2, 3, 4, 5, 6, 8, 9), q_ref, k_ref, grad_ref, aux_ref, received, a_ref, b_ref, aux_all)
    for slot in (2, 3, 4, 5, 6, 8):
        s_ref[slot] = jnp.zeros(s_ref.shape[1:], jnp.float32)
    units = [(*pick(u), False) for u in range(5)] + [(0, 2, True), (1, 3, True)]
    each_unit(units, *mixed_work(a_ref, b_ref, aux_all, s_ref), (buf0, buf1))
    for i, slot in enumerate((2, 3, 4, 8)):
        carry_ref[i] = s_ref[slot]
    bits = level_bits()
    for ref, slot, bit in ((tz_ref, 5, bits[1]), (t4_ref, 6, bits[2])):
        going_up(ref, 0, v_ref, s_ref, slot, bit)


def going_up(ref, lane0, v_ref, s_ref, slot, bit):
    @pl.when(bit == 0)
    def _():
        ref[:, lane0 : lane0 + LANES] = v_ref[:, LANES : 2 * LANES]

    @pl.when(bit != 0)
    def _():
        ref[:, lane0 : lane0 + LANES] = s_ref[slot].astype(jnp.bfloat16)


def mixed_second(
    q_ref, k_ref, grad_ref, aux_ref, rx_ref, r6a_ref, r6b_ref, v_ref, carry_ref,
    dv_ref, tx_ref, t6_ref, a_ref, b_ref, aux_all, s_ref, buf0, buf1,
):
    received = {4: rx_ref, 7: (r6a_ref, r6b_ref)}
    fill_slots((1, 2, 7, 8, 9), q_ref, k_ref, grad_ref, aux_ref, received, a_ref, b_ref, aux_all)
    s_ref[7] = jnp.zeros(s_ref.shape[1:], jnp.float32)
    for i, slot in enumerate((2, 3, 4, 8)):
        s_ref[slot] = carry_ref[i]
    each_unit([(*pick(u), False) for u in (5, 6)], *mixed_work(a_ref, b_ref, aux_all, s_ref), (buf0, buf1))
    dv_ref[...] = s_ref[2:4]
    tx_ref[:, 0:LANES] = s_ref[8].astype(jnp.bfloat16)
    tx_ref[:, LANES : 2 * LANES] = s_ref[4].astype(jnp.bfloat16)
    going_up(t6_ref, 0, v_ref, s_ref, 7, level_bits()[2])


def score_work(a_ref, b_ref, aux_all, s_ref):
    rows = a_ref.shape[1]

    def products(qs, ks, buf):
        query0, query1 = halves(a_ref[qs])
        key = a_ref[ks]
        buf[0] = nt(key, query0)
        buf[1] = nt(key, query1)
        buf[2] = nt(b_ref[ks], b_ref[qs])

    def consume(qs, ks, buf, masked):
        query0, query1 = halves(a_ref[qs])
        key0, key1 = halves(a_ref[ks])
        aux = aux_all[qs]
        map0, map1 = maps_of(buf, aux, masked)
        dots = buf[2]
        score0 = (map0 * (dots - aux[2:3])).astype(jnp.bfloat16)
        score1 = (map1 * (aux[3:4] - dots)).astype(jnp.bfloat16)
        s_ref[ks] += jnp.dot(score0, query0, preferred_element_type=jnp.float32) + jnp.dot(
            score1, query1, preferred_element_type=jnp.float32
        )
        turned = tn(key0, score0) + tn(key1, score1)
        for i in range(rows // LANES):
            s_ref[qs, i * LANES : (i + 1) * LANES, :] += turned[:, i * LANES : (i + 1) * LANES]

    return products, consume


def late_values(b_ref, slot, ref, lane0, bit):
    @pl.when(bit != 0)
    def _():
        b_ref[slot] = ref[:, lane0 : lane0 + LANES]


def score_own(q_ref, k_ref, grad_ref, aux_ref, rx_ref, v_ref, vx_ref, own_ref, near_ref, a_ref, b_ref, aux_all, s_ref, buf0, buf1):
    fill_slots((0, 1, 2, 3, 4), q_ref, k_ref, grad_ref, aux_ref, {4: rx_ref}, a_ref, b_ref, aux_all)
    for h in range(2):
        b_ref[2 + h] = v_ref[:, h * LANES : (h + 1) * LANES]
    late_values(b_ref, 4, vx_ref, LANES, level_bits()[0])
    s_ref[0:5] = jnp.zeros((5,) + s_ref.shape[1:], jnp.float32)
    units = [(*pick(0), False), (0, 2, True), (1, 3, True)]
    each_unit(units, *score_work(a_ref, b_ref, aux_all, s_ref), (buf0, buf1))
    own_ref[...] = s_ref[0:4]
    near_ref[...] = s_ref[4].astype(jnp.bfloat16)


CARRIED = (1, 2, 5)


def score_far(
    q_ref, k_ref, grad_ref, aux_ref, rx_ref, rz_ref, r4a_ref, r4b_ref, r6a_ref, r6b_ref, v_ref, vx_ref, vz_ref, v4_ref, v6_ref, near_ref,
    carry_ref, tx_ref, t4_ref, t6_ref, a_ref, b_ref, aux_all, s_ref, buf0, buf1,
):
    bits = level_bits()
    received = {4: rx_ref, 5: rz_ref, 6: (r4a_ref, r4b_ref), 7: (r6a_ref, r6b_ref)}
    used = (1, 2, 5, 6, 7, 8, 9)
    fill_slots(used, q_ref, k_ref, grad_ref, aux_ref, received, a_ref, b_ref, aux_all)
    b_ref[2] = v_ref[:, 0:LANES]
    b_ref[8] = vx_ref[:, 0:LANES]
    late_values(b_ref, 5, vz_ref, 0, bits[1])
    late_values(b_ref, 6, v4_ref, 0, bits[2])
    late_values(b_ref, 7, v6_ref, 0, bits[2])
    for slot in used:
        s_ref[slot] = jnp.zeros(s_ref.shape[1:], jnp.float32)
    each_unit([(*pick(u), False) for u in (3, 4, 5, 6, 2)], *score_work(a_ref, b_ref, aux_all, s_ref), (buf0, buf1))
    for i, slot in enumerate(CARRIED):
        carry_ref[i] = s_ref[slot]
    t4_ref[...] = s_ref[6].astype(jnp.bfloat16)
    t6_ref[...] = s_ref[7].astype(jnp.bfloat16)
    tx_ref[:, 0:LANES] = near_ref[...]
    for i, slot in enumerate((8, 9)):
        tx_ref[:, (i + 1) * LANES : (i + 2) * LANES] = s_ref[slot].astype(jnp.bfloat16)


def score_near(
    q_ref, k_ref, grad_ref, aux_ref, rz_ref, v_ref, vz_ref, own0_ref, carry_ref,
    own_ref, tz_ref, a_ref, b_ref, aux_all, s_ref, buf0, buf1,
):
    fill_slots((1, 2, 5), q_ref, k_ref, grad_ref, aux_ref, {5: rz_ref}, a_ref, b_ref, aux_all)
    b_ref[2] = v_ref[:, 0:LANES]
    late_values(b_ref, 5, vz_ref, 0, level_bits()[1])
    for i, slot in enumerate(CARRIED):
        s_ref[slot] = carry_ref[i]
    each_unit([(*pick(1), False)], *score_work(a_ref, b_ref, aux_all, s_ref), (buf0, buf1))
    own_ref[...] = own0_ref[...]
    own_ref[1] += s_ref[1]
    own_ref[2] += s_ref[2]
    tz_ref[...] = s_ref[5].astype(jnp.bfloat16)


def join_kernel(own_ref, ux_ref, uz_ref, u4_ref, u6_ref, dq_ref, dk_ref, s_ref):
    bits = level_bits()
    for i in range(4):
        s_ref[i] = own_ref[i]
    s_ref[2] += ux_ref[:, LANES : 2 * LANES].astype(jnp.float32)
    s_ref[1] += ux_ref[:, 2 * LANES : 3 * LANES].astype(jnp.float32)
    for ref, bit in ((ux_ref, bits[0]), (uz_ref, bits[1]), (u4_ref, bits[2]), (u6_ref, bits[2])):
        spot = jnp.where(bit == 0, 3, 0)
        s_ref[spot] += ref[:, 0:LANES].astype(jnp.float32)
    for h in range(2):
        for i in range(s_ref.shape[1] // LANES):
            spot = slice(i * LANES, (i + 1) * LANES)
            dq_ref[spot, h * LANES : (h + 1) * LANES] = jnp.transpose(s_ref[h, spot, :]) * 0.125
        dk_ref[:, h * LANES : (h + 1) * LANES] = s_ref[2 + h] * 0.125


def call(kernel, outs, args, scratch=(), smem=(), micros=1, grant=20):
    vmem = pl.BlockSpec(memory_space=pltpu.VMEM)
    specs = [pl.BlockSpec(memory_space=pltpu.SMEM) if i in smem else vmem for i in range(len(args))]
    return pl.pallas_call(
        kernel,
        out_shape=[jax.ShapeDtypeStruct(s, d) for s, d in outs],
        in_specs=specs,
        out_specs=[vmem] * len(outs),
        scratch_shapes=list(scratch),
        cost_estimate=pl.CostEstimate(flops=micros * 14_000_000, bytes_accessed=1_000_000, transcendentals=0),
        compiler_params=pltpu.CompilerParams(vmem_limit_bytes=grant * 2**20),
    )(*args)


def swap(x, axis, size, mask):
    return lax.ppermute(x, axis, [(i, i ^ mask) for i in range(size)])


def paired_device(*args):
    return paired_steps(*args)


def paired_steps(queries, key_vectors, latents, w_value, log_sums, out_pair, cotangent, lambdas, out_gain):
    rows, width = queries.shape
    narrow, wide = jnp.bfloat16, jnp.float32
    seq, feat = lax.axis_size("sp"), lax.axis_size("tp")
    slot_shape = (rows, LANES)
    half = rows // 2
    far = swap(latents, "tp", feat, 2)
    near = swap(latents, "tp", feat, 1)
    grad, aux, px, pz, pma, pmb = call(
        prep_kernel,
        [((rows, width), narrow), ((16, rows), wide), ((rows + AUX_ROWS, 5 * LANES), narrow),
         ((rows + AUX_ROWS, width), narrow), ((half + AUX_ROWS, width), narrow), ((half, width), narrow)],
        (queries, key_vectors, log_sums.T, out_pair, cotangent, lambdas, out_gain[None, :]),
        smem=(5,), micros=4, grant=58,
    )
    r4 = swap(pma, "sp", seq, 4), swap(pmb, "sp", seq, 4)
    rz = swap(pz, "sp", seq, 2)
    rx = swap(px, "sp", seq, 1)
    r6 = swap(r4[0], "sp", seq, 2), swap(r4[1], "sp", seq, 2)
    next_far = swap(far, "tp", feat, 1)
    values, = call(value_kernel, [((rows, width), narrow)], (latents, far, near, next_far, w_value), micros=3)
    vx = swap(values, "sp", seq, 1)
    slots = [pltpu.VMEM((SLOTS,) + slot_shape, narrow), pltpu.VMEM((SLOTS,) + slot_shape, narrow), pltpu.VMEM((SLOTS, 8, rows), wide)]
    sums = [pltpu.VMEM((SLOTS,) + slot_shape, wide)]
    two, three = [pltpu.VMEM((2, rows, rows), wide)] * 2, [pltpu.VMEM((3, rows, rows), wide)] * 2
    base = (queries, key_vectors, grad, aux)
    carry, tz, t4 = call(
        mixed_first, [((4,) + slot_shape, wide)] + [(slot_shape, narrow)] * 2,
        base + (rx, rz) + r4 + (values,), scratch=slots + sums + two, micros=5, grant=20,
    )
    dv0, tx, t6 = call(
        mixed_second, [((2,) + slot_shape, wide), ((rows, 2 * LANES), narrow), (slot_shape, narrow)],
        base + (rx,) + r6 + (values, carry), scratch=slots + sums + two, micros=2, grant=20,
    )
    u4 = swap(t4, "sp", seq, 4)
    u6 = swap(t6, "sp", seq, 6)
    uz = swap(tz, "sp", seq, 2)
    ux = swap(tx, "sp", seq, 1)
    own0, near_sum = call(
        score_own, [((4,) + slot_shape, wide), (slot_shape, narrow)], base + (rx, values, vx),
        scratch=slots + sums + three, micros=4, grant=24,
    )
    piece = (2, width, latents.shape[1] * feat // seq)
    w0, w1, w2, w3, dv = call(
        weight_kernel, [(piece, narrow)] * 4 + [((rows, width), wide)],
        (latents, far, near, next_far, dv0, ux, uz, u4, u6),
        scratch=[pltpu.VMEM((4,) + piece, narrow), pltpu.VMEM((rows, width), narrow)], micros=5,
    )
    w3 = swap(w3, "sp", seq, 3)
    w1 = swap(w1, "sp", seq, 1)
    w2 = swap(w2, "sp", seq, 2)
    carry, sx, s4, s6 = call(
        score_far, [((3,) + slot_shape, wide), ((rows, 3 * LANES), narrow)] + [(slot_shape, narrow)] * 2,
        base + (rx, rz) + r4 + r6 + (values, vx, uz, u4, u6, near_sum), scratch=slots + sums + three, micros=7, grant=24,
    )
    w4 = swap(s4, "sp", seq, 4)
    w6 = swap(s6, "sp", seq, 6)
    wx = swap(sx, "sp", seq, 1)
    keep, send = call(fold_kernel, [(piece[:0:-1], wide), (piece[:0:-1], narrow)], (w0, w1, w2, w3), micros=1)
    last = swap(send, "sp", seq, 4)
    own, sz = call(
        score_near, [((4,) + slot_shape, wide), (slot_shape, narrow)],
        base + (rz, values, uz, own0, carry), scratch=slots + sums + three, micros=3, grant=24,
    )
    wz = swap(sz, "sp", seq, 2)
    dq, dk = call(
        join_kernel, [((rows, width), wide)] * 2, (own, wx, wz, w4, w6),
        scratch=[pltpu.VMEM((4,) + slot_shape, wide)], micros=3,
    )
    keep, dq, dk = lax.optimization_barrier((keep, dq, dk))
    return dq, dk, dv, keep + last.astype(wide)


def solution(mesh):
    paired = (mesh.shape["sp"], mesh.shape["tp"]) == (8, 4)
    return jax.shard_map(
        paired_device if paired else general_device,
        mesh=mesh,
        in_specs=(
            P("sp", "tp"),
            P("sp", "tp"),
            P("sp", "tp"),
            P(None, "tp"),
            P("sp", "tp"),
            P("sp", "tp"),
            P("sp", "tp"),
            P("tp"),
            P(),
        ),
        out_specs=(P("sp", "tp"), P("sp", "tp"), P("sp", "tp"), P("sp", "tp")),
        check_vma=False,
    )
```
